256 devices in a mesh: ep: 128 (over z, y, x), tp: 2 (over core).
Axes of the slice: x: 4, y: 4, z: 8, core: 2. Of those that a mesh axis runs over, the one named last changes fastest.
Arguments:
- stream: bfloat16 [2048, 2048], P('ep', 'tp'), may hold values from -6 to 6
- hidden_state: float32 [2048, 2048], P('ep', 'tp'), may hold values from -6 to 6
- conv_state: bfloat16 [2048, 3, 2048], P('ep', None, 'tp'), may hold values from -6 to 6
- first_gain: float32 [2048], P('tp'), may hold values from 0.1 to 1.9
- input_weight: bfloat16 [2048, 2048], P('tp', 'ep'), may hold values from -0.125 to 0.125
- branch_weight: bfloat16 [2048, 2048], P('tp', 'ep'), may hold values from -0.125 to 0.125
- conv_taps: bfloat16 [4, 2048], P(None, 'tp'), may hold values from -3 to 3
- recur_gate: bfloat16 [32, 64, 64], P('tp'), may hold values from -0.75 to 0.75
- input_gate: bfloat16 [32, 64, 64], P('tp'), may hold values from -0.75 to 0.75
- decay_logit: float32 [2048], P('tp'), may hold values from 1.5 to 8
- output_weight: bfloat16 [2048, 2048], P('tp', 'ep'), may hold values from -0.25 to 0.25
- second_gain: float32 [2048], P('tp'), may hold values from 0.1 to 1.9
- routes: int32 [2048, 2], P('ep'), may hold values from 0 to 31, all different within a row; in each aligned block of 16 rows (0 to 15, 16 to 31, ...) at most 2 rows name the same one
- route_weight: float32 [2048, 2], P('ep'), may hold values from 0.25 to 1
- expert_gate: bfloat16 [2048, 98304], P(None, ('ep', 'tp')), may hold values from -0.125 to 0.125
- expert_up: bfloat16 [2048, 98304], P(None, ('ep', 'tp')), may hold values from -0.125 to 0.125
- expert_down: bfloat16 [98304, 2048], P(('ep', 'tp')), may hold values from -0.21875 to 0.21875
Outputs:
- new_stream: bfloat16 [2048, 2048], P('ep', 'tp')
- new_hidden: float32 [2048, 2048], P('ep', 'tp')
- new_conv: bfloat16 [2048, 3, 2048], P('ep', None, 'tp')
The draws below stay inside these ranges and needn't reach their ends.
Inputs may be any that keep to these rules, and one draw needn't show every extreme that they name: `routes`: among the rows of one index of ep, no expert is named more than 2 times; in every draw some expert is named exactly 2 times by the rows of some index. Each row names different experts.
All inputs are finite; a program needn't handle non-finite values.
Results may differ from the reference program's by a relative error of at most 0.022.
Values may be sent and summed in bfloat16 or wider, within the bound.
A program may use at most 128 MiB of HBM per device.

```python
import math
import jax
import jax.numpy as jnp
import numpy as np
from jax import lax

D = 2048
F = 3072
BLOCK = 64
CONV_W = 4
TOPK = 2
SEQ_DEV = 16
SEQS = 2048
HEADS = 32
EXPERTS = 32
CAP = 2
N_EP = 128


def levels(key, shape, cuts, smallest, largest):
    gain = 1.0
    for axis_at, shards_of in cuts:
        draws = jax.random.uniform(jax.random.fold_in(jax.random.fold_in(key, 6), axis_at), (shards_of,), jnp.float32, smallest / len(cuts), largest / len(cuts))
        gain = gain * jnp.repeat(jnp.exp(draws), shape[axis_at] // shards_of).reshape((-1,) + (1,) * (len(shape) - 1 - axis_at))
    return gain


def assign_block(key, own, number, rows, amount, top, bound, skew):
    sequence = jax.random.permutation(key, amount)
    packed, common = load_shares(amount, rows * top, bound, skew, True), load_shares(amount, rows * top, bound, skew, False)
    places = jnp.arange(amount)

    def named(lengths, offset_by):
        used = int((lengths > 0).sum())
        fixed = max(1, used // 4)
        shifted = fixed + (places - fixed + offset_by * (used - fixed)) % max(1, amount - fixed)
        return jnp.zeros((amount,), jnp.int32).at[sequence[jnp.where(places < fixed, places, shifted)]].set(jnp.asarray(lengths, jnp.int32))

    lengths = jnp.where(number % 4 == 0, named(packed, number // 4), named(common, number - number // 4 - 1))
    mixed = jax.random.permutation(jax.random.fold_in(own, 3), amount)
    donor, sink = mixed[0:amount // 2 * 2:2], mixed[1:amount // 2 * 2:2]
    margin = jnp.minimum(lengths[donor] - 1, bound - lengths[sink]) // 2
    margin = jnp.where((donor == sequence[0]) | (sink == sequence[0]) | (lengths[sink] == 0), 0, jnp.maximum(margin, 0))
    shifted = jax.random.randint(jax.random.fold_in(own, 4), (amount // 2,), 0, 1 << 20) % (margin + 1)
    lengths = lengths.at[donor].add(-shifted).at[sink].add(shifted)
    members = jnp.searchsorted(jnp.cumsum(lengths), jnp.arange(rows * top), side="right").astype(jnp.int32)
    grid = members.reshape(top, rows).T
    grid = grid[jax.random.permutation(jax.random.fold_in(own, 1), rows)]
    offset_by = jax.random.randint(jax.random.fold_in(own, 2), (rows, 1), 0, top)
    return jnp.take_along_axis(grid, (jnp.arange(top)[None, :] + offset_by) % top, axis=1)


def load_shares(count, total, bound, skew, full):
    loads = [(1 << 20) // math.isqrt(standing ** skew) + 1 for standing in range(1, count + 1)]
    largest = bound if full else min(bound, max(-(-total // count), total * loads[0] // sum(loads)))
    least = 1 if total - largest >= count - 1 else 0
    counts, surplus = [largest] + [least] * (count - 1), total - largest - least * (count - 1)
    while surplus > 0:
        movable = [i for i in range(1, count) if counts[i] < largest] or [i for i in range(1, count) if counts[i] < bound]
        mass, remaining = sum([loads[i] for i in movable]), surplus
        for i in movable:
            more = min(bound - counts[i], max(1, remaining * loads[i] // mass), surplus)
            counts[i] = counts[i] + more
            surplus = surplus - more
    return np.array(counts)


def normal_values(own_key, shape, width, reach, cuts=(), kind=jnp.bfloat16):
    values = width * jax.random.normal(own_key, shape, jnp.float32)
    if cuts:
        values = values * levels(own_key, shape, cuts, -0.22, 0.18)
    return jnp.clip(values, -reach, reach).astype(kind)


def setup_inputs(seed: int = 0) -> dict:
    arg_keys = jax.random.split(jax.random.key(seed), 18)
    stream = normal_values(arg_keys[0], (SEQS, D), 1.0, 6.0, ((0, 128), (1, 2)))
    hidden_state = normal_values(arg_keys[1], (SEQS, D), 1.0, 6.0, ((0, 128), (1, 2)), jnp.float32)
    conv_state = normal_values(arg_keys[2], (SEQS, CONV_W - 1, D), 1.0, 6.0, ((0, 128), (2, 2)))
    first_gain = jnp.clip(1.0 + 0.18 * jax.random.normal(arg_keys[3], (D,), jnp.float32), 0.1, 1.9)
    input_weight = normal_values(arg_keys[4], (D, D), D ** -0.5, 0.125, ((0, 2), (1, 128)))
    branch_weight = normal_values(arg_keys[5], (D, D), D ** -0.5, 0.125, ((0, 2), (1, 128)))
    conv_taps = normal_values(arg_keys[6], (CONV_W, D), 0.5, 3.0, ((1, 2),))
    recur_gate = normal_values(arg_keys[7], (HEADS, BLOCK, BLOCK), BLOCK ** -0.5, 0.75, ((0, 2),))
    input_gate = normal_values(arg_keys[8], (HEADS, BLOCK, BLOCK), BLOCK ** -0.5, 0.75, ((0, 2),))
    decay_logit = jnp.clip(1.5 + 6.5 * jax.random.uniform(arg_keys[9], (D,), jnp.float32) ** levels(arg_keys[9], (D,), ((0, 2),), -0.2, 0.2), 1.5, 8.0)
    output_weight = normal_values(arg_keys[10], (D, D), (D // 4) ** -0.5, 0.25, ((0, 2), (1, 128)))
    second_gain = jnp.clip(1.0 + 0.18 * jax.random.normal(arg_keys[11], (D,), jnp.float32), 0.1, 1.9)
    routes_keys = jax.random.split(jax.random.fold_in(arg_keys[12], 1), SEQS // SEQ_DEV)
    routes_turns = jax.random.permutation(jax.random.fold_in(arg_keys[12], 3), SEQS // SEQ_DEV)
    routes = jax.vmap(lambda own, number: assign_block(jax.random.fold_in(arg_keys[12], 2), own, number, SEQ_DEV, EXPERTS, TOPK, CAP, 1))(routes_keys, routes_turns).reshape((SEQS, TOPK))
    route_weight = jnp.clip(0.25 + 0.75 * jax.random.uniform(arg_keys[13], (SEQS, TOPK), jnp.float32) ** levels(arg_keys[13], (SEQS, TOPK), ((0, 128),), -0.2, 0.2), 0.25, 1.0)
    expert_gate = normal_values(arg_keys[14], (D, EXPERTS * F), D ** -0.5, 0.125, ((1, 256),))
    expert_up = normal_values(arg_keys[15], (D, EXPERTS * F), D ** -0.5, 0.125, ((1, 256),))
    expert_down = normal_values(arg_keys[16], (EXPERTS * F, D), (F // 4) ** -0.5, 0.21875, ((0, 256),))
    return {"stream": stream, "hidden_state": hidden_state, "conv_state": conv_state, "first_gain": first_gain, "input_weight": input_weight, "branch_weight": branch_weight, "conv_taps": conv_taps, "recur_gate": recur_gate, "input_gate": input_gate, "decay_logit": decay_logit, "output_weight": output_weight, "second_gain": second_gain, "routes": routes, "route_weight": route_weight, "expert_gate": expert_gate, "expert_up": expert_up, "expert_down": expert_down}


epsilon = 1e-06
decay_power = 8.0

def block_map(values, table):
    split = values.astype(jnp.float32).reshape(SEQS, HEADS, BLOCK)
    mapped = jnp.einsum('shi,hij->shj', split, table.astype(jnp.float32))
    return mapped.reshape(SEQS, D)

def reference(stream, hidden_state, conv_state, first_gain, input_weight, branch_weight, conv_taps, recur_gate, input_gate, decay_logit, output_weight, second_gain, routes, route_weight, expert_gate, expert_up, expert_down):
    values = stream.astype(jnp.float32)
    first_power = lax.optimization_barrier(jnp.mean(values * values, axis=1, keepdims=True))
    row_scale = lax.rsqrt(first_power + epsilon)
    scaled = (values * first_gain).astype(jnp.bfloat16)
    forward = (jnp.dot(scaled, input_weight, preferred_element_type=jnp.float32) * row_scale).astype(jnp.bfloat16)
    branch = (jnp.dot(scaled, branch_weight, preferred_element_type=jnp.float32) * row_scale).astype(jnp.bfloat16)
    window = jnp.concatenate([conv_state, forward[:, None, :]], axis=1)
    new_conv = window[:, 1:]
    conv_out = jnp.einsum('skc,kc->sc', window.astype(jnp.float32), conv_taps.astype(jnp.float32)).astype(jnp.bfloat16)
    recur_open = jax.nn.sigmoid(block_map(conv_out, recur_gate))
    inward = jax.nn.sigmoid(block_map(conv_out, input_gate))
    log_decay = -decay_power * recur_open * jax.nn.softplus(-decay_logit)
    new_hidden = jnp.exp(log_decay) * hidden_state + jnp.sqrt(-jnp.expm1(2.0 * log_decay)) * (inward * conv_out.astype(jnp.float32))
    mixed = (jax.nn.gelu(branch.astype(jnp.float32)) * new_hidden).astype(jnp.bfloat16)
    middle = (values + jnp.dot(mixed, output_weight, preferred_element_type=jnp.float32)).astype(jnp.bfloat16)
    mid_values = middle.astype(jnp.float32)
    second_power = lax.optimization_barrier(jnp.mean(mid_values * mid_values, axis=1, keepdims=True))
    normed = (mid_values * lax.rsqrt(second_power + epsilon) * second_gain).astype(jnp.bfloat16)
    row_bound = CAP * N_EP

    def one_expert(carry_terms, expert_index):
        chosen = routes == expert_index
        weight = lax.optimization_barrier(jnp.sum(jnp.where(chosen, route_weight, 0.0), axis=1))
        routed = jnp.any(chosen, axis=1)
        rows = jnp.nonzero(routed, size=row_bound, fill_value=0)[0].astype(jnp.int32)
        live_rows = jnp.arange(row_bound) < jnp.sum(routed.astype(jnp.int32))
        picked = normed[rows].astype(jnp.float32)
        start = (expert_index * F).astype(jnp.int32)
        gate_cols = lax.dynamic_slice_in_dim(expert_gate, start, F, 1).astype(jnp.float32)
        up_cols = lax.dynamic_slice_in_dim(expert_up, start, F, 1).astype(jnp.float32)
        down_rows = lax.dynamic_slice_in_dim(expert_down, start, F, 0).astype(jnp.float32)
        gate_act = jnp.dot(picked, gate_cols)
        upper = jnp.dot(picked, up_cols)
        inner = lax.optimization_barrier((jax.nn.silu(gate_act) * upper).astype(jnp.bfloat16)).astype(jnp.float32)
        expert_out = jnp.dot(inner, down_rows)
        factor = jnp.where(live_rows, weight[rows], 0.0)
        return (carry_terms.at[rows].add(expert_out * factor[:, None]), None)
    expert_mix, _ = lax.scan(one_expert, jnp.zeros((SEQS, D), jnp.float32), jnp.arange(EXPERTS, dtype=jnp.int32))
    new_stream = (mid_values + expert_mix).astype(jnp.bfloat16)
    return (new_stream, new_hidden, new_conv)
```

```python
import jax
import jax.numpy as jnp
from jax import lax
from jax.experimental import pallas as pl
from jax.experimental.pallas import tpu as pltpu
from jax.sharding import Mesh
from jax.sharding import PartitionSpec as P

EP = ("z", "y", "x")
EP_TP = ("z", "y", "x", "tp")
MESH = pl.DeviceIdType.MESH
NZ, NY, NX = 8, 4, 4
ORDER = {8: (1, 7, 2, 6, 3, 5, 4), 4: (1, 3, 2)}
BF, F32 = jnp.bfloat16, jnp.float32
EPSILON = 1e-6
DECAY_POWER = 8.0
S, H, D, FD = 16, 1024, 2048, 384
LANES, Q = 128, 8
EXPERTS, CAP = 32, 2
HIGHEST = lax.Precision.HIGHEST


def scratch_shapes():
    vm, dma = pltpu.VMEM, pltpu.SemaphoreType.DMA
    return dict(
        sv=vm((S, H), BF),
        hv=vm((S, H), F32),
        cv=vm((3, S, H), BF),
        g1v=vm((1, H), F32),
        tv=vm((4, H), BF),
        rgv=vm((H, 64), BF),
        igv=vm((H, 64), BF),
        dv=vm((1, H), F32),
        g2v=vm((1, H), F32),
        rtv=vm((2, S), jnp.int32),
        rwv=vm((2, S), F32),
        wg=vm((Q, 2, LANES, FD), BF),
        wu=vm((Q, 2, LANES, FD), BF),
        wd=vm((FD, D), BF),
        xs=vm((NZ, S, H), BF),
        ms=vm((NZ, S, H), BF),
        wt=vm((3, 4, 4, S, H), BF),
        ps=vm((NZ * S, 512), BF),
        pr=vm((NZ * S, 512), BF),
        ss=vm((NZ, S, 512), BF),
        ra=vm((4, S, 512), BF),
        ps2=vm((NZ * S, 256), BF),
        pr2=vm((NZ * S, 256), BF),
        ss2=vm((NZ, S, 256), BF),
        rb=vm((4, S, 256), BF),
        qs=vm((2, S, LANES), F32),
        qr=vm((2, S, LANES), F32),
        bd=vm((2, 4, 256, 256), BF),
        pm=vm((EXPERTS * 16, LANES), BF),
        pw=vm((EXPERTS * 16, LANES), F32),
        zsend=vm((NZ, NY, 16, LANES), BF),
        zrecv=vm((NZ, NY, 16, LANES), BF),
        fb=vm((2, NX, NY, NZ, 16, LANES), BF),
        ab=vm((256, D), BF),
        ib=vm((256, FD), BF),
        hs=vm((NX, 64, H), BF),
        hr=vm((NX, 64, H), BF),
        own=vm((NX, 64, H), F32),
        xsend=vm((NX, 64, H), BF),
        xrecv=vm((NX, 64, H), BF),
        ysend=vm((NY, NZ, 16, LANES), BF),
        ry=vm((NY, NZ, 16, LANES), BF),
        rz=vm((NZ, NY, 16, LANES), BF),
        nh=vm((S, H), F32),
        nc=vm((3, S, H), BF),
        ns=vm((S, H), BF),
        loads=dma((24,)),
        stores=dma((3,)),
        x_s=dma((8,)), x_r=dma((8,)),
        m_s=dma((8,)), m_r=dma((8,)),
        w1_s=dma((2, 4)), w1_r=dma((2, 4)),
        w2_s=dma((2, 4)), w2_r=dma((2, 4)),
        t_s=dma((4,)), t_r=dma((4,)),
        a_s=dma((8,)), a_r=dma((4,)),
        b_s=dma((8,)), b_r=dma((4,)),
        dz_s=dma((8,)), dz_r=dma((8,)),
        dy_s=dma((4,)), dy_r=dma((4,)),
        dx_s=dma((4,)), dx_r=dma((4,)),
        dt_s=dma((4,)), dt_r=dma((4,)),
        ht_s=dma((4,)), ht_r=dma((4,)),
        rx_s=dma((4,)), rx_r=dma((4,)),
        ry_s=dma((4,)), ry_r=dma((4,)),
        rz_s=dma((8,)), rz_r=dma((8,)),
    )


NAMES = tuple(scratch_shapes())


def dot(a, b, dims=((1,), (0,)), precision=None):
    return lax.dot_general(a, b, (dims, ((), ())), precision=precision, preferred_element_type=F32)


def iota(shape, dim):
    return lax.broadcasted_iota(jnp.int32, shape, dim)


def expm1(v):
    series = 1.0 + v * (1.0 / 9.0)
    for n in range(8, 1, -1):
        series = 1.0 + v * (1.0 / n) * series
    return jnp.where(v > -0.5, v * series, jnp.exp(v) - 1.0)


def remote(src, dst, ssem, rsem, where):
    return pltpu.make_async_remote_copy(
        src_ref=src, dst_ref=dst, send_sem=ssem, recv_sem=rsem, device_id=where, device_id_type=MESH
    )


def kernel(*refs):
    (stream, hidden, conv, gain1, w_in, w_br, taps, rg, ig, decay, w_out, gain2, routes, rw, eg, eu, ed) = refs[:17]
    o_stream, o_hidden, o_conv = refs[17:20]
    k = dict(zip(NAMES, refs[20:]))
    z, y, x, tp = (lax.axis_index(a) for a in EP_TP)
    other = 1 - tp
    sent = []

    barrier = pltpu.get_barrier_semaphore()
    for axis, me in (("z", z), ("y", y), ("x", x)):
        n = {"z": NZ, "y": NY, "x": NX}[axis]
        for d in ORDER[n]:
            pl.semaphore_signal(barrier, inc=1, device_id={axis: lax.rem(me + d, n)}, device_id_type=MESH)
    pl.semaphore_signal(barrier, inc=1, device_id={"tp": other}, device_id_type=MESH)

    a = y + tp * (x - y)
    b = x + tp * (y - x)
    plan = [
        (stream, k["sv"]), (gain1, k["g1v"]),
        (w_in, k["wt"].at[0, a, b]), (w_br, k["wt"].at[1, a, b]), (w_out, k["wt"].at[2, a, b]),
        (rg, k["rgv"]), (ig, k["igv"]), (routes, k["rtv"]), (rw, k["rwv"]),
        (conv, k["cv"]), (taps, k["tv"]), (decay, k["dv"]), (hidden, k["hv"]), (gain2, k["g2v"]),
        (eg.at[0], k["wg"].at[:, 0]), (eg.at[1], k["wg"].at[:, 1]),
        (eu.at[0], k["wu"].at[:, 0]), (eu.at[1], k["wu"].at[:, 1]), (ed, k["wd"]),
    ]
    loads = [pltpu.make_async_copy(s, t, k["loads"].at[i]) for i, (s, t) in enumerate(plan)]
    for c in loads:
        c.start()

    def start(src, dst, ssem, rsem, where):
        c = remote(src, dst, ssem, rsem, where)
        c.start()
        sent.append(c)

    def await_recv(ref, ssem, rsem, where):
        remote(ref, ref, ssem, rsem, where).wait_recv()

    loads[0].wait()
    loads[1].wait()
    values = k["sv"][...].astype(F32)
    k["xs"][z] = (values * k["g1v"][...]).astype(BF)
    k["qs"][0] = jnp.broadcast_to(jnp.sum(values * values, axis=1, keepdims=True), (S, LANES))
    for i in (2, 3, 4):
        loads[i].wait()
    pl.semaphore_wait(barrier, 14)

    for kinds, n in ((pl.ds(0, 2), 0), (pl.ds(2, 1), 1)):
        for d in ORDER[4]:
            there = {"y": lax.rem(y + d * tp, NY), "x": lax.rem(x + d * other, NX)}
            block = k["wt"].at[kinds, a, b]
            start(block, block, k["w1_s"].at[n, d], k["w1_r"].at[n, d], there)
        if n == 0:
            for d in ORDER[8]:
                start(k["xs"].at[z], k["xs"].at[z], k["x_s"].at[d], k["x_r"].at[d], {"z": lax.rem(z + d, NZ)})
            start(k["qs"].at[0], k["qr"].at[0], k["t_s"].at[0], k["t_r"].at[0], {"tp": other})

    def second_stage(kinds, n):
        for d in ORDER[4]:
            block = k["wt"].at[kinds, a, lax.rem(b - d + 4, 4)]
            await_recv(block, k["w1_s"].at[n, d], k["w1_r"].at[n, d], {"tp": other})
        for d in ORDER[4]:
            there = {"y": lax.rem(y + d * other, NY), "x": lax.rem(x + d * tp, NX)}
            block = k["wt"].at[kinds, a]
            start(block, block, k["w2_s"].at[n, d], k["w2_r"].at[n, d], there)

    def second_arrived(kinds, n):
        for d in ORDER[4]:
            block = k["wt"].at[kinds, lax.rem(a - d + 4, 4)]
            await_recv(block, k["w2_s"].at[n, d], k["w2_r"].at[n, d], {"tp": other})

    second_stage(pl.ds(0, 2), 0)

    loads[5].wait()
    loads[6].wait()
    eye = (iota((64, 256), 1) % 64 == iota((64, 256), 0)).astype(BF)
    on = iota((H, 256), 0) // 64 % 4 == iota((H, 256), 1) // 64
    for n, ref in enumerate((k["rgv"], k["igv"])):
        k["bd"][n] = jnp.where(on, dot(ref[...], eye), 0.0).astype(BF).reshape(4, 256, 256)

    loads[7].wait()
    loads[8].wait()
    spread = (iota((S, LANES), 1) % S == iota((S, LANES), 0)).astype(F32)
    named = dot(k["rtv"][...].astype(F32), spread, precision=HIGHEST)
    weights = dot(k["rwv"][...], spread, precision=HIGHEST)
    rows = (EXPERTS * 16, LANES)
    expert = (iota(rows, 0) // 16).astype(F32)
    hit0, hit1 = named[0:1] == expert, named[1:2] == expert
    hits = jnp.where(hit0 | hit1, 1.0, 0.0)
    square = (LANES, LANES)
    before = (iota(square, 0) < iota(square, 1) % S).astype(BF)
    rank = dot(hits.astype(BF), before)
    slot = (iota(rows, 0) // Q % CAP).astype(F32)
    chosen = (hits > 0.5) & (rank == slot) & (iota(rows, 0) % Q == iota(rows, 1) // S)
    k["pm"][...] = jnp.where(chosen, 1.0, 0.0).astype(BF)
    k["pw"][...] = jnp.where(chosen, jnp.where(hit0, weights[0:1], weights[1:2]), 0.0)

    second_stage(pl.ds(2, 1), 1)
    for d in ORDER[8]:
        await_recv(k["xs"].at[lax.rem(z - d + NZ, NZ)], k["x_s"].at[d], k["x_r"].at[d], {"tp": other})
    second_arrived(pl.ds(0, 2), 0)

    def columns(kind):
        blocks = []
        for i in range(4):
            for j in range(4):
                blocks.append(k["wt"][kind, i + tp * (j - i), j + tp * (i - j)])
        return jnp.concatenate(blocks, axis=0)

    def project(rows_ref, kinds, width, ps, pr, ss, land, t, sends, lands):
        lhs = k[rows_ref][...].reshape(NZ * S, H)
        part = jnp.concatenate([dot(lhs, columns(kind), ((1,), (1,))) for kind in kinds], axis=1)

        @pl.when(tp != z // 4)
        def _():
            k[ps][...] = part.astype(BF)
            c = remote(k[ps], k[pr], k["t_s"].at[t], k["t_r"].at[t], {"tp": other})
            c.start()
            c.wait_send()

        @pl.when(tp == z // 4)
        def _():
            await_recv(k[pr], k["t_s"].at[t], k["t_r"].at[t], {"tp": other})
            total = (part + k[pr][...].astype(F32)).astype(BF)
            k[ss][...] = total.reshape(NZ, S, width)
            mine = lax.rem(z, 4)
            for d in ORDER[8]:
                there = lax.rem(z + d, NZ)
                remote(k[ss].at[there], k[land].at[mine], k[sends].at[d], k[lands].at[mine], {"z": there}).start()
            k[land][mine] = k[ss][z]

        for i in range(4):
            @pl.when(4 * tp + i != z)
            def _():
                await_recv(k[land].at[i], k[sends].at[0], k[lands].at[i], {"tp": other})

    def sends_done(ss, land, sends, lands):
        @pl.when(tp == z // 4)
        def _():
            for d in ORDER[8]:
                remote(k[ss].at[0], k[land].at[0], k[sends].at[d], k[lands].at[0], {"tp": other}).wait_send()

    project("xs", (0, 1), 512, "ps", "pr", "ss", "ra", 1, "a_s", "a_r")
    await_recv(k["qr"].at[0], k["t_s"].at[0], k["t_r"].at[0], {"tp": other})
    row_scale = lax.rsqrt((k["qs"][0] + k["qr"][0])[:, 0:1] / D + EPSILON)
    forward = (jnp.concatenate([k["ra"][i, :, 0:256] for i in range(4)], axis=1).astype(F32) * row_scale).astype(BF)
    branch = (jnp.concatenate([k["ra"][i, :, 256:512] for i in range(4)], axis=1).astype(F32) * row_scale).astype(BF)
    for i in range(9, 14):
        loads[i].wait()
    window = [k["cv"][0], k["cv"][1], k["cv"][2], forward]
    k["nc"][0] = window[1]
    k["nc"][1] = window[2]
    k["nc"][2] = forward
    store_conv = pltpu.make_async_copy(k["nc"], o_conv, k["stores"].at[0])
    store_conv.start()
    tap_rows = k["tv"][...].astype(F32)
    conv_out = sum(window[i].astype(F32) * tap_rows[i : i + 1] for i in range(4)).astype(BF)

    def gate_map(n):
        return jnp.concatenate([dot(conv_out[:, g * 256 : g * 256 + 256], k["bd"][n, g]) for g in range(4)], axis=1)

    recur_open = jax.nn.sigmoid(gate_map(0))
    inward = jax.nn.sigmoid(gate_map(1))
    logit = -k["dv"][...]
    softplus = jnp.maximum(logit, 0.0) + jnp.log1p(jnp.exp(-jnp.abs(logit)))
    log_decay = -DECAY_POWER * recur_open * softplus
    new_hidden = jnp.exp(log_decay) * k["hv"][...] + jnp.sqrt(-expm1(2.0 * log_decay)) * (
        inward * conv_out.astype(F32)
    )
    k["nh"][...] = new_hidden
    store_hidden = pltpu.make_async_copy(k["nh"], o_hidden, k["stores"].at[1])
    store_hidden.start()
    k["ms"][z] = (jax.nn.gelu(branch.astype(F32)) * new_hidden).astype(BF)
    for d in ORDER[8]:
        start(k["ms"].at[z], k["ms"].at[z], k["m_s"].at[d], k["m_r"].at[d], {"z": lax.rem(z + d, NZ)})
    second_arrived(pl.ds(2, 1), 1)
    for d in ORDER[8]:
        await_recv(k["ms"].at[lax.rem(z - d + NZ, NZ)], k["m_s"].at[d], k["m_r"].at[d], {"tp": other})
    project("ms", (2,), 256, "ps2", "pr2", "ss2", "rb", 2, "b_s", "b_r")
    out_terms = jnp.concatenate([k["rb"][i] for i in range(4)], axis=1).astype(F32)
    middle = (values + out_terms).astype(BF)
    mid_values = middle.astype(F32)
    k["qs"][1] = jnp.broadcast_to(jnp.sum(mid_values * mid_values, axis=1, keepdims=True), (S, LANES))
    start(k["qs"].at[1], k["qr"].at[1], k["t_s"].at[3], k["t_r"].at[3], {"tp": other})
    await_recv(k["qr"].at[1], k["t_s"].at[3], k["t_r"].at[3], {"tp": other})
    mid_scale = lax.rsqrt((k["qs"][1] + k["qr"][1])[:, 0:1] / D + EPSILON)
    normed = (mid_values * mid_scale * k["g2v"][...]).astype(BF)

    stacked = jnp.concatenate([normed[:, q * LANES : (q + 1) * LANES] for q in range(Q)], axis=0)
    k["zsend"][...] = dot(k["pm"][...], stacked).astype(BF).reshape(NZ, NY, 16, LANES)
    for d in ORDER[8]:
        there = lax.rem(z + d, NZ)
        start(k["zsend"].at[there], k["zrecv"].at[z], k["dz_s"].at[d], k["dz_r"].at[d], {"z": there})
    k["zrecv"][z] = k["zsend"][z]
    for d in ORDER[8]:
        await_recv(k["zrecv"].at[lax.rem(z - d + NZ, NZ)], k["dz_s"].at[d], k["dz_r"].at[d], {"tp": other})
    for d in ORDER[4]:
        there = lax.rem(y + d, NY)
        start(k["zrecv"].at[:, there], k["fb"].at[tp, x, y], k["dy_s"].at[d], k["dy_r"].at[d], {"y": there})
    k["fb"][tp, x, y] = k["zrecv"][:, y]
    for d in ORDER[4]:
        block = k["fb"].at[tp, x, lax.rem(y - d + NY, NY)]
        await_recv(block, k["dy_s"].at[d], k["dy_r"].at[d], {"tp": other})
    for d in ORDER[4]:
        there = lax.rem(x + d, NX)
        start(k["fb"].at[tp, x], k["fb"].at[tp, x], k["dx_s"].at[d], k["dx_r"].at[d], {"x": there})
    for d in (0,) + ORDER[4]:
        block = k["fb"].at[tp, lax.rem(x - d + NX, NX)]
        if d:
            await_recv(block, k["dx_s"].at[d], k["dx_r"].at[d], {"tp": other})
        start(block, block, k["dt_s"].at[d], k["dt_r"].at[d], {"tp": other})
    for i in range(14, 19):
        loads[i].wait()
    for d in (0,) + ORDER[4]:
        block = k["fb"].at[other, lax.rem(x - d + NX, NX)]
        await_recv(block, k["dt_s"].at[d], k["dt_r"].at[d], {"tp": other})

    turn = iota(square, 1) == iota(square, 0) % 16 * Q + iota(square, 0) // 16
    turn = jnp.where(turn, 1.0, 0.0).astype(BF)
    for g in range(NX * NY):
        pair = jnp.concatenate([k["fb"][h, g // NY, g % NY].reshape(LANES, LANES) for h in range(2)], axis=1)
        turned = dot(turn, pair).astype(BF)
        for q in range(Q):
            k["ab"][g * 16 : g * 16 + 16, q * 256 : q * 256 + 256] = turned[q * 16 : q * 16 + 16]
    gate_act = dot(k["ab"][...], k["wg"][...].reshape(D, FD))
    upper = dot(k["ab"][...], k["wu"][...].reshape(D, FD))
    k["ib"][...] = (jax.nn.silu(gate_act) * upper).astype(BF)

    for d in ORDER[4] + (0,):
        there = lax.rem(x + d, NX)
        inner = k["ib"][pl.ds(pl.multiple_of(there * 64, 64), 64)]
        theirs = pl.ds(pl.multiple_of(other * H, H), H)
        ours = pl.ds(pl.multiple_of(tp * H, H), H)
        k["hs"][there] = dot(inner, k["wd"][:, theirs]).astype(BF)
        start(k["hs"].at[there], k["hr"].at[there], k["ht_s"].at[d], k["ht_r"].at[d], {"tp": other})
        k["own"][there] = dot(inner, k["wd"][:, ours])
    for d in ORDER[4] + (0,):
        there = lax.rem(x + d, NX)
        await_recv(k["hr"].at[there], k["ht_s"].at[d], k["ht_r"].at[d], {"tp": other})
        whole = k["own"][there] + k["hr"][there].astype(F32)
        if d:
            k["xsend"][there] = whole.astype(BF)
            start(k["xsend"].at[there], k["xrecv"].at[x], k["rx_s"].at[d], k["rx_r"].at[d], {"x": there})
    for d in ORDER[4]:
        source = lax.rem(x - d + NX, NX)
        await_recv(k["xrecv"].at[source], k["rx_s"].at[d], k["rx_r"].at[d], {"tp": other})
        whole = whole + k["xrecv"][source].astype(F32)
    whole = whole.astype(BF)
    back = iota(square, 0) == iota(square, 1) % 16 * Q + iota(square, 1) // 16
    back = jnp.where(back, 1.0, 0.0).astype(BF)
    for g in range(NY):
        part = whole[g * 16 : g * 16 + 16]
        part = jnp.concatenate([part[:, q * LANES : (q + 1) * LANES] for q in range(Q)], axis=0)
        k["ysend"][g] = dot(back, part).astype(BF).reshape(NZ, 16, LANES)
    for d in ORDER[4]:
        there = lax.rem(y + d, NY)
        start(k["ysend"].at[there], k["ry"].at[y], k["ry_s"].at[d], k["ry_r"].at[d], {"y": there})
    k["ry"][y] = k["ysend"][y]
    for d in ORDER[4]:
        await_recv(k["ry"].at[lax.rem(y - d + NY, NY)], k["ry_s"].at[d], k["ry_r"].at[d], {"tp": other})
    for d in ORDER[8]:
        there = lax.rem(z + d, NZ)
        start(k["ry"].at[:, there], k["rz"].at[z], k["rz_s"].at[d], k["rz_r"].at[d], {"z": there})
    k["rz"][z] = k["ry"][:, z]
    for d in ORDER[8]:
        await_recv(k["rz"].at[lax.rem(z - d + NZ, NZ)], k["rz_s"].at[d], k["rz_r"].at[d], {"tp": other})
    returned = k["rz"][...].reshape(EXPERTS * 16, LANES).astype(F32)
    mix = dot(k["pw"][...], returned, ((0,), (0,)), HIGHEST)
    expert_mix = jnp.concatenate([mix[q * S : (q + 1) * S] for q in range(Q)], axis=1)
    k["ns"][...] = (mid_values + expert_mix).astype(BF)
    store_stream = pltpu.make_async_copy(k["ns"], o_stream, k["stores"].at[2])
    store_stream.start()

    for c in sent:
        c.wait_send()
    sends_done("ss", "ra", "a_s", "a_r")
    sends_done("ss2", "rb", "b_s", "b_r")
    store_conv.wait()
    store_hidden.wait()
    store_stream.wait()


def per_device(
    stream, hidden_state, conv_state, first_gain, input_weight, branch_weight, conv_taps, recur_gate, input_gate,
    decay_logit, output_weight, second_gain, routes, route_weight, expert_gate, expert_up, expert_down,
):
    shapes = scratch_shapes()
    anywhere = pl.BlockSpec(memory_space=pl.ANY)
    outs = pl.pallas_call(
        kernel,
        name="layer",
        out_shape=(
            jax.ShapeDtypeStruct((S, H), BF),
            jax.ShapeDtypeStruct((S, H), F32),
            jax.ShapeDtypeStruct((3, S, H), BF),
        ),
        in_specs=[anywhere] * 17,
        out_specs=(anywhere,) * 3,
        scratch_shapes=[shapes[n] for n in NAMES],
        compiler_params=pltpu.CompilerParams(
            collective_id=0, has_side_effects=True, vmem_limit_bytes=60 * 1024 * 1024
        ),
    )(
        stream,
        hidden_state,
        conv_state.transpose(1, 0, 2),
        first_gain.reshape(1, H),
        input_weight.T,
        branch_weight.T,
        conv_taps,
        recur_gate.reshape(H, 64),
        input_gate.reshape(H, 64),
        decay_logit.reshape(1, H),
        output_weight.T,
        second_gain.reshape(1, H),
        routes.T,
        route_weight.T,
        expert_gate.reshape(2, Q, LANES, FD),
        expert_up.reshape(2, Q, LANES, FD),
        expert_down,
    )
    new_stream, new_hidden, new_conv = outs
    return new_stream, new_hidden, new_conv.transpose(1, 0, 2)


def solution(mesh):
    torus = Mesh(mesh.devices.reshape(NZ, NY, NX, mesh.shape["tp"]), EP_TP)
    in_specs = (
        P(EP, "tp"),
        P(EP, "tp"),
        P(EP, None, "tp"),
        P("tp"),
        P("tp", EP),
        P("tp", EP),
        P(None, "tp"),
        P("tp", None, None),
        P("tp", None, None),
        P("tp"),
        P("tp", EP),
        P("tp"),
        P(EP, None),
        P(EP, None),
        P(None, EP_TP),
        P(None, EP_TP),
        P(EP_TP, None),
    )
    out_specs = (P(EP, "tp"), P(EP, "tp"), P(EP, None, "tp"))
    return jax.shard_map(per_device, mesh=torus, in_specs=in_specs, out_specs=out_specs, check_vma=False)
```

```python
import jax
import jax.numpy as jnp
from jax import lax
from jax.experimental import pallas as pl
from jax.experimental.pallas import tpu as pltpu
from jax.sharding import Mesh
from jax.sharding import PartitionSpec as P

EP = ("z", "y", "x")
EP_TP = ("z", "y", "x", "tp")
MESH = pl.DeviceIdType.MESH
NZ, NY, NX = 8, 4, 4
ORDER = {8: (1, 7, 2, 6, 3, 5, 4), 4: (1, 3, 2)}
ZORD, XORD = (0,) + ORDER[8], (0,) + ORDER[4]
GROUPS = ((0, 5), (5, 3))
BF, F32 = jnp.bfloat16, jnp.float32
EPSILON = 1e-6
DECAY_POWER = 8.0
S, H, D, FD = 16, 1024, 2048, 384
LANES, Q = 128, 8
EXPERTS, CAP = 32, 2
HIGHEST = lax.Precision.HIGHEST


def scratch_shapes():
    vm, dma = pltpu.VMEM, pltpu.SemaphoreType.DMA
    return dict(
        sv=vm((S, H), BF),
        hv=vm((S, H), F32),
        cv=vm((3, S, H), BF),
        g1v=vm((1, H), F32),
        tv=vm((4, H), BF),
        rgv=vm((H, 64), BF),
        igv=vm((H, 64), BF),
        dv=vm((1, H), F32),
        g2v=vm((1, H), F32),
        rtv=vm((2, S), jnp.int32),
        rwv=vm((2, S), F32),
        wg=vm((Q, 2, LANES, FD), BF),
        wu=vm((Q, 2, LANES, FD), BF),
        wd=vm((FD, D), BF),
        xs=vm((NZ, S, H), BF),
        ms=vm((NY, S, H), BF),
        wt=vm((2, 4, 4, S, H), BF),
        wo=vm((NX, NZ, S, H), BF),
        ps=vm((NZ * S, 512), BF),
        pr=vm((NZ * S, 512), BF),
        ss=vm((NZ, S, 512), BF),
        ra=vm((4, S, 512), BF),
        po=vm((2, NY * S, 256), F32),
        ps2=vm((2, NY * S, 256), BF),
        pr2=vm((NY * S, 256), BF),
        ss2=vm((NY, S, 256), BF),
        rb=vm((NY, S, 256), BF),
        qs=vm((2, S, LANES), F32),
        qr=vm((2, S, LANES), F32),
        bd=vm((2, 4, 256, 256), BF),
        pm=vm((EXPERTS * 16, LANES), BF),
        pw=vm((EXPERTS * 16, LANES), F32),
        zsend=vm((NZ, NY, 16, LANES), BF),
        zrecv=vm((NZ, NY, 16, LANES), BF),
        fb=vm((2, NX, NY, NZ, 16, LANES), BF),
        ab=vm((256, D), BF),
        ib=vm((256, FD), BF),
        hs=vm((NX, 64, H), BF),
        hr=vm((NX, 64, H), BF),
        own=vm((NX, 64, H), F32),
        xsend=vm((NX, 2, 32, H), BF),
        rl=vm((2, 32, H), BF),
        xrecv=vm((2, 2, 32, H), BF),
        ysend=vm((NY, NZ, 16, LANES), BF),
        ry=vm((NY, NZ, 16, LANES), BF),
        rz=vm((NZ, NY, 16, LANES), BF),
        nh=vm((S, H), F32),
        nc=vm((3, S, H), BF),
        ns=vm((S, H), BF),
        loads=dma((24,)),
        stores=dma((3,)),
        x_s=dma((8,)), x_r=dma((8,)),
        m_s=dma((8,)), m_r=dma((8,)),
        w_s=dma((16,)), w_r=dma((16,)),
        oz_s=dma((8,)), oz_r=dma((8,)),
        ox_s=dma((4,)), ox_r=dma((4,)),
        t_s=dma((4,)), t_r=dma((4,)),
        a_s=dma((8,)), a_r=dma((4,)),
        b_s=dma((4,)), b_r=dma((4,)),
        dz_s=dma((8,)), dz_r=dma((8,)),
        dy_s=dma((2, 4)), dy_r=dma((2, 4)),
        dx_s=dma((2, 4, 2)), dx_r=dma((2, 4, 2)),
        dl_s=dma((2, 4)), dl_r=dma((2, 4)),
        dt_s=dma((4, 2)), dt_r=dma((4, 2)),
        ht_s=dma((4,)), ht_r=dma((4,)),
        rl_s=dma((2,)), rl_r=dma((2,)),
        rx_s=dma((2, 2)), rx_r=dma((2, 2)),
        ry_s=dma((4,)), ry_r=dma((4,)),
        rz_s=dma((2, 8)), rz_r=dma((2, 8)),
    )


NAMES = tuple(scratch_shapes())


def dot(a, b, dims=((1,), (0,)), precision=None):
    return lax.dot_general(a, b, (dims, ((), ())), precision=precision, preferred_element_type=F32)


def iota(shape, dim):
    return lax.broadcasted_iota(jnp.int32, shape, dim)


def expm1(v):
    series = 1.0 + v * (1.0 / 9.0)
    for n in range(8, 1, -1):
        series = 1.0 + v * (1.0 / n) * series
    return jnp.where(v > -0.5, v * series, jnp.exp(v) - 1.0)


def remote(src, dst, ssem, rsem, where):
    return pltpu.make_async_remote_copy(
        src_ref=src, dst_ref=dst, send_sem=ssem, recv_sem=rsem, device_id=where, device_id_type=MESH
    )


def kernel(*refs):
    (stream, hidden, conv, gain1, w_in, w_br, taps, rg, ig, decay, w_out, gain2, routes, rw, eg, eu, ed) = refs[:17]
    o_stream, o_hidden, o_conv = refs[17:20]
    k = dict(zip(NAMES, refs[20:]))
    z, y, x, tp = (lax.axis_index(a) for a in EP_TP)
    other = 1 - tp
    sent = []

    barrier = pltpu.get_barrier_semaphore()
    for axis, me in (("z", z), ("y", y), ("x", x)):
        n = {"z": NZ, "y": NY, "x": NX}[axis]
        for d in ORDER[n]:
            pl.semaphore_signal(barrier, inc=1, device_id={axis: lax.rem(me + d, n)}, device_id_type=MESH)
    pl.semaphore_signal(barrier, inc=1, device_id={"tp": other}, device_id_type=MESH)

    a = y + tp * (x - y)
    b = x + tp * (y - x)
    plan = [
        (stream, k["sv"]), (gain1, k["g1v"]),
        (w_in, k["wt"].at[0, a, b]), (w_br, k["wt"].at[1, a, b]), (w_out, k["wo"].at[x, z]),
        (rg, k["rgv"]), (ig, k["igv"]), (routes, k["rtv"]), (rw, k["rwv"]),
        (conv, k["cv"]), (taps, k["tv"]), (decay, k["dv"]), (hidden, k["hv"]), (gain2, k["g2v"]),
        (eg.at[0], k["wg"].at[:, 0]), (eg.at[1], k["wg"].at[:, 1]),
        (eu.at[0], k["wu"].at[:, 0]), (eu.at[1], k["wu"].at[:, 1]), (ed, k["wd"]),
    ]
    loads = [pltpu.make_async_copy(s, t, k["loads"].at[i]) for i, (s, t) in enumerate(plan)]
    for c in loads:
        c.start()

    def start(src, dst, ssem, rsem, where):
        c = remote(src, dst, ssem, rsem, where)
        c.start()
        sent.append(c)

    def await_recv(ref, ssem, rsem, where):
        remote(ref, ref, ssem, rsem, where).wait_recv()

    loads[0].wait()
    loads[1].wait()
    values = k["sv"][...].astype(F32)
    k["xs"][z] = (values * k["g1v"][...]).astype(BF)
    k["qs"][0] = jnp.broadcast_to(jnp.sum(values * values, axis=1, keepdims=True), (S, LANES))
    for i in (2, 3, 4):
        loads[i].wait()
    pl.semaphore_wait(barrier, 14)

    def along_b(d):
        return {"y": lax.rem(y + d * tp, NY), "x": lax.rem(x + d * other, NX)}

    def along_a(d):
        return {"y": lax.rem(y + d * other, NY), "x": lax.rem(x + d * tp, NX)}

    both = pl.ds(0, 2)

    def block(da, db, kinds=both):
        return k["wt"].at[kinds, lax.rem(a - da + 4, 4), lax.rem(b - db + 4, 4)]

    def push(ref, i, where):
        start(ref, ref, k["w_s"].at[i], k["w_r"].at[i], where)

    def pull(ref, i):
        await_recv(ref, k["w_s"].at[i], k["w_r"].at[i], {"tp": other})

    def push_a(i):
        push(block(0, XORD[i]), 4 + 2 * i, along_a(1))
        push(block(0, XORD[i]), 5 + 2 * i, along_a(3))

    push(block(0, 0), 0, along_b(1))
    push(block(0, 0), 1, along_b(3))
    push_a(0)
    for d in ORDER[8]:
        start(k["xs"].at[z], k["xs"].at[z], k["x_s"].at[d], k["x_r"].at[d], {"z": lax.rem(z + d, NZ)})
    start(k["qs"].at[0], k["qr"].at[0], k["t_s"].at[0], k["t_r"].at[0], {"tp": other})
    for d in ORDER[8]:
        mine = k["wo"].at[x, z]
        start(mine, mine, k["oz_s"].at[d], k["oz_r"].at[d], {"z": lax.rem(z + d, NZ)})
    first, second = pl.ds(0, 1), pl.ds(1, 1)
    with jax.named_scope("w_b"):
        pull(block(0, 1), 0)
        push(block(0, 1, first), 2, along_b(1))
        push_a(1)
        pull(block(0, 3), 1)
        push(block(0, 3, second), 3, along_b(3))
        push_a(2)
    with jax.named_scope("w_a0"):
        pull(block(1, 0), 4)
        push(block(1, 0), 12, along_a(1))
    with jax.named_scope("w_b2"):
        pull(block(0, 2, first), 2)
        pull(block(0, 2, second), 3)
        push_a(3)
    with jax.named_scope("w_a1"):
        pull(block(1, 1), 6)
        push(block(1, 1), 13, along_a(1))
        pull(block(3, 3), 9)
        push(block(3, 3), 14, along_a(3))

    loads[5].wait()
    loads[6].wait()
    eye = (iota((64, 256), 1) % 64 == iota((64, 256), 0)).astype(BF)
    on = iota((H, 256), 0) // 64 % 4 == iota((H, 256), 1) // 64
    for n, ref in enumerate((k["rgv"], k["igv"])):
        k["bd"][n] = jnp.where(on, dot(ref[...], eye), 0.0).astype(BF).reshape(4, 256, 256)

    loads[7].wait()
    loads[8].wait()
    spread = (iota((S, LANES), 1) % S == iota((S, LANES), 0)).astype(F32)
    named = dot(k["rtv"][...].astype(F32), spread, precision=HIGHEST)
    weights = dot(k["rwv"][...], spread, precision=HIGHEST)
    rows = (EXPERTS * 16, LANES)
    expert = (iota(rows, 0) // 16).astype(F32)
    hit0, hit1 = named[0:1] == expert, named[1:2] == expert
    hits = jnp.where(hit0 | hit1, 1.0, 0.0)
    square = (LANES, LANES)
    before = (iota(square, 0) < iota(square, 1) % S).astype(BF)
    rank = dot(hits.astype(BF), before)
    slot = (iota(rows, 0) // Q % CAP).astype(F32)
    same = iota(rows, 0) % Q == iota(rows, 1) // S
    chosen = (hits > 0.5) & (rank == slot) & same
    k["pm"][...] = jnp.where(chosen, 1.0, 0.0).astype(BF)
    step = iota(rows, 0) // 16 % 4
    step = jnp.where(step == 2, 3, jnp.where(step == 3, 2, step))
    expert = (iota(rows, 0) // 64 * 4 + (y + step) % 4).astype(F32)
    hit0, hit1 = named[0:1] == expert, named[1:2] == expert
    hits = jnp.where(hit0 | hit1, 1.0, 0.0)
    chosen = (hits > 0.5) & (dot(hits.astype(BF), before) == slot) & same
    k["pw"][...] = jnp.where(chosen, jnp.where(hit0, weights[0:1], weights[1:2]), 0.0)

    with jax.named_scope("w_a2"):
        pull(block(3, 2), 11)
        push(block(3, 2), 15, along_a(3))
    with jax.named_scope("w_xg"):
        for d in ORDER[8]:
            await_recv(k["xs"].at[lax.rem(z - d + NZ, NZ)], k["x_s"].at[d], k["x_r"].at[d], {"tp": other})
    with jax.named_scope("w_oz"):
        for d in ORDER[8]:
            await_recv(k["wo"].at[x, lax.rem(z - d + NZ, NZ)], k["oz_s"].at[d], k["oz_r"].at[d], {"tp": other})
        for i in range(2):
            there = lax.rem(x + (1, 3)[i], NX)
            start(k["wo"].at[x], k["wo"].at[x], k["ox_s"].at[i], k["ox_r"].at[i], {"x": there})
    with jax.named_scope("w_aend"):
        pull(block(3, 0), 5)
        pull(block(3, 1), 7)
        pull(block(1, 3), 8)
        pull(block(1, 2), 10)
        pull(block(2, 0), 12)
        pull(block(2, 1), 13)
        pull(block(2, 3), 14)
        pull(block(2, 2), 15)

    def columns(kind):
        blocks = []
        for i in range(4):
            for j in range(4):
                blocks.append(k["wt"][kind, i + tp * (j - i), j + tp * (i - j)])
        return jnp.concatenate(blocks, axis=0)

    def project(rows_ref, kinds, width, ps, pr, ss, land, t, sends, lands):
        lhs = k[rows_ref][...].reshape(NZ * S, H)
        part = jnp.concatenate([dot(lhs, columns(kind), ((1,), (1,))) for kind in kinds], axis=1)

        @pl.when(tp != z // 4)
        def _():
            k[ps][...] = part.astype(BF)
            c = remote(k[ps], k[pr], k["t_s"].at[t], k["t_r"].at[t], {"tp": other})
            c.start()
            c.wait_send()

        @pl.when(tp == z // 4)
        def _():
            await_recv(k[pr], k["t_s"].at[t], k["t_r"].at[t], {"tp": other})
            total = (part + k[pr][...].astype(F32)).astype(BF)
            k[ss][...] = total.reshape(NZ, S, width)
            mine = lax.rem(z, 4)
            for d in ORDER[8]:
                there = lax.rem(z + d, NZ)
                remote(k[ss].at[there], k[land].at[mine], k[sends].at[d], k[lands].at[mine], {"z": there}).start()
            k[land][mine] = k[ss][z]

        for i in range(4):
            @pl.when(4 * tp + i != z)
            def _():
                await_recv(k[land].at[i], k[sends].at[0], k[lands].at[i], {"tp": other})

    def sends_done(ss, land, sends, lands):
        @pl.when(tp == z // 4)
        def _():
            for d in ORDER[8]:
                remote(k[ss].at[0], k[land].at[0], k[sends].at[d], k[lands].at[0], {"tp": other}).wait_send()

    project("xs", (0, 1), 512, "ps", "pr", "ss", "ra", 1, "a_s", "a_r")
    with jax.named_scope("w_ox"):
        half = (pl.ds(0, 4), pl.ds(4, 4))
        for i in range(2):
            source = k["wo"].at[lax.rem(x + (3, 1)[i], NX)]
            await_recv(source, k["ox_s"].at[i], k["ox_r"].at[i], {"tp": other})
            passed = source.at[half[i]]
            start(passed, passed, k["ox_s"].at[2 + i], k["ox_r"].at[2 + i], {"x": lax.rem(x + (1, 3)[i], NX)})
    await_recv(k["qr"].at[0], k["t_s"].at[0], k["t_r"].at[0], {"tp": other})
    row_scale = lax.rsqrt((k["qs"][0] + k["qr"][0])[:, 0:1] / D + EPSILON)
    forward = (jnp.concatenate([k["ra"][i, :, 0:256] for i in range(4)], axis=1).astype(F32) * row_scale).astype(BF)
    branch = (jnp.concatenate([k["ra"][i, :, 256:512] for i in range(4)], axis=1).astype(F32) * row_scale).astype(BF)
    for i in range(9, 14):
        loads[i].wait()
    window = [k["cv"][0], k["cv"][1], k["cv"][2], forward]
    k["nc"][0] = window[1]
    k["nc"][1] = window[2]
    k["nc"][2] = forward
    store_conv = pltpu.make_async_copy(k["nc"], o_conv, k["stores"].at[0])
    store_conv.start()
    tap_rows = k["tv"][...].astype(F32)
    conv_out = sum(window[i].astype(F32) * tap_rows[i : i + 1] for i in range(4)).astype(BF)

    def gate_map(n):
        return jnp.concatenate([dot(conv_out[:, g * 256 : g * 256 + 256], k["bd"][n, g]) for g in range(4)], axis=1)

    recur_open = jax.nn.sigmoid(gate_map(0))
    inward = jax.nn.sigmoid(gate_map(1))
    logit = -k["dv"][...]
    softplus = jnp.maximum(logit, 0.0) + jnp.log1p(jnp.exp(-jnp.abs(logit)))
    log_decay = -DECAY_POWER * recur_open * softplus
    new_hidden = jnp.exp(log_decay) * k["hv"][...] + jnp.sqrt(-expm1(2.0 * log_decay)) * (
        inward * conv_out.astype(F32)
    )
    k["nh"][...] = new_hidden
    store_hidden = pltpu.make_async_copy(k["nh"], o_hidden, k["stores"].at[1])
    store_hidden.start()
    k["ms"][y] = (jax.nn.gelu(branch.astype(F32)) * new_hidden).astype(BF)
    for d in ORDER[4]:
        start(k["ms"].at[y], k["ms"].at[y], k["m_s"].at[d], k["m_r"].at[d], {"y": lax.rem(y + d, NY)})
    with jax.named_scope("w_ox2"):
        for i in range(2):
            passed = k["wo"].at[lax.rem(x + 2, NX), half[i]]
            await_recv(passed, k["ox_s"].at[2 + i], k["ox_r"].at[2 + i], {"tp": other})
    with jax.named_scope("w_mg"):
        for d in ORDER[4]:
            await_recv(k["ms"].at[lax.rem(y - d + NY, NY)], k["m_s"].at[d], k["m_r"].at[d], {"tp": other})
    lhs = k["ms"][...].reshape(NY * S, H)
    for h in range(2):
        out_columns = jnp.concatenate([k["wo"][j, 4 * h + i] for i in range(4) for j in range(NX)], axis=0)
        part = dot(lhs, out_columns, ((1,), (1,)))
        k["po"][h] = part
        k["ps2"][h] = part.astype(BF)
    start(k["ps2"].at[other], k["pr2"], k["t_s"].at[2], k["t_r"].at[2], {"tp": other})
    with jax.named_scope("w_pt"):
        await_recv(k["pr2"], k["t_s"].at[2], k["t_r"].at[2], {"tp": other})
    k["ss2"][...] = (k["po"][tp] + k["pr2"][...].astype(F32)).astype(BF).reshape(NY, S, 256)
    for d in ORDER[4]:
        there = lax.rem(y + d, NY)
        start(k["ss2"].at[there], k["rb"].at[y], k["b_s"].at[d], k["b_r"].at[d], {"y": there})
    k["rb"][y] = k["ss2"][y]
    with jax.named_scope("w_rb"):
        for d in ORDER[4]:
            await_recv(k["rb"].at[lax.rem(y - d + NY, NY)], k["b_s"].at[d], k["b_r"].at[d], {"tp": other})
    out_terms = jnp.concatenate(
        [k["rb"][j, :, i * 64 : i * 64 + 64].astype(F32) for i in range(4) for j in range(NY)], axis=1
    )
    middle = (values + out_terms).astype(BF)
    mid_values = middle.astype(F32)
    k["qs"][1] = jnp.broadcast_to(jnp.sum(mid_values * mid_values, axis=1, keepdims=True), (S, LANES))
    start(k["qs"].at[1], k["qr"].at[1], k["t_s"].at[3], k["t_r"].at[3], {"tp": other})
    await_recv(k["qr"].at[1], k["t_s"].at[3], k["t_r"].at[3], {"tp": other})
    mid_scale = lax.rsqrt((k["qs"][1] + k["qr"][1])[:, 0:1] / D + EPSILON)
    normed = (mid_values * mid_scale * k["g2v"][...]).astype(BF)

    stacked = jnp.concatenate([normed[:, q * LANES : (q + 1) * LANES] for q in range(Q)], axis=0)
    k["zsend"][...] = dot(k["pm"][...], stacked).astype(BF).reshape(NZ, NY, 16, LANES)
    for i in range(1, 8):
        there = lax.rem(z + ZORD[i], NZ)
        start(k["zsend"].at[there], k["zrecv"].at[i], k["dz_s"].at[i], k["dz_r"].at[i], {"z": there})
    k["zrecv"][0] = k["zsend"][z]
    steps = (1, 3)

    def part_of(xi, yi, g, h=tp):
        return k["fb"].at[h, xi, yi, pl.ds(*GROUPS[g])]

    def send_x(yi, g):
        for n in range(2):
            where = {"x": lax.rem(x + steps[n], NX)}
            start(part_of(0, yi, g), part_of(1 + n, yi, g), k["dx_s"].at[n, yi, g], k["dx_r"].at[n, yi, g], where)

    def wait_x(n, yi, g):
        await_recv(part_of(1 + n, yi, g), k["dx_s"].at[n, yi, g], k["dx_r"].at[n, yi, g], {"tp": other})
        if yi // 2 == n:
            where = {"x": lax.rem(x + steps[n], NX)}
            start(part_of(1 + n, yi, g), part_of(3, yi, g), k["dl_s"].at[g, yi], k["dl_r"].at[g, yi], where)

    def send_core(xi, g):
        ref = k["fb"].at[tp, xi, :, pl.ds(*GROUPS[g])]
        start(ref, ref, k["dt_s"].at[xi, g], k["dt_r"].at[xi, g], {"tp": other})

    for g, (low, count) in enumerate(GROUPS):
        with jax.named_scope(f"w_dz{g}"):
            for i in range(max(low, 1), low + count):
                await_recv(k["zrecv"].at[i], k["dz_s"].at[i], k["dz_r"].at[i], {"tp": other})
        for i in range(1, 4):
            there = lax.rem(y + XORD[i], NY)
            src = k["zrecv"].at[pl.ds(low, count), there]
            start(src, part_of(0, i, g), k["dy_s"].at[g, i], k["dy_r"].at[g, i], {"y": there})
        k["fb"][tp, 0, 0, low : low + count] = k["zrecv"][low : low + count, y]
        send_x(0, g)
    for g in range(2):
        with jax.named_scope(f"w_dy{g}"):
            for i in range(1, 4):
                await_recv(part_of(0, i, g), k["dy_s"].at[g, i], k["dy_r"].at[g, i], {"tp": other})
                send_x(i, g)
        send_core(0, g)
        with jax.named_scope(f"w_dx0{g}"):
            wait_x(0, 0, g)
    with jax.named_scope("w_dxr"):
        for g in range(2):
            wait_x(0, 1, g)
            wait_x(1, 2, g)
            wait_x(1, 3, g)
    with jax.named_scope("w_dxe"):
        for g in range(2):
            wait_x(0, 2, g)
            wait_x(0, 3, g)
            send_core(1, g)
            wait_x(1, 0, g)
            wait_x(1, 1, g)
            send_core(2, g)
    with jax.named_scope("w_dxl"):
        for g in range(2):
            for yi in range(4):
                await_recv(part_of(3, yi, g), k["dl_s"].at[g, yi], k["dl_r"].at[g, yi], {"tp": other})
            send_core(3, g)
    with jax.named_scope("w_we"):
        for i in range(14, 19):
            loads[i].wait()

    turn = iota(square, 1) == iota(square, 0) % 16 * Q + iota(square, 0) // 16
    turn = jnp.where(turn, 1.0, 0.0).astype(BF)
    for xi in range(NX):
        with jax.named_scope(f"w_dt{xi}"):
            for g in range(2):
                ref = k["fb"].at[other, xi, :, pl.ds(*GROUPS[g])]
                await_recv(ref, k["dt_s"].at[xi, g], k["dt_r"].at[xi, g], {"tp": other})
        for yi in range(NY):
            pair = jnp.concatenate([k["fb"][h, xi, yi].reshape(LANES, LANES) for h in range(2)], axis=1)
            turned = dot(turn, pair).astype(BF)
            at = (xi * NY + yi) * 16
            for q in range(Q):
                k["ab"][at : at + 16, q * 256 : q * 256 + 256] = turned[q * 16 : q * 16 + 16]
    gate_act = dot(k["ab"][...], k["wg"][...].reshape(D, FD))
    upper = dot(k["ab"][...], k["wu"][...].reshape(D, FD))
    k["ib"][...] = (jax.nn.silu(gate_act) * upper).astype(BF)

    theirs = pl.ds(pl.multiple_of(other * H, H), H)
    ours = pl.ds(pl.multiple_of(tp * H, H), H)
    ahead, behind = {"x": lax.rem(x + 1, NX)}, {"x": lax.rem(x + 3, NX)}

    def down(xi):
        inner = k["ib"][xi * 64 : xi * 64 + 64]
        k["hs"][xi] = dot(inner, k["wd"][:, theirs]).astype(BF)
        start(k["hs"].at[xi], k["hr"].at[xi], k["ht_s"].at[xi], k["ht_r"].at[xi], {"tp": other})
        k["own"][xi] = dot(inner, k["wd"][:, ours])

    def whole(xi):
        with jax.named_scope(f"w_ht{xi}"):
            await_recv(k["hr"].at[xi], k["ht_s"].at[xi], k["ht_r"].at[xi], {"tp": other})
        return k["own"][xi] + k["hr"][xi].astype(F32)

    def send_sum(xi, half, rows):
        n = 2 - xi
        k["xsend"][xi, half] = rows.astype(BF)
        start(
            k["xsend"].at[xi, half],
            k["xrecv"].at[n, half],
            k["rx_s"].at[n, half],
            k["rx_r"].at[n, half],
            (ahead, behind)[n],
        )

    down(3)
    down(2)
    far = whole(3)
    for half in range(2):
        k["xsend"][3, half] = far[half * 32 : half * 32 + 32].astype(BF)
        src, dst = k["xsend"].at[3, half], k["rl"].at[half]
        start(src, dst, k["rl_s"].at[half], k["rl_r"].at[half], (ahead, behind)[half])
    down(1)
    next_sum = whole(2)
    send_sum(2, 1, next_sum[32:])
    down(0)
    last_sum = whole(1)
    send_sum(1, 0, last_sum[:32])
    with jax.named_scope("w_rl0"):
        await_recv(k["rl"].at[0], k["rl_s"].at[0], k["rl_r"].at[0], {"tp": other})
    send_sum(2, 0, next_sum[:32] + k["rl"][0].astype(F32))
    with jax.named_scope("w_rl1"):
        await_recv(k["rl"].at[1], k["rl_s"].at[1], k["rl_r"].at[1], {"tp": other})
    send_sum(1, 1, last_sum[32:] + k["rl"][1].astype(F32))
    home = whole(0)
    back = iota(square, 0) == iota(square, 1) % 16 * Q + iota(square, 1) // 16
    back = jnp.where(back, 1.0, 0.0).astype(BF)
    for half in (1, 0):
        with jax.named_scope(f"w_rx{half}"):
            for n in range(2):
                await_recv(k["xrecv"].at[n, half], k["rx_s"].at[n, half], k["rx_r"].at[n, half], {"tp": other})
        rows = home[half * 32 : half * 32 + 32]
        rows = (rows + k["xrecv"][0, half].astype(F32) + k["xrecv"][1, half].astype(F32)).astype(BF)
        for yi in (3, 2) if half else (1, 0):
            part = rows[yi % 2 * 16 : yi % 2 * 16 + 16]
            part = jnp.concatenate([part[:, q * LANES : (q + 1) * LANES] for q in range(Q)], axis=0)
            part = dot(back, part).astype(BF).reshape(NZ, 16, LANES)
            if yi:
                k["ysend"][yi] = part
                where = {"y": lax.rem(y - XORD[yi] + NY, NY)}
                start(k["ysend"].at[yi], k["ry"].at[yi], k["ry_s"].at[yi], k["ry_r"].at[yi], where)
            else:
                k["ry"][0] = part
    for half in (1, 0):
        with jax.named_scope(f"w_ry{half}"):
            for yi in (2, 3) if half else (1,):
                await_recv(k["ry"].at[yi], k["ry_s"].at[yi], k["ry_r"].at[yi], {"tp": other})
        pair = pl.ds(2 * half, 2)
        for i in range(1, 8):
            there = lax.rem(z - ZORD[i] + NZ, NZ)
            start(
                k["ry"].at[pair, i], k["rz"].at[z, pair], k["rz_s"].at[half, i], k["rz_r"].at[half, i], {"z": there}
            )
        k["rz"][z, 2 * half : 2 * half + 2] = k["ry"][2 * half : 2 * half + 2, 0]
    with jax.named_scope("w_rz"):
        for half in (1, 0):
            pair = pl.ds(2 * half, 2)
            for i in range(1, 8):
                ref = k["rz"].at[lax.rem(z + ZORD[i], NZ), pair]
                await_recv(ref, k["rz_s"].at[half, i], k["rz_r"].at[half, i], {"tp": other})
    returned = k["rz"][...].reshape(EXPERTS * 16, LANES).astype(F32)
    mix = dot(k["pw"][...], returned, ((0,), (0,)), HIGHEST)
    expert_mix = jnp.concatenate([mix[q * S : (q + 1) * S] for q in range(Q)], axis=1)
    k["ns"][...] = (mid_values + expert_mix).astype(BF)
    store_stream = pltpu.make_async_copy(k["ns"], o_stream, k["stores"].at[2])
    store_stream.start()

    for c in sent:
        c.wait_send()
    sends_done("ss", "ra", "a_s", "a_r")
    store_conv.wait()
    store_hidden.wait()
    store_stream.wait()


def handed_on(*refs):
    for src, dst in zip(refs[:3], refs[3:]):
        dst[...] = src[...]


def per_device(
    stream, hidden_state, conv_state, first_gain, input_weight, branch_weight, conv_taps, recur_gate, input_gate,
    decay_logit, output_weight, second_gain, routes, route_weight, expert_gate, expert_up, expert_down,
):
    shapes = scratch_shapes()
    anywhere = pl.BlockSpec(memory_space=pl.ANY)
    outs = pl.pallas_call(
        kernel,
        name="layer",
        out_shape=(
            jax.ShapeDtypeStruct((S, H), BF),
            jax.ShapeDtypeStruct((S, H), F32),
            jax.ShapeDtypeStruct((3, S, H), BF),
        ),
        in_specs=[anywhere] * 17,
        out_specs=(anywhere,) * 3,
        scratch_shapes=[shapes[n] for n in NAMES],
        compiler_params=pltpu.CompilerParams(
            collective_id=0, has_side_effects=True, vmem_limit_bytes=60 * 1024 * 1024
        ),
    )(
        stream,
        hidden_state,
        conv_state.transpose(1, 0, 2),
        first_gain.reshape(1, H),
        input_weight.T,
        branch_weight.T,
        conv_taps,
        recur_gate.reshape(H, 64),
        input_gate.reshape(H, 64),
        decay_logit.reshape(1, H),
        output_weight.T,
        second_gain.reshape(1, H),
        routes.T,
        route_weight.T,
        expert_gate.reshape(2, Q, LANES, FD),
        expert_up.reshape(2, Q, LANES, FD),
        expert_down,
    )
    vmem = pl.BlockSpec(memory_space=pltpu.VMEM)
    new_stream, new_hidden, new_conv = pl.pallas_call(
        handed_on,
        name="handed_on",
        out_shape=tuple(jax.ShapeDtypeStruct(o.shape, o.dtype) for o in outs),
        in_specs=[vmem] * 3,
        out_specs=(vmem,) * 3,
    )(*outs)
    return new_stream, new_hidden, new_conv.transpose(1, 0, 2)


def solution(mesh):
    torus = Mesh(mesh.devices.reshape(NZ, NY, NX, mesh.shape["tp"]), EP_TP)
    in_specs = (
        P(EP, "tp"),
        P(EP, "tp"),
        P(EP, None, "tp"),
        P("tp"),
        P("tp", EP),
        P("tp", EP),
        P(None, "tp"),
        P("tp", None, None),
        P("tp", None, None),
        P("tp"),
        P("tp", EP),
        P("tp"),
        P(EP, None),
        P(EP, None),
        P(None, EP_TP),
        P(None, EP_TP),
        P(EP_TP, None),
    )
    out_specs = (P(EP, "tp"), P(EP, "tp"), P(EP, None, "tp"))
    return jax.shard_map(per_device, mesh=torus, in_specs=in_specs, out_specs=out_specs, check_vma=False)
```

```python
import jax
import jax.numpy as jnp
from jax import lax
from jax.experimental import pallas as pl
from jax.experimental.pallas import tpu as pltpu
from jax.sharding import Mesh
from jax.sharding import PartitionSpec as P

EP = ("z", "y", "x")
EP_TP = ("z", "y", "x", "tp")
MESH = pl.DeviceIdType.MESH
NZ, NY, NX = 8, 4, 4
ORDER = {8: (4, 3, 5, 2, 6, 1, 7), 4: (2, 1, 3)}
ZORD, XORD = (0, 1, 7, 2, 6, 3, 5, 4), (0, 1, 3, 2)
GROUPS = ((0, 5), (5, 3))
BF, F32 = jnp.bfloat16, jnp.float32
EPSILON = 1e-6
DECAY_POWER = 8.0
S, H, D, FD = 16, 1024, 2048, 384
LANES, Q = 128, 8
EXPERTS, CAP = 32, 2
HIGHEST = lax.Precision.HIGHEST


def scratch_shapes():
    vm, dma = pltpu.VMEM, pltpu.SemaphoreType.DMA
    return dict(
        sv=vm((S, H), BF),
        hv=vm((S, H), F32),
        cv=vm((3, S, H), BF),
        g1v=vm((1, H), F32),
        tv=vm((4, H), BF),
        rgv=vm((H, 64), BF),
        igv=vm((H, 64), BF),
        dv=vm((1, H), F32),
        g2v=vm((1, H), F32),
        rtv=vm((2, S), jnp.int32),
        rwv=vm((2, S), F32),
        wg=vm((Q, 2, LANES, FD), BF),
        wu=vm((Q, 2, LANES, FD), BF),
        wd=vm((FD, D), BF),
        xs=vm((NZ, S, H), BF),
        ms=vm((NY, S, H), BF),
        wt=vm((2, 4, 4, S, H), BF),
        wo=vm((NX, NZ, S, H), BF),
        ps=vm((NZ * S, 512), BF),
        pr=vm((NZ * S, 512), BF),
        ss=vm((NZ, S, 512), BF),
        ra=vm((4, S, 512), BF),
        ps2=vm((2, NY, S, 256), BF),
        rb=vm((2, NY, S, 256), BF),
        qs=vm((2, S, LANES), F32),
        qr=vm((2, S, LANES), F32),
        bd=vm((2, 4, 256, 256), BF),
        pm=vm((EXPERTS * 16, LANES), BF),
        pw=vm((EXPERTS * 16, LANES), F32),
        zsend=vm((NZ, NY, 16, LANES), BF),
        zrecv=vm((NZ, NY, 16, LANES), BF),
        fb=vm((2, NX, NY, NZ, 16, LANES), BF),
        ab=vm((256, D), BF),
        ib=vm((256, FD), BF),
        hs=vm((NX, 64, H), BF),
        hr=vm((NX, 64, H), BF),
        own=vm((NX, 64, H), F32),
        xsend=vm((NX, 2, 32, H), BF),
        xrecv=vm((NX, 2, 32, H), BF),
        ysend=vm((NY, NZ, 16, LANES), BF),
        ry=vm((NY, NZ, 16, LANES), BF),
        rz=vm((NZ, NY, 16, LANES), BF),
        loads=dma((24,)),
        x_s=dma((8,)), x_r=dma((8,)),
        m_s=dma((8,)), m_r=dma((8,)),
        w_s=dma((5, 4)), w_r=dma((5, 4)),
        oz_s=dma((8,)), oz_r=dma((8,)),
        ox_s=dma((2, 8)), ox_r=dma((2, 8)),
        ol_s=dma((8,)), ol_r=dma((8,)),
        t_s=dma((4,)), t_r=dma((4,)),
        a_s=dma((8,)), a_r=dma((4,)),
        b_s=dma((2, 4)), b_r=dma((2, 4)),
        dz_s=dma((8,)), dz_r=dma((8,)),
        dy_s=dma((2, 4)), dy_r=dma((2, 4)),
        dx_s=dma((3, 4, 2)), dx_r=dma((3, 4, 2)),
        dl_s=dma((2, 4)), dl_r=dma((2, 4)),
        dt_s=dma((4, 2)), dt_r=dma((4, 2)),
        ht_s=dma((4,)), ht_r=dma((4,)),
        rx_s=dma((4, 2)), rx_r=dma((4, 2)),
        ry_s=dma((4,)), ry_r=dma((4,)),
        rz_s=dma((2, 8)), rz_r=dma((2, 8)),
    )


NAMES = tuple(scratch_shapes())


def dot(a, b, dims=((1,), (0,)), precision=None):
    return lax.dot_general(a, b, (dims, ((), ())), precision=precision, preferred_element_type=F32)


def iota(shape, dim):
    return lax.broadcasted_iota(jnp.int32, shape, dim)


def expm1(v):
    series = 1.0 + v * (1.0 / 9.0)
    for n in range(8, 1, -1):
        series = 1.0 + v * (1.0 / n) * series
    return jnp.where(v > -0.5, v * series, jnp.exp(v) - 1.0)


def remote(src, dst, ssem, rsem, where):
    return pltpu.make_async_remote_copy(
        src_ref=src, dst_ref=dst, send_sem=ssem, recv_sem=rsem, device_id=where, device_id_type=MESH
    )


def kernel(*refs):
    (stream, hidden, conv, gain1, w_in, w_br, taps, rg, ig, decay, w_out, gain2, routes, rw, eg, eu, ed) = refs[:17]
    o_stream, o_hidden, o_conv = refs[17:20]
    k = dict(zip(NAMES, refs[20:]))
    z, y, x, tp = (lax.axis_index(a) for a in EP_TP)
    other = 1 - tp
    sent = []

    barrier = pltpu.get_barrier_semaphore()
    for axis, me in (("z", z), ("y", y), ("x", x)):
        n = {"z": NZ, "y": NY, "x": NX}[axis]
        for d in ORDER[n]:
            pl.semaphore_signal(barrier, inc=1, device_id={axis: lax.rem(me + d, n)}, device_id_type=MESH)
    for d in ORDER[4]:
        there = {"y": lax.rem(y + d, NY), "tp": other}
        pl.semaphore_signal(barrier, inc=1, device_id=there, device_id_type=MESH)
    pl.semaphore_signal(barrier, inc=1, device_id={"tp": other}, device_id_type=MESH)

    a = y + tp * (x - y)
    b = x + tp * (y - x)
    plan = [
        (stream, k["sv"]), (gain1, k["g1v"]),
        (w_in, k["wt"].at[0, a, b]), (w_br, k["wt"].at[1, a, b]), (w_out, k["wo"].at[x, z]),
        (rg, k["rgv"]), (ig, k["igv"]), (routes, k["rtv"]), (rw, k["rwv"]),
        (conv, k["cv"]), (taps, k["tv"]), (decay, k["dv"]), (hidden, k["hv"]), (gain2, k["g2v"]),
        (eg.at[0], k["wg"].at[:, 0]), (eg.at[1], k["wg"].at[:, 1]),
        (eu.at[0], k["wu"].at[:, 0]), (eu.at[1], k["wu"].at[:, 1]), (ed, k["wd"]),
    ]
    loads = [pltpu.make_async_copy(s, t, k["loads"].at[i]) for i, (s, t) in enumerate(plan)]
    for c in loads:
        c.start()

    def start(src, dst, ssem, rsem, where):
        c = remote(src, dst, ssem, rsem, where)
        c.start()
        sent.append(c)

    def await_recv(ref, ssem, rsem, where):
        remote(ref, ref, ssem, rsem, where).wait_recv()

    loads[0].wait()
    loads[1].wait()
    values = k["sv"][...].astype(F32)
    k["xs"][z] = (values * k["g1v"][...]).astype(BF)
    k["qs"][0] = jnp.broadcast_to(jnp.sum(values * values, axis=1, keepdims=True), (S, LANES))
    loads[5].wait()
    loads[6].wait()
    eye = (iota((64, 256), 1) % 64 == iota((64, 256), 0)).astype(BF)
    on = iota((H, 256), 0) // 64 % 4 == iota((H, 256), 1) // 64
    for n, ref in enumerate((k["rgv"], k["igv"])):
        k["bd"][n] = jnp.where(on, dot(ref[...], eye), 0.0).astype(BF).reshape(4, 256, 256)

    loads[7].wait()
    loads[8].wait()
    spread = (iota((S, LANES), 1) % S == iota((S, LANES), 0)).astype(F32)
    named = dot(k["rtv"][...].astype(F32), spread, precision=HIGHEST)
    weights = dot(k["rwv"][...], spread, precision=HIGHEST)
    rows = (EXPERTS * 16, LANES)
    expert = (iota(rows, 0) // 16).astype(F32)
    hit0, hit1 = named[0:1] == expert, named[1:2] == expert
    hits = jnp.where(hit0 | hit1, 1.0, 0.0)
    square = (LANES, LANES)
    before = (iota(square, 0) < iota(square, 1) % S).astype(BF)
    rank = dot(hits.astype(BF), before)
    slot = (iota(rows, 0) // Q % CAP).astype(F32)
    same = iota(rows, 0) % Q == iota(rows, 1) // S
    chosen = (hits > 0.5) & (rank == slot) & same
    k["pm"][...] = jnp.where(chosen, 1.0, 0.0).astype(BF)
    step = iota(rows, 0) // 16 % 4
    step = jnp.where(step == 2, 3, jnp.where(step == 3, 2, step))
    expert = (iota(rows, 0) // 64 * 4 + (y + step) % 4).astype(F32)
    hit0, hit1 = named[0:1] == expert, named[1:2] == expert
    hits = jnp.where(hit0 | hit1, 1.0, 0.0)
    chosen = (hits > 0.5) & (dot(hits.astype(BF), before) == slot) & same
    k["pw"][...] = jnp.where(chosen, jnp.where(hit0, weights[0:1], weights[1:2]), 0.0)

    for i in (2, 3, 4):
        loads[i].wait()
    with jax.named_scope("w_bar"):
        pl.semaphore_wait(barrier, 17)

    def along_b(d):
        return {"y": lax.rem(y + d * tp, NY), "x": lax.rem(x + d * other, NX)}

    def along_a(d):
        return {"y": lax.rem(y + d * other, NY), "x": lax.rem(x + d * tp, NX)}

    both = pl.ds(0, 2)

    def block(da, db):
        return k["wt"].at[both, lax.rem(a - da + 4, 4), lax.rem(b - db + 4, 4)]

    def push(ref, i, along):
        for d in ORDER[4]:
            start(ref, ref, k["w_s"].at[i, d], k["w_r"].at[i, d], along(d))

    def pull(ref, i, d):
        await_recv(ref, k["w_s"].at[i, d], k["w_r"].at[i, d], {"tp": other})

    push(block(0, 0), 4, along_b)
    push(block(0, 0), 0, along_a)
    near = (2, 6, 1, 7)
    lanes = (pl.ds(0, H // 2), pl.ds(H // 2, H // 2))

    def along_z(d):
        return {"z": lax.rem(z + d, NZ)}

    def slot(ref, d):
        return ref.at[lax.rem(z - d + NZ, NZ)]

    def column_send(ref, ssem, rsem):
        for d in near:
            start(ref.at[z], ref.at[z], ssem.at[d], rsem.at[d], along_z(d))

    def column_relay(ref, ssem, rsem):
        for n, d in enumerate((2, 6)):
            got, piece = slot(ref, d), slot(ref, d).at[:, lanes[n]]
            await_recv(got, ssem.at[d], rsem.at[d], {"tp": other})
            start(piece, piece, ssem.at[(0, 4)[n]], rsem.at[(0, 4)[n]], along_z(d))
            start(got, got, ssem.at[(3, 5)[n]], rsem.at[(3, 5)[n]], along_z((1, 7)[n]))

    def column_end(ref, ssem, rsem):
        for d in (3, 5):
            await_recv(slot(ref, d), ssem.at[d], rsem.at[d], {"tp": other})
        for n in range(2):
            await_recv(slot(ref, 4).at[:, lanes[n]], ssem.at[(0, 4)[n]], rsem.at[(0, 4)[n]], {"tp": other})

    rows_column = (k["xs"], k["x_s"], k["x_r"])
    weight_column = (k["wo"].at[x], k["oz_s"], k["oz_r"])
    column_send(*rows_column)
    start(k["qs"].at[0], k["qr"].at[0], k["t_s"].at[0], k["t_r"].at[0], {"tp": other})
    column_send(*weight_column)
    def spread_slot(d):
        for n in range(2):
            ref, where = k["wo"].at[x, lax.rem(z - d + NZ, NZ)], {"x": lax.rem(x + (1, 3)[n], NX)}
            start(ref, ref, k["ox_s"].at[n, d], k["ox_r"].at[n, d], where)

    def relay_slot(d):
        for n in range(2):
            ref = k["wo"].at[lax.rem(x + (3, 1)[n], NX), lax.rem(z - d + NZ, NZ)]
            await_recv(ref, k["ox_s"].at[n, d], k["ox_r"].at[n, d], {"tp": other})
            if n == (d in (3, 4, 5, 6)):
                start(ref, ref, k["ol_s"].at[d], k["ol_r"].at[d], {"x": lax.rem(x + (1, 3)[n], NX)})

    with jax.named_scope("w_b"):
        for i in (1, 3, 2):
            pull(block(0, i), 4, i)
            push(block(0, i), i, along_a)
    with jax.named_scope("w_xz"):
        column_relay(*rows_column)
    with jax.named_scope("w_oz"):
        column_relay(*weight_column)
        for d in (1, 7):
            await_recv(slot(weight_column[0], d), k["oz_s"].at[d], k["oz_r"].at[d], {"tp": other})
        for d in (0, 1, 7, 2, 6):
            spread_slot(d)
    with jax.named_scope("w_xg"):
        for d in (1, 7):
            await_recv(slot(k["xs"], d), k["x_s"].at[d], k["x_r"].at[d], {"tp": other})
        column_end(*rows_column)
    with jax.named_scope("w_oze"):
        column_end(*weight_column)
        for d in (3, 5, 4):
            spread_slot(d)
    with jax.named_scope("w_aend"):
        for i in (0, 1, 3, 2):
            for d in (1, 3, 2):
                pull(block(d, i), i, d)

    def columns(kind):
        blocks = []
        for i in range(4):
            for j in range(4):
                blocks.append(k["wt"][kind, i + tp * (j - i), j + tp * (i - j)])
        return jnp.concatenate(blocks, axis=0)

    def project(rows_ref, kinds, width, ps, pr, ss, land, t, sends, lands, meanwhile):
        lhs = k[rows_ref][...].reshape(NZ * S, H)
        part = jnp.concatenate([dot(lhs, columns(kind), ((1,), (1,))) for kind in kinds], axis=1)

        @pl.when(tp != z // 4)
        def _():
            k[ps][...] = part.astype(BF)
            c = remote(k[ps], k[pr], k["t_s"].at[t], k["t_r"].at[t], {"tp": other})
            c.start()
            c.wait_send()

        @pl.when(tp == z // 4)
        def _():
            await_recv(k[pr], k["t_s"].at[t], k["t_r"].at[t], {"tp": other})
            total = (part + k[pr][...].astype(F32)).astype(BF)
            k[ss][...] = total.reshape(NZ, S, width)
            mine = lax.rem(z, 4)
            for d in ORDER[8]:
                there = lax.rem(z + d, NZ)
                remote(k[ss].at[there], k[land].at[mine], k[sends].at[d], k[lands].at[mine], {"z": there}).start()
            k[land][mine] = k[ss][z]

        meanwhile()
        for i in range(4):
            @pl.when(4 * tp + i != z)
            def _():
                await_recv(k[land].at[i], k[sends].at[0], k[lands].at[i], {"tp": other})

    def sends_done(ss, land, sends, lands):
        @pl.when(tp == z // 4)
        def _():
            for d in ORDER[8]:
                remote(k[ss].at[0], k[land].at[0], k[sends].at[d], k[lands].at[0], {"tp": other}).wait_send()

    def output_weight():
        with jax.named_scope("w_ox"):
            for d in (0, 1, 7, 2, 6):
                relay_slot(d)

    project("xs", (0, 1), 512, "ps", "pr", "ss", "ra", 1, "a_s", "a_r", output_weight)
    await_recv(k["qr"].at[0], k["t_s"].at[0], k["t_r"].at[0], {"tp": other})
    row_scale = lax.rsqrt((k["qs"][0] + k["qr"][0])[:, 0:1] / D + EPSILON)
    forward = (jnp.concatenate([k["ra"][i, :, 0:256] for i in range(4)], axis=1).astype(F32) * row_scale).astype(BF)
    branch = (jnp.concatenate([k["ra"][i, :, 256:512] for i in range(4)], axis=1).astype(F32) * row_scale).astype(BF)
    for i in range(9, 14):
        loads[i].wait()
    window = [k["cv"][0], k["cv"][1], k["cv"][2], forward]
    o_conv[0] = window[1]
    o_conv[1] = window[2]
    o_conv[2] = forward
    tap_rows = k["tv"][...].astype(F32)
    conv_out = sum(window[i].astype(F32) * tap_rows[i : i + 1] for i in range(4)).astype(BF)

    def gate_map(n):
        return jnp.concatenate([dot(conv_out[:, g * 256 : g * 256 + 256], k["bd"][n, g]) for g in range(4)], axis=1)

    recur_open = jax.nn.sigmoid(gate_map(0))
    inward = jax.nn.sigmoid(gate_map(1))
    logit = -k["dv"][...]
    softplus = jnp.maximum(logit, 0.0) + jnp.log1p(jnp.exp(-jnp.abs(logit)))
    log_decay = -DECAY_POWER * recur_open * softplus
    new_hidden = jnp.exp(log_decay) * k["hv"][...] + jnp.sqrt(-expm1(2.0 * log_decay)) * (
        inward * conv_out.astype(F32)
    )
    o_hidden[...] = new_hidden
    k["ms"][y] = (jax.nn.gelu(branch.astype(F32)) * new_hidden).astype(BF)
    for d in ORDER[4]:
        start(k["ms"].at[y], k["ms"].at[y], k["m_s"].at[d], k["m_r"].at[d], {"y": lax.rem(y + d, NY)})
    with jax.named_scope("w_ox2"):
        for d in (3, 5, 4):
            relay_slot(d)
        for d in range(NZ):
            ref = k["wo"].at[lax.rem(x + 2, NX), lax.rem(z - d + NZ, NZ)]
            await_recv(ref, k["ol_s"].at[d], k["ol_r"].at[d], {"tp": other})
    with jax.named_scope("w_mg"):
        for d in ORDER[4]:
            await_recv(k["ms"].at[lax.rem(y - d + NY, NY)], k["m_s"].at[d], k["m_r"].at[d], {"tp": other})
    lhs = k["ms"][...].reshape(NY * S, H)
    for h in range(2):
        out_columns = jnp.concatenate([k["wo"][j, 4 * h + i] for i in range(4) for j in range(NX)], axis=0)
        part = dot(lhs, out_columns, ((1,), (1,)))
        k["ps2"][h] = part.astype(BF).reshape(NY, S, 256)
    for d in ORDER[4] + (0,):
        there = lax.rem(y + d, NY)
        for n, core in enumerate((tp, other)):
            if d or n:
                where = {"y": there, "tp": core}
                start(k["ps2"].at[core, there], k["rb"].at[n, y], k["b_s"].at[n, d], k["b_r"].at[n, d], where)
    k["rb"][0, y] = k["ps2"][tp, y]
    with jax.named_scope("w_rb"):
        for d in ORDER[4] + (0,):
            for n in range(2):
                if d or n:
                    ref = k["rb"].at[n, lax.rem(y - d + NY, NY)]
                    await_recv(ref, k["b_s"].at[n, d], k["b_r"].at[n, d], {"tp": other})
    landed = k["rb"][0].astype(F32) + k["rb"][1].astype(F32)
    out_terms = jnp.concatenate(
        [landed[j, :, i * 64 : i * 64 + 64] for i in range(4) for j in range(NY)], axis=1
    )
    middle = (values + out_terms).astype(BF)
    mid_values = middle.astype(F32)
    k["qs"][1] = jnp.broadcast_to(jnp.sum(mid_values * mid_values, axis=1, keepdims=True), (S, LANES))
    start(k["qs"].at[1], k["qr"].at[1], k["t_s"].at[3], k["t_r"].at[3], {"tp": other})
    await_recv(k["qr"].at[1], k["t_s"].at[3], k["t_r"].at[3], {"tp": other})
    mid_scale = lax.rsqrt((k["qs"][1] + k["qr"][1])[:, 0:1] / D + EPSILON)
    normed = (mid_values * mid_scale * k["g2v"][...]).astype(BF)

    stacked = jnp.concatenate([normed[:, q * LANES : (q + 1) * LANES] for q in range(Q)], axis=0)
    k["zsend"][...] = dot(k["pm"][...], stacked).astype(BF).reshape(NZ, NY, 16, LANES)
    for i in range(7, 0, -1):
        there = lax.rem(z + ZORD[i], NZ)
        start(k["zsend"].at[there], k["zrecv"].at[i], k["dz_s"].at[i], k["dz_r"].at[i], {"z": there})
    k["zrecv"][0] = k["zsend"][z]

    def part_of(xi, yi, g, h=tp):
        return k["fb"].at[h, xi, yi, pl.ds(*GROUPS[g])]

    def send_x(yi, g):
        for n in (2, 0, 1) if g else (0, 1):
            where = {"x": lax.rem(x + (1, 3, 2)[n], NX)}
            start(part_of(0, yi, g), part_of(1 + n, yi, g), k["dx_s"].at[n, yi, g], k["dx_r"].at[n, yi, g], where)

    def wait_x(n, yi, g):
        await_recv(part_of(1 + n, yi, g), k["dx_s"].at[n, yi, g], k["dx_r"].at[n, yi, g], {"tp": other})
        if yi // 2 == n and not g:
            where = {"x": lax.rem(x + (1, 3)[n], NX)}
            start(part_of(1 + n, yi, g), part_of(3, yi, g), k["dl_s"].at[g, yi], k["dl_r"].at[g, yi], where)

    def send_core(xi, g):
        ref = k["fb"].at[tp, xi, :, pl.ds(*GROUPS[g])]
        start(ref, ref, k["dt_s"].at[xi, g], k["dt_r"].at[xi, g], {"tp": other})

    for g, (low, count) in enumerate(GROUPS):
        with jax.named_scope(f"w_dz{g}"):
            for i in range(max(low, 1), low + count):
                await_recv(k["zrecv"].at[i], k["dz_s"].at[i], k["dz_r"].at[i], {"tp": other})
        for i in (3, 1, 2):
            there = lax.rem(y + XORD[i], NY)
            src = k["zrecv"].at[pl.ds(low, count), there]
            start(src, part_of(0, i, g), k["dy_s"].at[g, i], k["dy_r"].at[g, i], {"y": there})
        k["fb"][tp, 0, 0, low : low + count] = k["zrecv"][low : low + count, y]
        send_x(0, g)
    for g in range(2):
        with jax.named_scope(f"w_dy{g}"):
            for i in range(1, 4):
                await_recv(part_of(0, i, g), k["dy_s"].at[g, i], k["dy_r"].at[g, i], {"tp": other})
                send_x(i, g)
        send_core(0, g)
        if not g:
            with jax.named_scope("w_dx0"):
                wait_x(0, 0, 0)
    with jax.named_scope("w_dxr"):
        wait_x(0, 1, 0)
        wait_x(1, 2, 0)
        wait_x(1, 3, 0)
    with jax.named_scope("w_dxe"):
        for yi in (2, 3):
            wait_x(0, yi, 0)
        send_core(1, 0)
        for yi in (0, 1):
            wait_x(1, yi, 0)
        send_core(2, 0)
        for n in range(2):
            for yi in range(NY):
                wait_x(n, yi, 1)
            send_core(1 + n, 1)
    with jax.named_scope("w_we"):
        for i in range(14, 19):
            loads[i].wait()

    turn = iota(square, 1) == iota(square, 0) % 16 * Q + iota(square, 0) // 16
    turn = jnp.where(turn, 1.0, 0.0).astype(BF)

    def to_rows(xi):
        with jax.named_scope(f"w_dt{xi}"):
            for g in range(2):
                ref = k["fb"].at[other, xi, :, pl.ds(*GROUPS[g])]
                await_recv(ref, k["dt_s"].at[xi, g], k["dt_r"].at[xi, g], {"tp": other})
        for yi in range(NY):
            pair = jnp.concatenate([k["fb"][h, xi, yi].reshape(LANES, LANES) for h in range(2)], axis=1)
            turned = dot(turn, pair).astype(BF)
            at = (xi * NY + yi) * 16
            for q in range(Q):
                k["ab"][at : at + 16, q * 256 : q * 256 + 256] = turned[q * 16 : q * 16 + 16]

    def up(low, high):
        rows = k["ab"][low:high]
        gate_act = dot(rows, k["wg"][...].reshape(D, FD))
        upper = dot(rows, k["wu"][...].reshape(D, FD))
        k["ib"][low:high] = (jax.nn.silu(gate_act) * upper).astype(BF)

    theirs = pl.ds(pl.multiple_of(other * H, H), H)
    ours = pl.ds(pl.multiple_of(tp * H, H), H)

    def down(xi):
        inner = k["ib"][xi * 64 : xi * 64 + 64]
        k["hs"][xi] = dot(inner, k["wd"][:, theirs]).astype(BF)
        start(k["hs"].at[xi], k["hr"].at[xi], k["ht_s"].at[xi], k["ht_r"].at[xi], {"tp": other})
        k["own"][xi] = dot(inner, k["wd"][:, ours])

    def whole(xi):
        with jax.named_scope(f"w_ht{xi}"):
            await_recv(k["hr"].at[xi], k["ht_s"].at[xi], k["ht_r"].at[xi], {"tp": other})
        return k["own"][xi] + k["hr"][xi].astype(F32)

    def send_sum(xi):
        where = {"x": lax.rem(x - XORD[xi] + NX, NX)}
        total = whole(xi).astype(BF)
        for half in (1, 0):
            k["xsend"][xi, half] = total[half * 32 : half * 32 + 32]
            src, dst = k["xsend"].at[xi, half], k["xrecv"].at[xi, half]
            start(src, dst, k["rx_s"].at[xi, half], k["rx_r"].at[xi, half], where)

    for xi in range(3):
        to_rows(xi)
    up(0, 192)
    with jax.named_scope("w_dxl"):
        for yi in range(NY):
            await_recv(part_of(3, yi, 0), k["dl_s"].at[0, yi], k["dl_r"].at[0, yi], {"tp": other})
        send_core(3, 0)
        for yi in range(NY):
            wait_x(2, yi, 1)
        send_core(3, 1)
    down(1)
    down(2)
    to_rows(3)
    up(192, 256)
    down(3)
    send_sum(1)
    send_sum(2)
    send_sum(3)
    down(0)
    home = whole(0)
    back = iota(square, 0) == iota(square, 1) % 16 * Q + iota(square, 1) // 16
    back = jnp.where(back, 1.0, 0.0).astype(BF)
    for half in (1, 0):
        with jax.named_scope(f"w_rx{half}"):
            for n in range(1, 4):
                await_recv(k["xrecv"].at[n, half], k["rx_s"].at[n, half], k["rx_r"].at[n, half], {"tp": other})
        rows = home[half * 32 : half * 32 + 32]
        rows = sum((k["xrecv"][n, half].astype(F32) for n in range(1, 4)), rows).astype(BF)
        for yi in (3, 2) if half else (1, 0):
            part = rows[yi % 2 * 16 : yi % 2 * 16 + 16]
            part = jnp.concatenate([part[:, q * LANES : (q + 1) * LANES] for q in range(Q)], axis=0)
            part = dot(back, part).astype(BF).reshape(NZ, 16, LANES)
            if yi:
                k["ysend"][yi] = part
                where = {"y": lax.rem(y - XORD[yi] + NY, NY)}
                start(k["ysend"].at[yi], k["ry"].at[yi], k["ry_s"].at[yi], k["ry_r"].at[yi], where)
            else:
                k["ry"][0] = part
    for half in (1, 0):
        with jax.named_scope(f"w_ry{half}"):
            for yi in (2, 3) if half else (1,):
                await_recv(k["ry"].at[yi], k["ry_s"].at[yi], k["ry_r"].at[yi], {"tp": other})
        pair = pl.ds(2 * half, 2)
        for i in range(7, 0, -1):
            there = lax.rem(z - ZORD[i] + NZ, NZ)
            start(
                k["ry"].at[pair, i], k["rz"].at[z, pair], k["rz_s"].at[half, i], k["rz_r"].at[half, i], {"z": there}
            )
        k["rz"][z, 2 * half : 2 * half + 2] = k["ry"][2 * half : 2 * half + 2, 0]
    with jax.named_scope("w_rz"):
        for half in (1, 0):
            pair = pl.ds(2 * half, 2)
            for i in range(1, 8):
                ref = k["rz"].at[lax.rem(z + ZORD[i], NZ), pair]
                await_recv(ref, k["rz_s"].at[half, i], k["rz_r"].at[half, i], {"tp": other})
    returned = k["rz"][...].reshape(EXPERTS * 16, LANES).astype(F32)
    mix = dot(k["pw"][...], returned, ((0,), (0,)), HIGHEST)
    expert_mix = jnp.concatenate([mix[q * S : (q + 1) * S] for q in range(Q)], axis=1)
    o_stream[...] = (mid_values + expert_mix).astype(BF)
    for c in sent:
        c.wait_send()
    sends_done("ss", "ra", "a_s", "a_r")


def handed_on(*refs):
    for src, dst in zip(refs[:3], refs[3:]):
        dst[...] = src[...]


def per_device(
    stream, hidden_state, conv_state, first_gain, input_weight, branch_weight, conv_taps, recur_gate, input_gate,
    decay_logit, output_weight, second_gain, routes, route_weight, expert_gate, expert_up, expert_down,
):
    shapes = scratch_shapes()
    vmem = pl.BlockSpec(memory_space=pltpu.VMEM)
    anywhere = pl.BlockSpec(memory_space=pl.ANY)
    outs = pl.pallas_call(
        kernel,
        name="layer",
        out_shape=(
            jax.ShapeDtypeStruct((S, H), BF),
            jax.ShapeDtypeStruct((S, H), F32),
            jax.ShapeDtypeStruct((3, S, H), BF),
        ),
        in_specs=[anywhere] * 17,
        out_specs=(vmem,) * 3,
        scratch_shapes=[shapes[n] for n in NAMES],
        compiler_params=pltpu.CompilerParams(
            collective_id=0, has_side_effects=True, vmem_limit_bytes=60 * 1024 * 1024
        ),
    )(
        stream,
        hidden_state,
        conv_state.transpose(1, 0, 2),
        first_gain.reshape(1, H),
        input_weight.T,
        branch_weight.T,
        conv_taps,
        recur_gate.reshape(H, 64),
        input_gate.reshape(H, 64),
        decay_logit.reshape(1, H),
        output_weight.T,
        second_gain.reshape(1, H),
        routes.T,
        route_weight.T,
        expert_gate.reshape(2, Q, LANES, FD),
        expert_up.reshape(2, Q, LANES, FD),
        expert_down,
    )
    new_stream, new_hidden, new_conv = pl.pallas_call(
        handed_on,
        name="handed_on",
        out_shape=tuple(jax.ShapeDtypeStruct(o.shape, o.dtype) for o in outs),
        in_specs=[vmem] * 3,
        out_specs=(vmem,) * 3,
    )(*outs)
    return new_stream, new_hidden, new_conv.transpose(1, 0, 2)


def solution(mesh):
    torus = Mesh(mesh.devices.reshape(NZ, NY, NX, mesh.shape["tp"]), EP_TP)
    in_specs = (
        P(EP, "tp"),
        P(EP, "tp"),
        P(EP, None, "tp"),
        P("tp"),
        P("tp", EP),
        P("tp", EP),
        P(None, "tp"),
        P("tp", None, None),
        P("tp", None, None),
        P("tp"),
        P("tp", EP),
        P("tp"),
        P(EP, None),
        P(EP, None),
        P(None, EP_TP),
        P(None, EP_TP),
        P(EP_TP, None),
    )
    out_specs = (P(EP, "tp"), P(EP, "tp"), P(EP, None, "tp"))
    return jax.shard_map(per_device, mesh=torus, in_specs=in_specs, out_specs=out_specs, check_vma=False)
```

```python
import jax
import jax.numpy as jnp
from jax import lax
from jax.experimental import pallas as pl
from jax.experimental.pallas import tpu as pltpu
from jax.sharding import Mesh
from jax.sharding import PartitionSpec as P

EP = ("z", "y", "x")
EP_TP = ("z", "y", "x", "tp")
MESH = pl.DeviceIdType.MESH
NZ, NY, NX = 8, 4, 4
ORDER = {8: (4, 3, 5, 2, 6, 1, 7), 4: (2, 1, 3)}
ZORD, XORD = (0, 1, 7, 2, 6, 3, 5, 4), (0, 1, 3, 2)
GROUPS = ((0, 5), (5, 3))
BF, F32 = jnp.bfloat16, jnp.float32
EPSILON = 1e-6
DECAY_POWER = 8.0
S, H, D, FD = 16, 1024, 2048, 384
LANES, Q = 128, 8
EXPERTS, CAP = 32, 2
HIGHEST = lax.Precision.HIGHEST


SENDS = 32


def semaphores():
    first = {
        "load": [(i,) for i in range(19)],
        "t": [(i,) for i in range(4)],
        "w": [(i, d) for i in range(5) for d in (1, 2, 3)],
        "x": [(d,) for d in range(8)],
        "oz": [(d,) for d in range(8)],
        "ox": [(n, d) for n in range(2) for d in range(8)],
        "ol": [(d,) for d in range(8)],
        "m": [(d,) for d in (1, 2, 3)],
        "b": [(n, d) for n in range(2) for d in range(4) if n or d],
    }
    at = {}
    for name, indices in first.items():
        for index in indices:
            at[(name, *index)] = len(at)
    count = len(at)

    def share(keys, *names):
        free = [at[(name, *index)] for name in names for index in first[name]]
        for key, i in zip(keys, free, strict=False):
            at[key] = i
        return free[len(keys) :]

    groups, halves = (0, 1), (0, 1)
    along = [("dz", i) for i in range(1, 8)] + [("dy", g, i) for g in groups for i in (1, 2, 3)]
    left = share(along, "w")
    left += [at[("load", i)] for i in range(9, 14)] + [at[("t", 0)]]
    for key, i in zip([("dt", xi, g) for xi in range(4) for g in groups], left, strict=True):
        at[key] = i
    rows = [("dx", n, yi, 0) for n in range(2) for yi in range(4)] + [("dx", n, yi, 1) for n in range(3) for yi in range(4)]
    share(rows + [("dl", 0, yi) for yi in range(4)], "x", "oz", "load")
    back = [("ht", xi) for xi in range(4)] + [("rx", xi, half) for xi in (1, 2, 3) for half in halves]
    back += [("ry", yi) for yi in (1, 2, 3)] + [("rz", half, i) for half in halves for i in range(1, 8)]
    assert not share(back, "ox", "ol", "m")
    return at, count


AT, COUNT = semaphores()


def scratch_shapes():
    vm, dma = pltpu.VMEM, pltpu.SemaphoreType.DMA
    return dict(
        sv=vm((S, H), BF),
        hv=vm((S, H), F32),
        cv=vm((3, S, H), BF),
        g1v=vm((1, H), F32),
        tv=vm((4, H), BF),
        rgv=vm((H, 64), BF),
        igv=vm((H, 64), BF),
        dv=vm((1, H), F32),
        g2v=vm((1, H), F32),
        rtv=vm((2, S), jnp.int32),
        rwv=vm((2, S), F32),
        wg=vm((Q, 2, LANES, FD), BF),
        wu=vm((Q, 2, LANES, FD), BF),
        wd=vm((FD, D), BF),
        xs=vm((NZ, S, H), BF),
        ms=vm((NY, S, H), BF),
        wt=vm((2, 4, 4, S, H), BF),
        wo=vm((NX, NZ, S, H), BF),
        ps=vm((NZ * S, 512), BF),
        pr=vm((NZ * S, 512), BF),
        ss=vm((NZ, S, 512), BF),
        ra=vm((4, S, 512), BF),
        ps2=vm((2, NY, S, 256), BF),
        rb=vm((2, NY, S, 256), BF),
        qs=vm((2, S, LANES), F32),
        qr=vm((2, S, LANES), F32),
        bd=vm((2, 4, 256, 256), BF),
        pm=vm((EXPERTS * 16, LANES), BF),
        pw=vm((EXPERTS * 16, LANES), F32),
        zsend=vm((NZ, NY, 16, LANES), BF),
        zrecv=vm((NZ, NY, 16, LANES), BF),
        fb=vm((2, NX, NY, NZ, 16, LANES), BF),
        ab=vm((256, D), BF),
        ib=vm((256, FD), BF),
        hs=vm((NX, 64, H), BF),
        hr=vm((NX, 64, H), BF),
        own=vm((NX, 64, H), F32),
        xsend=vm((NX, 2, 32, H), BF),
        xrecv=vm((NX, 2, 32, H), BF),
        ysend=vm((NY, NZ, 16, LANES), BF),
        ry=vm((NY, NZ, 16, LANES), BF),
        rz=vm((NZ, NY, 16, LANES), BF),
        sends=dma((SENDS,)),
        a_s=dma((8,)),
        a_r=dma((4,)),
        p_s=dma((1,)),
        r=dma((COUNT,)),
    )


NAMES = tuple(scratch_shapes())


def dot(a, b, dims=((1,), (0,)), precision=None):
    return lax.dot_general(a, b, (dims, ((), ())), precision=precision, preferred_element_type=F32)


def iota(shape, dim):
    return lax.broadcasted_iota(jnp.int32, shape, dim)


def expm1(v):
    series = 1.0 + v * (1.0 / 9.0)
    for n in range(8, 1, -1):
        series = 1.0 + v * (1.0 / n) * series
    return jnp.where(v > -0.5, v * series, jnp.exp(v) - 1.0)


def remote(src, dst, ssem, rsem, where):
    return pltpu.make_async_remote_copy(
        src_ref=src, dst_ref=dst, send_sem=ssem, recv_sem=rsem, device_id=where, device_id_type=MESH
    )


def kernel(*refs):
    (stream, hidden, conv, gain1, w_in, w_br, taps, rg, ig, decay, w_out, gain2, routes, rw, eg, eu, ed) = refs[:17]
    o_stream, o_hidden, o_conv = refs[17:20]
    k = dict(zip(NAMES, refs[20:]))
    z, y, x, tp = (lax.axis_index(a) for a in EP_TP)
    other = 1 - tp
    sent = []

    barrier = pltpu.get_barrier_semaphore()
    for axis, me in (("z", z), ("y", y), ("x", x)):
        n = {"z": NZ, "y": NY, "x": NX}[axis]
        for d in ORDER[n]:
            pl.semaphore_signal(barrier, inc=1, device_id={axis: lax.rem(me + d, n)}, device_id_type=MESH)
    for d in ORDER[4]:
        there = {"y": lax.rem(y + d, NY), "tp": other}
        pl.semaphore_signal(barrier, inc=1, device_id=there, device_id_type=MESH)
    pl.semaphore_signal(barrier, inc=1, device_id={"tp": other}, device_id_type=MESH)

    a = y + tp * (x - y)
    b = x + tp * (y - x)
    plan = [
        (stream, k["sv"]), (gain1, k["g1v"]),
        (w_in, k["wt"].at[0, a, b]), (w_br, k["wt"].at[1, a, b]), (w_out, k["wo"].at[x, z]),
        (rg, k["rgv"]), (ig, k["igv"]), (routes, k["rtv"]), (rw, k["rwv"]),
        (conv, k["cv"]), (taps, k["tv"]), (decay, k["dv"]), (hidden, k["hv"]), (gain2, k["g2v"]),
        (eg.at[0], k["wg"].at[:, 0]), (eg.at[1], k["wg"].at[:, 1]),
        (eu.at[0], k["wu"].at[:, 0]), (eu.at[1], k["wu"].at[:, 1]), (ed, k["wd"]),
    ]
    loads = [pltpu.make_async_copy(s, t, k["r"].at[AT[("load", i)]]) for i, (s, t) in enumerate(plan)]
    for c in loads:
        c.start()

    def sem(name, *index):
        return k["r"].at[AT[(name, *index)]]

    def start(src, dst, rsem, where):
        n = len(sent)
        if n >= SENDS:
            sent[n - SENDS].wait_send()
        c = remote(src, dst, k["sends"].at[n % SENDS], rsem, where)
        c.start()
        sent.append(c)

    def await_recv(ref, rsem, where):
        remote(ref, ref, k["sends"].at[0], rsem, where).wait_recv()

    loads[0].wait()
    loads[1].wait()
    values = k["sv"][...].astype(F32)
    k["xs"][z] = (values * k["g1v"][...]).astype(BF)
    k["qs"][0] = jnp.broadcast_to(jnp.sum(values * values, axis=1, keepdims=True), (S, LANES))
    loads[5].wait()
    loads[6].wait()
    eye = (iota((64, 256), 1) % 64 == iota((64, 256), 0)).astype(BF)
    on = iota((H, 256), 0) // 64 % 4 == iota((H, 256), 1) // 64
    for n, ref in enumerate((k["rgv"], k["igv"])):
        k["bd"][n] = jnp.where(on, dot(ref[...], eye), 0.0).astype(BF).reshape(4, 256, 256)

    loads[7].wait()
    loads[8].wait()
    spread = (iota((S, LANES), 1) % S == iota((S, LANES), 0)).astype(F32)
    named = dot(k["rtv"][...].astype(F32), spread, precision=HIGHEST)
    weights = dot(k["rwv"][...], spread, precision=HIGHEST)
    rows = (EXPERTS * 16, LANES)
    expert = (iota(rows, 0) // 16).astype(F32)
    hit0, hit1 = named[0:1] == expert, named[1:2] == expert
    hits = jnp.where(hit0 | hit1, 1.0, 0.0)
    square = (LANES, LANES)
    before = (iota(square, 0) < iota(square, 1) % S).astype(BF)
    rank = dot(hits.astype(BF), before)
    slot = (iota(rows, 0) // Q % CAP).astype(F32)
    same = iota(rows, 0) % Q == iota(rows, 1) // S
    chosen = (hits > 0.5) & (rank == slot) & same
    k["pm"][...] = jnp.where(chosen, 1.0, 0.0).astype(BF)
    step = iota(rows, 0) // 16 % 4
    step = jnp.where(step == 2, 3, jnp.where(step == 3, 2, step))
    expert = (iota(rows, 0) // 64 * 4 + (y + step) % 4).astype(F32)
    hit0, hit1 = named[0:1] == expert, named[1:2] == expert
    hits = jnp.where(hit0 | hit1, 1.0, 0.0)
    chosen = (hits > 0.5) & (dot(hits.astype(BF), before) == slot) & same
    k["pw"][...] = jnp.where(chosen, jnp.where(hit0, weights[0:1], weights[1:2]), 0.0)

    for i in (2, 3, 4):
        loads[i].wait()
    with jax.named_scope("w_bar"):
        pl.semaphore_wait(barrier, 17)

    def along_b(d):
        return {"y": lax.rem(y + d * tp, NY), "x": lax.rem(x + d * other, NX)}

    def along_a(d):
        return {"y": lax.rem(y + d * other, NY), "x": lax.rem(x + d * tp, NX)}

    both = pl.ds(0, 2)

    def block(da, db):
        return k["wt"].at[both, lax.rem(a - da + 4, 4), lax.rem(b - db + 4, 4)]

    def push(ref, i, along):
        for d in ORDER[4]:
            start(ref, ref, sem("w", i, d), along(d))

    def pull(ref, i, d):
        await_recv(ref, sem("w", i, d), {"tp": other})

    push(block(0, 0), 4, along_b)
    push(block(0, 0), 0, along_a)
    near = (2, 6, 1, 7)
    lanes = (pl.ds(0, H // 2), pl.ds(H // 2, H // 2))

    def along_z(d):
        return {"z": lax.rem(z + d, NZ)}

    def slot(ref, d):
        return ref.at[lax.rem(z - d + NZ, NZ)]

    def column_send(ref, name):
        for d in near:
            start(ref.at[z], ref.at[z], sem(name, d), along_z(d))

    def column_relay(ref, name):
        for n, d in enumerate((2, 6)):
            got, piece = slot(ref, d), slot(ref, d).at[:, lanes[n]]
            await_recv(got, sem(name, d), {"tp": other})
            start(piece, piece, sem(name, (0, 4)[n]), along_z(d))
            start(got, got, sem(name, (3, 5)[n]), along_z((1, 7)[n]))

    def column_end(ref, name):
        for d in (3, 5):
            await_recv(slot(ref, d), sem(name, d), {"tp": other})
        for n in range(2):
            await_recv(slot(ref, 4).at[:, lanes[n]], sem(name, (0, 4)[n]), {"tp": other})

    rows_column = (k["xs"], "x")
    weight_column = (k["wo"].at[x], "oz")
    column_send(*rows_column)
    start(k["qs"].at[0], k["qr"].at[0], sem("t", 0), {"tp": other})
    column_send(*weight_column)
    def spread_slot(d):
        for n in range(2):
            ref, where = k["wo"].at[x, lax.rem(z - d + NZ, NZ)], {"x": lax.rem(x + (1, 3)[n], NX)}
            start(ref, ref, sem("ox", n, d), where)

    def relay_slot(d):
        for n in range(2):
            ref = k["wo"].at[lax.rem(x + (3, 1)[n], NX), lax.rem(z - d + NZ, NZ)]
            await_recv(ref, sem("ox", n, d), {"tp": other})
            if n == (d in (3, 4, 5, 6)):
                start(ref, ref, sem("ol", d), {"x": lax.rem(x + (1, 3)[n], NX)})

    with jax.named_scope("w_b"):
        for i in (1, 3, 2):
            pull(block(0, i), 4, i)
            push(block(0, i), i, along_a)
    with jax.named_scope("w_xz"):
        column_relay(*rows_column)
    with jax.named_scope("w_oz"):
        column_relay(*weight_column)
        for d in (1, 7):
            await_recv(slot(weight_column[0], d), sem("oz", d), {"tp": other})
        for d in (0, 1, 7, 2, 6):
            spread_slot(d)
    with jax.named_scope("w_xg"):
        for d in (1, 7):
            await_recv(slot(k["xs"], d), sem("x", d), {"tp": other})
        column_end(*rows_column)
    with jax.named_scope("w_oze"):
        column_end(*weight_column)
        for d in (3, 5, 4):
            spread_slot(d)
    with jax.named_scope("w_aend"):
        for i in (0, 1, 3, 2):
            for d in (1, 3, 2):
                pull(block(d, i), i, d)

    def columns(kind):
        blocks = []
        for i in range(4):
            for j in range(4):
                blocks.append(k["wt"][kind, i + tp * (j - i), j + tp * (i - j)])
        return jnp.concatenate(blocks, axis=0)

    def project(rows_ref, kinds, width, ps, pr, ss, land, t, sends, lands, meanwhile):
        lhs = k[rows_ref][...].reshape(NZ * S, H)
        part = jnp.concatenate([dot(lhs, columns(kind), ((1,), (1,))) for kind in kinds], axis=1)

        @pl.when(tp != z // 4)
        def _():
            k[ps][...] = part.astype(BF)
            c = remote(k[ps], k[pr], k["p_s"].at[0], sem("t", t), {"tp": other})
            c.start()
            c.wait_send()

        @pl.when(tp == z // 4)
        def _():
            await_recv(k[pr], sem("t", t), {"tp": other})
            total = (part + k[pr][...].astype(F32)).astype(BF)
            k[ss][...] = total.reshape(NZ, S, width)
            mine = lax.rem(z, 4)
            for d in ORDER[8]:
                there = lax.rem(z + d, NZ)
                remote(k[ss].at[there], k[land].at[mine], k[sends].at[d], k[lands].at[mine], {"z": there}).start()
            k[land][mine] = k[ss][z]

        meanwhile()
        for i in range(4):
            @pl.when(4 * tp + i != z)
            def _():
                await_recv(k[land].at[i], k[lands].at[i], {"tp": other})

    def sends_done(ss, land, sends, lands):
        @pl.when(tp == z // 4)
        def _():
            for d in ORDER[8]:
                remote(k[ss].at[0], k[land].at[0], k[sends].at[d], k[lands].at[0], {"tp": other}).wait_send()

    def output_weight():
        with jax.named_scope("w_ox"):
            for d in (0, 1, 7, 2, 6):
                relay_slot(d)

    project("xs", (0, 1), 512, "ps", "pr", "ss", "ra", 1, "a_s", "a_r", output_weight)
    await_recv(k["qr"].at[0], sem("t", 0), {"tp": other})
    row_scale = lax.rsqrt((k["qs"][0] + k["qr"][0])[:, 0:1] / D + EPSILON)
    forward = (jnp.concatenate([k["ra"][i, :, 0:256] for i in range(4)], axis=1).astype(F32) * row_scale).astype(BF)
    branch = (jnp.concatenate([k["ra"][i, :, 256:512] for i in range(4)], axis=1).astype(F32) * row_scale).astype(BF)
    for i in range(9, 14):
        loads[i].wait()
    window = [k["cv"][0], k["cv"][1], k["cv"][2], forward]
    o_conv[0] = window[1]
    o_conv[1] = window[2]
    o_conv[2] = forward
    tap_rows = k["tv"][...].astype(F32)
    conv_out = sum(window[i].astype(F32) * tap_rows[i : i + 1] for i in range(4)).astype(BF)

    def gate_map(n):
        return jnp.concatenate([dot(conv_out[:, g * 256 : g * 256 + 256], k["bd"][n, g]) for g in range(4)], axis=1)

    recur_open = jax.nn.sigmoid(gate_map(0))
    inward = jax.nn.sigmoid(gate_map(1))
    logit = -k["dv"][...]
    softplus = jnp.maximum(logit, 0.0) + jnp.log1p(jnp.exp(-jnp.abs(logit)))
    log_decay = -DECAY_POWER * recur_open * softplus
    new_hidden = jnp.exp(log_decay) * k["hv"][...] + jnp.sqrt(-expm1(2.0 * log_decay)) * (
        inward * conv_out.astype(F32)
    )
    o_hidden[...] = new_hidden
    k["ms"][y] = (jax.nn.gelu(branch.astype(F32)) * new_hidden).astype(BF)
    for d in ORDER[4]:
        start(k["ms"].at[y], k["ms"].at[y], sem("m", d), {"y": lax.rem(y + d, NY)})
    with jax.named_scope("w_ox2"):
        for d in (3, 5, 4):
            relay_slot(d)
        for d in range(NZ):
            ref = k["wo"].at[lax.rem(x + 2, NX), lax.rem(z - d + NZ, NZ)]
            await_recv(ref, sem("ol", d), {"tp": other})
    with jax.named_scope("w_mg"):
        for d in ORDER[4]:
            await_recv(k["ms"].at[lax.rem(y - d + NY, NY)], sem("m", d), {"tp": other})
    lhs = k["ms"][...].reshape(NY * S, H)
    for h in range(2):
        out_columns = jnp.concatenate([k["wo"][j, 4 * h + i] for i in range(4) for j in range(NX)], axis=0)
        part = dot(lhs, out_columns, ((1,), (1,)))
        k["ps2"][h] = part.astype(BF).reshape(NY, S, 256)
    for d in ORDER[4] + (0,):
        there = lax.rem(y + d, NY)
        for n, core in enumerate((tp, other)):
            if d or n:
                where = {"y": there, "tp": core}
                start(k["ps2"].at[core, there], k["rb"].at[n, y], sem("b", n, d), where)
    k["rb"][0, y] = k["ps2"][tp, y]
    with jax.named_scope("w_rb"):
        for d in ORDER[4] + (0,):
            for n in range(2):
                if d or n:
                    ref = k["rb"].at[n, lax.rem(y - d + NY, NY)]
                    await_recv(ref, sem("b", n, d), {"tp": other})
    landed = k["rb"][0].astype(F32) + k["rb"][1].astype(F32)
    out_terms = jnp.concatenate(
        [landed[j, :, i * 64 : i * 64 + 64] for i in range(4) for j in range(NY)], axis=1
    )
    middle = (values + out_terms).astype(BF)
    mid_values = middle.astype(F32)
    k["qs"][1] = jnp.broadcast_to(jnp.sum(mid_values * mid_values, axis=1, keepdims=True), (S, LANES))
    start(k["qs"].at[1], k["qr"].at[1], sem("t", 3), {"tp": other})
    await_recv(k["qr"].at[1], sem("t", 3), {"tp": other})
    mid_scale = lax.rsqrt((k["qs"][1] + k["qr"][1])[:, 0:1] / D + EPSILON)
    normed = (mid_values * mid_scale * k["g2v"][...]).astype(BF)

    stacked = jnp.concatenate([normed[:, q * LANES : (q + 1) * LANES] for q in range(Q)], axis=0)
    k["zsend"][...] = dot(k["pm"][...], stacked).astype(BF).reshape(NZ, NY, 16, LANES)
    for i in range(7, 0, -1):
        there = lax.rem(z + ZORD[i], NZ)
        start(k["zsend"].at[there], k["zrecv"].at[i], sem("dz", i), {"z": there})
    k["zrecv"][0] = k["zsend"][z]

    def part_of(xi, yi, g, h=tp):
        return k["fb"].at[h, xi, yi, pl.ds(*GROUPS[g])]

    def send_x(yi, g):
        for n in (2, 0, 1) if g else (0, 1):
            where = {"x": lax.rem(x + (1, 3, 2)[n], NX)}
            start(part_of(0, yi, g), part_of(1 + n, yi, g), sem("dx", n, yi, g), where)

    def wait_x(n, yi, g):
        await_recv(part_of(1 + n, yi, g), sem("dx", n, yi, g), {"tp": other})
        if yi // 2 == n and not g:
            where = {"x": lax.rem(x + (1, 3)[n], NX)}
            start(part_of(1 + n, yi, g), part_of(3, yi, g), sem("dl", g, yi), where)

    def send_core(xi, g):
        ref = k["fb"].at[tp, xi, :, pl.ds(*GROUPS[g])]
        start(ref, ref, sem("dt", xi, g), {"tp": other})

    for g, (low, count) in enumerate(GROUPS):
        with jax.named_scope(f"w_dz{g}"):
            for i in range(max(low, 1), low + count):
                await_recv(k["zrecv"].at[i], sem("dz", i), {"tp": other})
        for i in (3, 1, 2):
            there = lax.rem(y + XORD[i], NY)
            src = k["zrecv"].at[pl.ds(low, count), there]
            start(src, part_of(0, i, g), sem("dy", g, i), {"y": there})
        k["fb"][tp, 0, 0, low : low + count] = k["zrecv"][low : low + count, y]
        send_x(0, g)
    for g in range(2):
        with jax.named_scope(f"w_dy{g}"):
            for i in range(1, 4):
                await_recv(part_of(0, i, g), sem("dy", g, i), {"tp": other})
                send_x(i, g)
        send_core(0, g)
        if not g:
            with jax.named_scope("w_dx0"):
                wait_x(0, 0, 0)
    with jax.named_scope("w_dxr"):
        wait_x(0, 1, 0)
        wait_x(1, 2, 0)
        wait_x(1, 3, 0)
    with jax.named_scope("w_dxe"):
        for yi in (2, 3):
            wait_x(0, yi, 0)
        send_core(1, 0)
        for yi in (0, 1):
            wait_x(1, yi, 0)
        send_core(2, 0)
        for n in range(2):
            for yi in range(NY):
                wait_x(n, yi, 1)
            send_core(1 + n, 1)
    with jax.named_scope("w_we"):
        for i in range(14, 19):
            loads[i].wait()

    turn = iota(square, 1) == iota(square, 0) % 16 * Q + iota(square, 0) // 16
    turn = jnp.where(turn, 1.0, 0.0).astype(BF)

    def to_rows(xi):
        with jax.named_scope(f"w_dt{xi}"):
            for g in range(2):
                ref = k["fb"].at[other, xi, :, pl.ds(*GROUPS[g])]
                await_recv(ref, sem("dt", xi, g), {"tp": other})
        for yi in range(NY):
            pair = jnp.concatenate([k["fb"][h, xi, yi].reshape(LANES, LANES) for h in range(2)], axis=1)
            turned = dot(turn, pair).astype(BF)
            at = (xi * NY + yi) * 16
            for q in range(Q):
                k["ab"][at : at + 16, q * 256 : q * 256 + 256] = turned[q * 16 : q * 16 + 16]

    def up(low, high):
        rows = k["ab"][low:high]
        gate_act = dot(rows, k["wg"][...].reshape(D, FD))
        upper = dot(rows, k["wu"][...].reshape(D, FD))
        k["ib"][low:high] = (jax.nn.silu(gate_act) * upper).astype(BF)

    theirs = pl.ds(pl.multiple_of(other * H, H), H)
    ours = pl.ds(pl.multiple_of(tp * H, H), H)

    def down(xi):
        inner = k["ib"][xi * 64 : xi * 64 + 64]
        k["hs"][xi] = dot(inner, k["wd"][:, theirs]).astype(BF)
        start(k["hs"].at[xi], k["hr"].at[xi], sem("ht", xi), {"tp": other})
        k["own"][xi] = dot(inner, k["wd"][:, ours])

    def whole(xi):
        with jax.named_scope(f"w_ht{xi}"):
            await_recv(k["hr"].at[xi], sem("ht", xi), {"tp": other})
        return k["own"][xi] + k["hr"][xi].astype(F32)

    def send_sum(xi):
        where = {"x": lax.rem(x - XORD[xi] + NX, NX)}
        total = whole(xi).astype(BF)
        for half in (1, 0):
            k["xsend"][xi, half] = total[half * 32 : half * 32 + 32]
            src, dst = k["xsend"].at[xi, half], k["xrecv"].at[xi, half]
            start(src, dst, sem("rx", xi, half), where)

    for xi in range(3):
        to_rows(xi)
    up(0, 192)
    with jax.named_scope("w_dxl"):
        for yi in range(NY):
            await_recv(part_of(3, yi, 0), sem("dl", 0, yi), {"tp": other})
        send_core(3, 0)
        for yi in range(NY):
            wait_x(2, yi, 1)
        send_core(3, 1)
    down(1)
    down(2)
    to_rows(3)
    up(192, 256)
    down(3)
    send_sum(1)
    send_sum(2)
    send_sum(3)
    down(0)
    home = whole(0)
    back = iota(square, 0) == iota(square, 1) % 16 * Q + iota(square, 1) // 16
    back = jnp.where(back, 1.0, 0.0).astype(BF)
    for half in (1, 0):
        with jax.named_scope(f"w_rx{half}"):
            for n in range(1, 4):
                await_recv(k["xrecv"].at[n, half], sem("rx", n, half), {"tp": other})
        rows = home[half * 32 : half * 32 + 32]
        rows = sum((k["xrecv"][n, half].astype(F32) for n in range(1, 4)), rows).astype(BF)
        for yi in (3, 2) if half else (1, 0):
            part = rows[yi % 2 * 16 : yi % 2 * 16 + 16]
            part = jnp.concatenate([part[:, q * LANES : (q + 1) * LANES] for q in range(Q)], axis=0)
            part = dot(back, part).astype(BF).reshape(NZ, 16, LANES)
            if yi:
                k["ysend"][yi] = part
                where = {"y": lax.rem(y - XORD[yi] + NY, NY)}
                start(k["ysend"].at[yi], k["ry"].at[yi], sem("ry", yi), where)
            else:
                k["ry"][0] = part
    for half in (1, 0):
        with jax.named_scope(f"w_ry{half}"):
            for yi in (2, 3) if half else (1,):
                await_recv(k["ry"].at[yi], sem("ry", yi), {"tp": other})
        pair = pl.ds(2 * half, 2)
        for i in range(7, 0, -1):
            there = lax.rem(z - ZORD[i] + NZ, NZ)
            start(
                k["ry"].at[pair, i], k["rz"].at[z, pair], sem("rz", half, i), {"z": there}
            )
        k["rz"][z, 2 * half : 2 * half + 2] = k["ry"][2 * half : 2 * half + 2, 0]
    with jax.named_scope("w_rz"):
        for half in (1, 0):
            pair = pl.ds(2 * half, 2)
            for i in range(1, 8):
                ref = k["rz"].at[lax.rem(z + ZORD[i], NZ), pair]
                await_recv(ref, sem("rz", half, i), {"tp": other})
    returned = k["rz"][...].reshape(EXPERTS * 16, LANES).astype(F32)
    mix = dot(k["pw"][...], returned, ((0,), (0,)), HIGHEST)
    expert_mix = jnp.concatenate([mix[q * S : (q + 1) * S] for q in range(Q)], axis=1)
    o_stream[...] = (mid_values + expert_mix).astype(BF)
    for c in sent[-SENDS:]:
        c.wait_send()
    sends_done("ss", "ra", "a_s", "a_r")


def handed_on(*refs):
    for src, dst in zip(refs[:3], refs[3:]):
        dst[...] = src[...]


def per_device(
    stream, hidden_state, conv_state, first_gain, input_weight, branch_weight, conv_taps, recur_gate, input_gate,
    decay_logit, output_weight, second_gain, routes, route_weight, expert_gate, expert_up, expert_down,
):
    shapes = scratch_shapes()
    vmem = pl.BlockSpec(memory_space=pltpu.VMEM)
    anywhere = pl.BlockSpec(memory_space=pl.ANY)
    outs = pl.pallas_call(
        kernel,
        name="layer",
        out_shape=(
            jax.ShapeDtypeStruct((S, H), BF),
            jax.ShapeDtypeStruct((S, H), F32),
            jax.ShapeDtypeStruct((3, S, H), BF),
        ),
        in_specs=[anywhere] * 17,
        out_specs=(vmem,) * 3,
        scratch_shapes=[shapes[n] for n in NAMES],
        compiler_params=pltpu.CompilerParams(
            collective_id=0, has_side_effects=True, vmem_limit_bytes=60 * 1024 * 1024
        ),
    )(
        stream,
        hidden_state,
        conv_state.transpose(1, 0, 2),
        first_gain.reshape(1, H),
        input_weight.T,
        branch_weight.T,
        conv_taps,
        recur_gate.reshape(H, 64),
        input_gate.reshape(H, 64),
        decay_logit.reshape(1, H),
        output_weight.T,
        second_gain.reshape(1, H),
        routes.T,
        route_weight.T,
        expert_gate.reshape(2, Q, LANES, FD),
        expert_up.reshape(2, Q, LANES, FD),
        expert_down,
    )
    new_stream, new_hidden, new_conv = pl.pallas_call(
        handed_on,
        name="handed_on",
        out_shape=tuple(jax.ShapeDtypeStruct(o.shape, o.dtype) for o in outs),
        in_specs=[vmem] * 3,
        out_specs=(vmem,) * 3,
    )(*outs)
    return new_stream, new_hidden, new_conv.transpose(1, 0, 2)


def solution(mesh):
    torus = Mesh(mesh.devices.reshape(NZ, NY, NX, mesh.shape["tp"]), EP_TP)
    in_specs = (
        P(EP, "tp"),
        P(EP, "tp"),
        P(EP, None, "tp"),
        P("tp"),
        P("tp", EP),
        P("tp", EP),
        P(None, "tp"),
        P("tp", None, None),
        P("tp", None, None),
        P("tp"),
        P("tp", EP),
        P("tp"),
        P(EP, None),
        P(EP, None),
        P(None, EP_TP),
        P(None, EP_TP),
        P(EP_TP, None),
    )
    out_specs = (P(EP, "tp"), P(EP, "tp"), P(EP, None, "tp"))
    return jax.shard_map(per_device, mesh=torus, in_specs=in_specs, out_specs=out_specs, check_vma=False)
```

```python
import jax
import jax.numpy as jnp
from jax import lax
from jax.experimental import pallas as pl
from jax.experimental.pallas import tpu as pltpu
from jax.sharding import Mesh
from jax.sharding import PartitionSpec as P

EP = ("z", "y", "x")
EP_TP = ("z", "y", "x", "tp")
MESH = pl.DeviceIdType.MESH
NZ, NY, NX = 8, 4, 4
ORDER = {8: (4, 3, 5, 2, 6, 1, 7), 4: (2, 1, 3)}
ZORD, XORD = (0, 1, 7, 2, 6, 3, 5, 4), (0, 1, 3, 2)
GROUPS = ((0, 5), (5, 3))
PLANE = tuple((i, j) for i in (3, 2, 1, 0) for j in (3, 2, 1, 0) if i or j)
BF, F32 = jnp.bfloat16, jnp.float32
EPSILON = 1e-6
DECAY_POWER = 8.0
S, H, D, FD = 16, 1024, 2048, 384
LANES, Q = 128, 8
EXPERTS, CAP = 32, 2
HIGHEST = lax.Precision.HIGHEST


SENDS = 32


def semaphores():
    first = {
        "load": [(i,) for i in range(19)],
        "t": [(i,) for i in range(4)],
        "w": [(i, d) for i in range(5) for d in (1, 2, 3)],
        "x": [(d,) for d in range(8)],
        "oz": [(d,) for d in range(8)],
        "ox": [(n, d) for n in range(2) for d in range(8)],
        "ol": [(d,) for d in range(8)],
        "m": [(d,) for d in (1, 2, 3)],
        "b": [(n, d) for n in range(2) for d in range(4) if n or d],
        "more": [(i,) for i in range(5)],
    }
    at = {}
    for name, indices in first.items():
        for index in indices:
            at[(name, *index)] = len(at)
    count = len(at)

    def share(keys, *names):
        free = [at[(name, *index)] for name in names for index in first[name]]
        for key, i in zip(keys, free, strict=False):
            at[key] = i
        return free[len(keys) :]

    groups, halves = (0, 1), (0, 1)
    left = share([("dz", i) for i in range(1, 8)], "w")
    for key, i in zip([("dt", xi, g) for xi in range(4) for g in groups], left, strict=True):
        at[key] = i
    plane = [(xi, yi) for xi in range(4) for yi in range(4) if xi or yi]
    share([("dp", g, *at_plane) for g in groups for at_plane in plane], "x", "oz", "more", "load")
    back = [("ht", xi) for xi in range(4)] + [("rx", *at_plane) for at_plane in plane]
    back += [("rz", half, i) for half in halves for i in range(1, 8)]
    share(back, "ox", "ol", "m", "b")
    return at, count


AT, COUNT = semaphores()


def scratch_shapes():
    vm, dma = pltpu.VMEM, pltpu.SemaphoreType.DMA
    return dict(
        sv=vm((S, H), BF),
        hv=vm((S, H), F32),
        cv=vm((3, S, H), BF),
        g1v=vm((1, H), F32),
        tv=vm((4, H), BF),
        rgv=vm((H, 64), BF),
        igv=vm((H, 64), BF),
        dv=vm((1, H), F32),
        g2v=vm((1, H), F32),
        rtv=vm((2, S), jnp.int32),
        rwv=vm((2, S), F32),
        wg=vm((Q, 2, LANES, FD), BF),
        wu=vm((Q, 2, LANES, FD), BF),
        wd=vm((FD, D), BF),
        xs=vm((NZ, S, H), BF),
        ms=vm((NY, S, H), BF),
        wt=vm((2, 4, 4, S, H), BF),
        wo=vm((NX, NZ, S, H), BF),
        ps=vm((NZ * S, 512), BF),
        pr=vm((NZ * S, 512), BF),
        ss=vm((NZ, S, 512), BF),
        ra=vm((4, S, 512), BF),
        ps2=vm((NY, 2, S, 256), BF),
        svo=vm((S, H), BF),
        rb=vm((2, NY, 2, S, 256), BF),
        qs=vm((S, LANES), F32),
        qr=vm((S, LANES), F32),
        bd=vm((2, 4, 256, 256), BF),
        pm=vm((EXPERTS * 16, LANES), BF),
        pw=vm((EXPERTS * 16, LANES), F32),
        zsend=vm((NZ, NY, 16, LANES), BF),
        zrecv=vm((NZ, NY, 16, LANES), BF),
        fb=vm((2, NX, NY, NZ, 16, LANES), BF),
        ab=vm((256, D), BF),
        ib=vm((256, FD), BF),
        hs=vm((NX, 64, H), BF),
        hr=vm((NX, 64, H), BF),
        own=vm((NX, 64, H), F32),
        xsend=vm((NX, NY, 16, H), BF),
        xrecv=vm((NX, NY, 16, H), BF),
        ry=vm((NY, NZ, 16, LANES), BF),
        rz=vm((NZ, NY, 16, LANES), BF),
        sends=dma((SENDS,)),
        spread=dma((2, 8)),
        a_s=dma((8,)),
        a_r=dma((4,)),
        p_s=dma((1,)),
        r=dma((COUNT,)),
    )


NAMES = tuple(scratch_shapes())


def dot(a, b, dims=((1,), (0,)), precision=None):
    return lax.dot_general(a, b, (dims, ((), ())), precision=precision, preferred_element_type=F32)


def iota(shape, dim):
    return lax.broadcasted_iota(jnp.int32, shape, dim)


def expm1(v):
    series = 1.0 + v * (1.0 / 9.0)
    for n in range(8, 1, -1):
        series = 1.0 + v * (1.0 / n) * series
    return jnp.where(v > -0.5, v * series, jnp.exp(v) - 1.0)


def remote(src, dst, ssem, rsem, where):
    return pltpu.make_async_remote_copy(
        src_ref=src, dst_ref=dst, send_sem=ssem, recv_sem=rsem, device_id=where, device_id_type=MESH
    )


def kernel(*refs):
    (stream, hidden, conv, gain1, w_in, w_br, taps, rg, ig, decay, w_out, gain2, routes, rw, eg, eu, ed) = refs[:17]
    o_stream, o_hidden, o_conv = refs[17:20]
    k = dict(zip(NAMES, refs[20:]))
    z, y, x, tp = (lax.axis_index(a) for a in EP_TP)
    other = 1 - tp
    sent = []

    barrier = pltpu.get_barrier_semaphore()
    for d in ORDER[8]:
        pl.semaphore_signal(barrier, inc=1, device_id={"z": lax.rem(z + d, NZ)}, device_id_type=MESH)
    for i, j in PLANE:
        there = {"y": lax.rem(y + XORD[j], NY), "x": lax.rem(x + XORD[i], NX)}
        pl.semaphore_signal(barrier, inc=1, device_id=there, device_id_type=MESH)
    for d in ORDER[4]:
        there = {"y": lax.rem(y + d, NY), "tp": other}
        pl.semaphore_signal(barrier, inc=1, device_id=there, device_id_type=MESH)
    pl.semaphore_signal(barrier, inc=1, device_id={"tp": other}, device_id_type=MESH)

    a = y + tp * (x - y)
    b = x + tp * (y - x)
    plan = [
        (stream, k["sv"]), (gain1, k["g1v"]),
        (w_in, k["wt"].at[0, a, b]), (w_br, k["wt"].at[1, a, b]), (w_out, k["wo"].at[x, z]),
        (rg, k["rgv"]), (ig, k["igv"]), (routes, k["rtv"]), (rw, k["rwv"]),
        (conv, k["cv"]), (taps, k["tv"]), (decay, k["dv"]), (hidden, k["hv"]), (gain2, k["g2v"]),
        (eg.at[0], k["wg"].at[:, 0]), (eg.at[1], k["wg"].at[:, 1]),
        (eu.at[0], k["wu"].at[:, 0]), (eu.at[1], k["wu"].at[:, 1]), (ed, k["wd"]),
    ]
    loads = [pltpu.make_async_copy(s, t, k["r"].at[AT[("load", i)]]) for i, (s, t) in enumerate(plan)]
    for c in loads:
        c.start()

    def sem(name, *index):
        return k["r"].at[AT[(name, *index)]]

    def start(src, dst, rsem, where):
        n = len(sent)
        if n >= SENDS:
            sent[n - SENDS].wait_send()
        c = remote(src, dst, k["sends"].at[n % SENDS], rsem, where)
        c.start()
        sent.append(c)

    def await_recv(ref, rsem, where):
        remote(ref, ref, k["sends"].at[0], rsem, where).wait_recv()

    loads[0].wait()
    loads[1].wait()
    values = k["sv"][...].astype(F32)
    k["xs"][z] = (values * k["g1v"][...]).astype(BF)
    k["qs"][...] = jnp.broadcast_to(jnp.sum(values * values, axis=1, keepdims=True), (S, LANES))
    loads[5].wait()
    loads[6].wait()
    eye = (iota((64, 256), 1) % 64 == iota((64, 256), 0)).astype(BF)
    on = iota((H, 256), 0) // 64 % 4 == iota((H, 256), 1) // 64
    for n, ref in enumerate((k["rgv"], k["igv"])):
        k["bd"][n] = jnp.where(on, dot(ref[...], eye), 0.0).astype(BF).reshape(4, 256, 256)

    loads[7].wait()
    loads[8].wait()
    spread = (iota((S, LANES), 1) % S == iota((S, LANES), 0)).astype(F32)
    named = dot(k["rtv"][...].astype(F32), spread, precision=HIGHEST)
    weights = dot(k["rwv"][...], spread, precision=HIGHEST)
    rows = (EXPERTS * 16, LANES)
    expert = (iota(rows, 0) // 16).astype(F32)
    hit0, hit1 = named[0:1] == expert, named[1:2] == expert
    hits = jnp.where(hit0 | hit1, 1.0, 0.0)
    square = (LANES, LANES)
    before = (iota(square, 0) < iota(square, 1) % S).astype(BF)
    rank = dot(hits.astype(BF), before)
    slot = (iota(rows, 0) // Q % CAP).astype(F32)
    same = iota(rows, 0) % Q == iota(rows, 1) // S
    chosen = (hits > 0.5) & (rank == slot) & same
    k["pm"][...] = jnp.where(chosen, 1.0, 0.0).astype(BF)
    step = iota(rows, 0) // 16 % 4
    step = jnp.where(step == 2, 3, jnp.where(step == 3, 2, step))
    expert = (iota(rows, 0) // 64 * 4 + (y + step) % 4).astype(F32)
    hit0, hit1 = named[0:1] == expert, named[1:2] == expert
    hits = jnp.where(hit0 | hit1, 1.0, 0.0)
    chosen = (hits > 0.5) & (dot(hits.astype(BF), before) == slot) & same
    k["pw"][...] = jnp.where(chosen, jnp.where(hit0, weights[0:1], weights[1:2]), 0.0)

    for i in (2, 3, 4):
        loads[i].wait()
    with jax.named_scope("w_bar"):
        pl.semaphore_wait(barrier, 26)

    def along_b(d):
        return {"y": lax.rem(y + d * tp, NY), "x": lax.rem(x + d * other, NX)}

    def along_a(d):
        return {"y": lax.rem(y + d * other, NY), "x": lax.rem(x + d * tp, NX)}

    both = pl.ds(0, 2)

    def block(da, db):
        return k["wt"].at[both, lax.rem(a - da + 4, 4), lax.rem(b - db + 4, 4)]

    def push(ref, i, along):
        for d in ORDER[4]:
            start(ref, ref, sem("w", i, d), along(d))

    def pull(ref, i, d):
        await_recv(ref, sem("w", i, d), {"tp": other})

    push(block(0, 0), 4, along_b)
    push(block(0, 0), 0, along_a)
    near = (2, 6, 1, 7)
    lanes = (pl.ds(0, H // 2), pl.ds(H // 2, H // 2))

    def along_z(d):
        return {"z": lax.rem(z + d, NZ)}

    def slot(ref, d):
        return ref.at[lax.rem(z - d + NZ, NZ)]

    def column_send(ref, name):
        for d in near:
            start(ref.at[z], ref.at[z], sem(name, d), along_z(d))

    def column_relay(ref, name):
        for n, d in enumerate((2, 6)):
            got, piece = slot(ref, d), slot(ref, d).at[:, lanes[n]]
            await_recv(got, sem(name, d), {"tp": other})
            start(piece, piece, sem(name, (0, 4)[n]), along_z(d))
            start(got, got, sem(name, (3, 5)[n]), along_z((1, 7)[n]))

    def column_end(ref, name):
        for d in (3, 5):
            await_recv(slot(ref, d), sem(name, d), {"tp": other})
        for n in range(2):
            await_recv(slot(ref, 4).at[:, lanes[n]], sem(name, (0, 4)[n]), {"tp": other})

    rows_column = (k["xs"], "x")
    weight_column = (k["wo"].at[x], "oz")
    column_send(*rows_column)
    start(k["qs"], k["qr"], sem("t", 0), {"tp": other})
    start(k["sv"], k["svo"], sem("t", 3), {"tp": other})
    column_send(*weight_column)
    def spread_slots(ds, core):
        copies = []
        for d in ds:
            for n in range(2):
                ref, where = k["wo"].at[x, lax.rem(z - d + NZ, NZ)], {"x": lax.rem(x + (1, 3)[n], NX)}
                copies.append(remote(ref, ref, k["spread"].at[n, d], sem("ox", n, d), where))

        @pl.when(tp == core)
        def _():
            for c in copies:
                c.start()

        return copies

    def relay_slot(d):
        for n in range(2):
            ref = k["wo"].at[lax.rem(x + (3, 1)[n], NX), lax.rem(z - d + NZ, NZ)]
            await_recv(ref, sem("ox", n, d), {"tp": other})
            if n == (d in (3, 4, 5, 6)):
                start(ref, ref, sem("ol", d), {"x": lax.rem(x + (1, 3)[n], NX)})

    with jax.named_scope("w_b"):
        for i in (1, 3, 2):
            pull(block(0, i), 4, i)
            push(block(0, i), i, along_a)
    with jax.named_scope("w_xz"):
        column_relay(*rows_column)
    with jax.named_scope("w_oz"):
        column_relay(*weight_column)
        for d in (1, 7):
            await_recv(slot(weight_column[0], d), sem("oz", d), {"tp": other})
        spread_slots((0, 1, 7, 2, 6), 1)
    with jax.named_scope("w_xg"):
        for d in (1, 7):
            await_recv(slot(k["xs"], d), sem("x", d), {"tp": other})
        column_end(*rows_column)
    with jax.named_scope("w_oze"):
        column_end(*weight_column)
        spread_slots((3, 5, 4), 1)
        spread_slots((0, 1, 7, 2, 6, 3, 5, 4), 0)
    with jax.named_scope("w_aend"):
        for i in (0, 1, 3, 2):
            for d in (1, 3, 2):
                pull(block(d, i), i, d)

    def columns(kind):
        blocks = []
        for i in range(4):
            for j in range(4):
                blocks.append(k["wt"][kind, i + tp * (j - i), j + tp * (i - j)])
        return jnp.concatenate(blocks, axis=0)

    def project(rows_ref, kinds, width, ps, pr, ss, land, t, sends, lands, meanwhile):
        lhs = k[rows_ref][...].reshape(NZ * S, H)
        part = jnp.concatenate([dot(lhs, columns(kind), ((1,), (1,))) for kind in kinds], axis=1)

        @pl.when(tp != z // 4)
        def _():
            k[ps][...] = part.astype(BF)
            c = remote(k[ps], k[pr], k["p_s"].at[0], sem("t", t), {"tp": other})
            c.start()
            c.wait_send()

        @pl.when(tp == z // 4)
        def _():
            await_recv(k[pr], sem("t", t), {"tp": other})
            total = (part + k[pr][...].astype(F32)).astype(BF)
            k[ss][...] = total.reshape(NZ, S, width)
            mine = lax.rem(z, 4)
            for d in ORDER[8]:
                there = lax.rem(z + d, NZ)
                remote(k[ss].at[there], k[land].at[mine], k[sends].at[d], k[lands].at[mine], {"z": there}).start()
            k[land][mine] = k[ss][z]

        meanwhile()
        for i in range(4):
            @pl.when(4 * tp + i != z)
            def _():
                await_recv(k[land].at[i], k[lands].at[i], {"tp": other})

    def sends_done(ss, land, sends, lands):
        @pl.when(tp == z // 4)
        def _():
            for d in ORDER[8]:
                remote(k[ss].at[0], k[land].at[0], k[sends].at[d], k[lands].at[0], {"tp": other}).wait_send()

    def output_weight():
        with jax.named_scope("w_ox"):
            for d in (0, 1, 7, 2, 6):
                relay_slot(d)

    project("xs", (0, 1), 512, "ps", "pr", "ss", "ra", 1, "a_s", "a_r", output_weight)
    await_recv(k["qr"], sem("t", 0), {"tp": other})
    row_scale = lax.rsqrt((k["qs"][...] + k["qr"][...])[:, 0:1] / D + EPSILON)
    forward = (jnp.concatenate([k["ra"][i, :, 0:256] for i in range(4)], axis=1).astype(F32) * row_scale).astype(BF)
    branch = (jnp.concatenate([k["ra"][i, :, 256:512] for i in range(4)], axis=1).astype(F32) * row_scale).astype(BF)
    for i in range(9, 14):
        loads[i].wait()
    window = [k["cv"][0], k["cv"][1], k["cv"][2], forward]
    o_conv[0] = window[1]
    o_conv[1] = window[2]
    o_conv[2] = forward
    tap_rows = k["tv"][...].astype(F32)
    conv_out = sum(window[i].astype(F32) * tap_rows[i : i + 1] for i in range(4)).astype(BF)

    def gate_map(n):
        return jnp.concatenate([dot(conv_out[:, g * 256 : g * 256 + 256], k["bd"][n, g]) for g in range(4)], axis=1)

    recur_open = jax.nn.sigmoid(gate_map(0))
    inward = jax.nn.sigmoid(gate_map(1))
    logit = -k["dv"][...]
    softplus = jnp.maximum(logit, 0.0) + jnp.log1p(jnp.exp(-jnp.abs(logit)))
    log_decay = -DECAY_POWER * recur_open * softplus
    new_hidden = jnp.exp(log_decay) * k["hv"][...] + jnp.sqrt(-expm1(2.0 * log_decay)) * (
        inward * conv_out.astype(F32)
    )
    o_hidden[...] = new_hidden
    k["ms"][y] = (jax.nn.gelu(branch.astype(F32)) * new_hidden).astype(BF)
    for d in ORDER[4]:
        start(k["ms"].at[y], k["ms"].at[y], sem("m", d), {"y": lax.rem(y + d, NY)})
    with jax.named_scope("w_ox2"):
        for d in (3, 5, 4):
            relay_slot(d)
        for d in range(NZ):
            ref = k["wo"].at[lax.rem(x + 2, NX), lax.rem(z - d + NZ, NZ)]
            await_recv(ref, sem("ol", d), {"tp": other})
    with jax.named_scope("w_mg"):
        for d in ORDER[4]:
            await_recv(k["ms"].at[lax.rem(y - d + NY, NY)], sem("m", d), {"tp": other})
    lhs = k["ms"][...].reshape(NY * S, H)
    for h in range(2):
        out_columns = jnp.concatenate([k["wo"][j, 4 * h + i] for i in range(4) for j in range(NX)], axis=0)
        part = dot(lhs, out_columns, ((1,), (1,)))
        k["ps2"][:, h] = part.astype(BF).reshape(NY, S, 256)
    for d in ORDER[4] + (0,):
        there = lax.rem(y + d, NY)
        for n, core in enumerate((tp, other)):
            if d or n:
                where = {"y": there, "tp": core}
                start(k["ps2"].at[there], k["rb"].at[n, y], sem("b", n, d), where)
    k["rb"][0, y] = k["ps2"][y]
    with jax.named_scope("w_rb"):
        await_recv(k["svo"], sem("t", 3), {"tp": other})
        for d in ORDER[4] + (0,):
            for n in range(2):
                if d or n:
                    ref = k["rb"].at[n, lax.rem(y - d + NY, NY)]
                    await_recv(ref, sem("b", n, d), {"tp": other})

    def middle_of(ref, h):
        landed = k["rb"][0, :, h].astype(F32) + k["rb"][1, :, h].astype(F32)
        out_terms = jnp.concatenate(
            [landed[j, :, i * 64 : i * 64 + 64] for i in range(4) for j in range(NY)], axis=1
        )
        return (ref[...].astype(F32) + out_terms).astype(BF).astype(F32)

    mid_values = middle_of(k["sv"], tp)
    theirs_mid = middle_of(k["svo"], other)
    mid_power = sum(jnp.sum(m * m, axis=1, keepdims=True) for m in (mid_values, theirs_mid)) / D
    mid_scale = lax.rsqrt(mid_power + EPSILON)
    normed = (mid_values * mid_scale * k["g2v"][...]).astype(BF)

    stacked = jnp.concatenate([normed[:, q * LANES : (q + 1) * LANES] for q in range(Q)], axis=0)
    k["zsend"][...] = dot(k["pm"][...], stacked).astype(BF).reshape(NZ, NY, 16, LANES)
    for i in range(1, 8):
        there = lax.rem(z + ZORD[i], NZ)
        start(k["zsend"].at[there], k["zrecv"].at[i], sem("dz", i), {"z": there})
    k["zrecv"][0] = k["zsend"][z]

    def part_of(xi, yi, g, h=tp):
        return k["fb"].at[h, xi, yi, pl.ds(*GROUPS[g])]

    def wait_plane(xi, yi, g):
        if xi or yi:
            await_recv(part_of(xi, yi, g), sem("dp", g, xi, yi), {"tp": other})

    def send_core(xi, g):
        ref = k["fb"].at[tp, xi, :, pl.ds(*GROUPS[g])]
        start(ref, ref, sem("dt", xi, g), {"tp": other})

    for g, (low, count) in enumerate(GROUPS):
        with jax.named_scope(f"w_dz{g}"):
            for i in range(max(low, 1), low + count):
                await_recv(k["zrecv"].at[i], sem("dz", i), {"tp": other})
        for i, j in PLANE:
            there = lax.rem(y + XORD[j], NY)
            src = k["zrecv"].at[pl.ds(low, count), there]
            start(src, part_of(i, j, g), sem("dp", g, i, j), {"y": there, "x": lax.rem(x + XORD[i], NX)})
        k["fb"][tp, 0, 0, low : low + count] = k["zrecv"][low : low + count, y]
    for xi in range(3):
        for g in range(2):
            with jax.named_scope(f"w_dp{xi}{g}"):
                for yi in range(NY):
                    wait_plane(xi, yi, g)
            send_core(xi, g)
    with jax.named_scope("w_we"):
        for i in range(14, 19):
            loads[i].wait()

    turn = iota(square, 1) == iota(square, 0) % 16 * Q + iota(square, 0) // 16
    turn = jnp.where(turn, 1.0, 0.0).astype(BF)

    def to_rows(xi):
        with jax.named_scope(f"w_dt{xi}"):
            for g in range(2):
                ref = k["fb"].at[other, xi, :, pl.ds(*GROUPS[g])]
                await_recv(ref, sem("dt", xi, g), {"tp": other})
        for yi in range(NY):
            pair = jnp.concatenate([k["fb"][h, xi, yi].reshape(LANES, LANES) for h in range(2)], axis=1)
            turned = dot(turn, pair).astype(BF)
            at = (xi * NY + yi) * 16
            for q in range(Q):
                k["ab"][at : at + 16, q * 256 : q * 256 + 256] = turned[q * 16 : q * 16 + 16]

    def up(low, high):
        rows = k["ab"][low:high]
        gate_act = dot(rows, k["wg"][...].reshape(D, FD))
        upper = dot(rows, k["wu"][...].reshape(D, FD))
        k["ib"][low:high] = (jax.nn.silu(gate_act) * upper).astype(BF)

    theirs = pl.ds(pl.multiple_of(other * H, H), H)
    ours = pl.ds(pl.multiple_of(tp * H, H), H)

    def down(xi):
        inner = k["ib"][xi * 64 : xi * 64 + 64]
        k["hs"][xi] = dot(inner, k["wd"][:, theirs]).astype(BF)
        start(k["hs"].at[xi], k["hr"].at[xi], sem("ht", xi), {"tp": other})
        k["own"][xi] = dot(inner, k["wd"][:, ours])

    def whole(xi):
        with jax.named_scope(f"w_ht{xi}"):
            await_recv(k["hr"].at[xi], sem("ht", xi), {"tp": other})
        return k["own"][xi] + k["hr"][xi].astype(F32)

    def send_sum(xi):
        total = whole(xi)
        for yi in (3, 2, 1, 0):
            if xi or yi:
                k["xsend"][xi, yi] = total[yi * 16 : yi * 16 + 16].astype(BF)
                where = {"y": lax.rem(y - XORD[yi] + NY, NY), "x": lax.rem(x - XORD[xi] + NX, NX)}
                start(k["xsend"].at[xi, yi], k["xrecv"].at[xi, yi], sem("rx", xi, yi), where)
        return total[:16]

    for xi in range(3):
        to_rows(xi)
    up(0, 192)
    with jax.named_scope("w_dxl"):
        for g in range(2):
            for yi in range(NY):
                wait_plane(3, yi, g)
            send_core(3, g)
    down(1)
    down(2)
    to_rows(3)
    up(192, 256)
    down(3)
    send_sum(1)
    send_sum(2)
    send_sum(3)
    down(0)
    home = send_sum(0)
    back = iota(square, 0) == iota(square, 1) % 16 * Q + iota(square, 1) // 16
    back = jnp.where(back, 1.0, 0.0).astype(BF)
    for half in (1, 0):
        for yi in (2 * half + 1, 2 * half):
            with jax.named_scope(f"w_rx{yi}"):
                for xi in range(0 if yi else 1, NX):
                    await_recv(k["xrecv"].at[xi, yi], sem("rx", xi, yi), {"tp": other})
            rows = sum(k["xrecv"][xi, yi].astype(F32) for xi in range(1, NX))
            rows = (rows + (k["xrecv"][0, yi].astype(F32) if yi else home)).astype(BF)
            part = jnp.concatenate([rows[:, q * LANES : (q + 1) * LANES] for q in range(Q)], axis=0)
            k["ry"][yi] = dot(back, part).astype(BF).reshape(NZ, 16, LANES)
        pair = pl.ds(2 * half, 2)
        for i in range(7, 0, -1):
            there = lax.rem(z - ZORD[i] + NZ, NZ)
            start(
                k["ry"].at[pair, i], k["rz"].at[z, pair], sem("rz", half, i), {"z": there}
            )
        k["rz"][z, 2 * half : 2 * half + 2] = k["ry"][2 * half : 2 * half + 2, 0]
    with jax.named_scope("w_rz"):
        for half in (1, 0):
            pair = pl.ds(2 * half, 2)
            for i in range(1, 8):
                ref = k["rz"].at[lax.rem(z + ZORD[i], NZ), pair]
                await_recv(ref, sem("rz", half, i), {"tp": other})
    returned = k["rz"][...].reshape(EXPERTS * 16, LANES).astype(F32)
    mix = dot(k["pw"][...], returned, ((0,), (0,)), HIGHEST)
    expert_mix = jnp.concatenate([mix[q * S : (q + 1) * S] for q in range(Q)], axis=1)
    o_stream[...] = (mid_values + expert_mix).astype(BF)
    for n in range(2):
        for d in range(8):
            ref = k["wo"].at[x, 0]
            remote(ref, ref, k["spread"].at[n, d], sem("ox", n, d), {"tp": other}).wait_send()
    for c in sent[-SENDS:]:
        c.wait_send()
    sends_done("ss", "ra", "a_s", "a_r")


def handed_on(*refs):
    for src, dst in zip(refs[:3], refs[3:]):
        dst[...] = src[...]


def per_device(
    stream, hidden_state, conv_state, first_gain, input_weight, branch_weight, conv_taps, recur_gate, input_gate,
    decay_logit, output_weight, second_gain, routes, route_weight, expert_gate, expert_up, expert_down,
):
    shapes = scratch_shapes()
    vmem = pl.BlockSpec(memory_space=pltpu.VMEM)
    anywhere = pl.BlockSpec(memory_space=pl.ANY)
    outs = pl.pallas_call(
        kernel,
        name="layer",
        out_shape=(
            jax.ShapeDtypeStruct((S, H), BF),
            jax.ShapeDtypeStruct((S, H), F32),
            jax.ShapeDtypeStruct((3, S, H), BF),
        ),
        in_specs=[anywhere] * 17,
        out_specs=(vmem,) * 3,
        scratch_shapes=[shapes[n] for n in NAMES],
        compiler_params=pltpu.CompilerParams(
            collective_id=0, has_side_effects=True, vmem_limit_bytes=60 * 1024 * 1024
        ),
    )(
        stream,
        hidden_state,
        conv_state.transpose(1, 0, 2),
        first_gain.reshape(1, H),
        input_weight.T,
        branch_weight.T,
        conv_taps,
        recur_gate.reshape(H, 64),
        input_gate.reshape(H, 64),
        decay_logit.reshape(1, H),
        output_weight.T,
        second_gain.reshape(1, H),
        routes.T,
        route_weight.T,
        expert_gate.reshape(2, Q, LANES, FD),
        expert_up.reshape(2, Q, LANES, FD),
        expert_down,
    )
    new_stream, new_hidden, new_conv = pl.pallas_call(
        handed_on,
        name="handed_on",
        out_shape=tuple(jax.ShapeDtypeStruct(o.shape, o.dtype) for o in outs),
        in_specs=[vmem] * 3,
        out_specs=(vmem,) * 3,
    )(*outs)
    return new_stream, new_hidden, new_conv.transpose(1, 0, 2)


def solution(mesh):
    torus = Mesh(mesh.devices.reshape(NZ, NY, NX, mesh.shape["tp"]), EP_TP)
    in_specs = (
        P(EP, "tp"),
        P(EP, "tp"),
        P(EP, None, "tp"),
        P("tp"),
        P("tp", EP),
        P("tp", EP),
        P(None, "tp"),
        P("tp", None, None),
        P("tp", None, None),
        P("tp"),
        P("tp", EP),
        P("tp"),
        P(EP, None),
        P(EP, None),
        P(None, EP_TP),
        P(None, EP_TP),
        P(EP_TP, None),
    )
    out_specs = (P(EP, "tp"), P(EP, "tp"), P(EP, None, "tp"))
    return jax.shard_map(per_device, mesh=torus, in_specs=in_specs, out_specs=out_specs, check_vma=False)
```

```python
import jax
import jax.numpy as jnp
from jax import lax
from jax.experimental import pallas as pl
from jax.experimental.pallas import tpu as pltpu
from jax.sharding import Mesh
from jax.sharding import PartitionSpec as P

EP = ("z", "y", "x")
EP_TP = ("z", "y", "x", "tp")
MESH = pl.DeviceIdType.MESH
NZ, NY, NX = 8, 4, 4
ORDER = {8: (4, 3, 5, 2, 6, 1, 7), 4: (2, 1, 3)}
ZORD, XORD = (0, 1, 7, 2, 6, 3, 5, 4), (0, 1, 3, 2)
GROUPS = ((0, 5), (5, 3))
PLANE = tuple((i, j) for i in (3, 2, 1, 0) for j in (3, 2, 1, 0) if i or j)
BF, F32 = jnp.bfloat16, jnp.float32
EPSILON = 1e-6
DECAY_POWER = 8.0
S, H, D, FD = 16, 1024, 2048, 384
LANES, Q = 128, 8
EXPERTS, CAP = 32, 2
HIGHEST = lax.Precision.HIGHEST


SENDS = 32


def semaphores():
    first = {
        "load": [(i,) for i in range(19)],
        "t": [(i,) for i in range(4)],
        "w": [(i, d) for i in range(5) for d in (1, 2, 3)],
        "x": [(d,) for d in range(8)],
        "oz": [(d,) for d in range(8)],
        "ox": [(n, d) for n in range(2) for d in range(8)],
        "ol": [(d,) for d in range(8)],
        "m": [(d,) for d in (1, 2, 3)],
        "b": [(n, d) for n in range(2) for d in range(4) if n or d],
        "more": [(i,) for i in range(5)],
    }
    at = {}
    for name, indices in first.items():
        for index in indices:
            at[(name, *index)] = len(at)
    count = len(at)

    def share(keys, *names):
        free = [at[(name, *index)] for name in names for index in first[name]]
        for key, i in zip(keys, free, strict=False):
            at[key] = i
        return free[len(keys) :]

    groups, halves = (0, 1), (0, 1)
    left = share([("dz", i) for i in range(1, 8)], "w")
    for key, i in zip([("dt", xi, g) for xi in range(4) for g in groups], left, strict=True):
        at[key] = i
    plane = [(xi, yi) for xi in range(4) for yi in range(4) if xi or yi]
    share([("dp", g, *at_plane) for g in groups for at_plane in plane], "x", "oz", "more", "load")
    back = [("ht", xi) for xi in range(4)] + [("rx", *at_plane) for at_plane in plane]
    back += [("rz", half, i) for half in halves for i in range(1, 8)]
    share(back, "ox", "ol", "m", "b")
    return at, count


AT, COUNT = semaphores()


def scratch_shapes():
    vm, dma = pltpu.VMEM, pltpu.SemaphoreType.DMA
    return dict(
        sv=vm((S, H), BF),
        hv=vm((S, H), F32),
        cv=vm((3, S, H), BF),
        g1v=vm((1, H), F32),
        tv=vm((4, H), BF),
        rgv=vm((H, 64), BF),
        igv=vm((H, 64), BF),
        dv=vm((1, H), F32),
        g2v=vm((1, H), F32),
        rtv=vm((2, S), jnp.int32),
        rwv=vm((2, S), F32),
        wg=vm((Q, 2, LANES, FD), BF),
        wu=vm((Q, 2, LANES, FD), BF),
        wd=vm((FD, D), BF),
        xs=vm((NZ, S, H), BF),
        ms=vm((NY, S, H), BF),
        wt=vm((2, 4, 4, S, H), BF),
        wo=vm((NX, NZ, S, H), BF),
        ps=vm((NZ * S, 512), BF),
        pr=vm((NZ * S, 512), BF),
        ss=vm((NZ, S, 512), BF),
        ra=vm((4, S, 512), BF),
        ps2=vm((NY, 2, S, 256), BF),
        svo=vm((S, H), BF),
        rb=vm((2, NY, 2, S, 256), BF),
        qs=vm((S, LANES), F32),
        qr=vm((S, LANES), F32),
        bd=vm((2, 4, 256, 256), BF),
        pm=vm((EXPERTS * 16, LANES), BF),
        pw=vm((EXPERTS * 16, LANES), F32),
        zsend=vm((NZ, NY, 16, LANES), BF),
        zrecv=vm((NZ, NY, 16, LANES), BF),
        fb=vm((2, NX, NY, NZ, 16, LANES), BF),
        ab=vm((256, D), BF),
        ib=vm((256, FD), BF),
        hs=vm((NX, 64, H), BF),
        hr=vm((NX, 64, H), BF),
        own=vm((NX, 64, H), F32),
        xsend=vm((NX, NY, 16, H), BF),
        xrecv=vm((NX, NY, 16, H), BF),
        ry=vm((NY, NZ, 16, LANES), BF),
        rz=vm((NZ, NY, 16, LANES), BF),
        sends=dma((SENDS,)),
        spread=dma((2, 8)),
        a_s=dma((8,)),
        a_r=dma((4,)),
        p_s=dma((1,)),
        r=dma((COUNT,)),
    )


NAMES = tuple(scratch_shapes())


def dot(a, b, dims=((1,), (0,)), precision=None):
    return lax.dot_general(a, b, (dims, ((), ())), precision=precision, preferred_element_type=F32)


def iota(shape, dim):
    return lax.broadcasted_iota(jnp.int32, shape, dim)


def expm1(v):
    series = 1.0 + v * (1.0 / 9.0)
    for n in range(8, 1, -1):
        series = 1.0 + v * (1.0 / n) * series
    return jnp.where(v > -0.5, v * series, jnp.exp(v) - 1.0)


def remote(src, dst, ssem, rsem, where):
    return pltpu.make_async_remote_copy(
        src_ref=src, dst_ref=dst, send_sem=ssem, recv_sem=rsem, device_id=where, device_id_type=MESH
    )


def kernel(*refs):
    (stream, hidden, conv, gain1, w_in, w_br, taps, rg, ig, decay, w_out, gain2, routes, rw, eg, eu, ed) = refs[:17]
    o_stream, o_hidden, o_conv = refs[17:20]
    k = dict(zip(NAMES, refs[20:]))
    z, y, x, tp = (lax.axis_index(a) for a in EP_TP)
    other = 1 - tp
    sent = []

    barrier = pltpu.get_barrier_semaphore()
    for d in ORDER[8]:
        pl.semaphore_signal(barrier, inc=1, device_id={"z": lax.rem(z + d, NZ)}, device_id_type=MESH)
    for i, j in PLANE:
        there = {"y": lax.rem(y + XORD[j], NY), "x": lax.rem(x + XORD[i], NX)}
        pl.semaphore_signal(barrier, inc=1, device_id=there, device_id_type=MESH)
    for d in ORDER[4]:
        there = {"y": lax.rem(y + d, NY), "tp": other}
        pl.semaphore_signal(barrier, inc=1, device_id=there, device_id_type=MESH)
    pl.semaphore_signal(barrier, inc=1, device_id={"tp": other}, device_id_type=MESH)

    a = y + tp * (x - y)
    b = x + tp * (y - x)
    plan = [
        (stream, k["sv"]), (gain1, k["g1v"]),
        (w_in, k["wt"].at[0, a, b]), (w_br, k["wt"].at[1, a, b]), (w_out, k["wo"].at[x, z]),
        (rg, k["rgv"]), (ig, k["igv"]), (routes, k["rtv"]), (rw, k["rwv"]),
        (conv, k["cv"]), (taps, k["tv"]), (decay, k["dv"]), (hidden, k["hv"]), (gain2, k["g2v"]),
        (eg.at[0], k["wg"].at[:, 0]), (eg.at[1], k["wg"].at[:, 1]),
        (eu.at[0], k["wu"].at[:, 0]), (eu.at[1], k["wu"].at[:, 1]), (ed, k["wd"]),
    ]
    loads = [pltpu.make_async_copy(s, t, k["r"].at[AT[("load", i)]]) for i, (s, t) in enumerate(plan)]
    for c in loads:
        c.start()

    def sem(name, *index):
        return k["r"].at[AT[(name, *index)]]

    def start(src, dst, rsem, where):
        n = len(sent)
        if n >= SENDS:
            sent[n - SENDS].wait_send()
        c = remote(src, dst, k["sends"].at[n % SENDS], rsem, where)
        c.start()
        sent.append(c)

    def await_recv(ref, rsem, where):
        remote(ref, ref, k["sends"].at[0], rsem, where).wait_recv()

    loads[0].wait()
    loads[1].wait()
    values = k["sv"][...].astype(F32)
    k["xs"][z] = (values * k["g1v"][...]).astype(BF)
    k["qs"][...] = jnp.broadcast_to(jnp.sum(values * values, axis=1, keepdims=True), (S, LANES))
    loads[5].wait()
    loads[6].wait()
    eye = (iota((64, 256), 1) % 64 == iota((64, 256), 0)).astype(BF)
    on = iota((H, 256), 0) // 64 % 4 == iota((H, 256), 1) // 64
    for n, ref in enumerate((k["rgv"], k["igv"])):
        k["bd"][n] = jnp.where(on, dot(ref[...], eye), 0.0).astype(BF).reshape(4, 256, 256)

    loads[7].wait()
    loads[8].wait()
    spread = (iota((S, LANES), 1) % S == iota((S, LANES), 0)).astype(F32)
    named = dot(k["rtv"][...].astype(F32), spread, precision=HIGHEST)
    weights = dot(k["rwv"][...], spread, precision=HIGHEST)
    rows = (EXPERTS * 16, LANES)
    expert = (iota(rows, 0) // 16).astype(F32)
    hit0, hit1 = named[0:1] == expert, named[1:2] == expert
    hits = jnp.where(hit0 | hit1, 1.0, 0.0)
    square = (LANES, LANES)
    before = (iota(square, 0) < iota(square, 1) % S).astype(BF)
    rank = dot(hits.astype(BF), before)
    slot = (iota(rows, 0) // Q % CAP).astype(F32)
    same = iota(rows, 0) % Q == iota(rows, 1) // S
    chosen = (hits > 0.5) & (rank == slot) & same
    k["pm"][...] = jnp.where(chosen, 1.0, 0.0).astype(BF)
    step = iota(rows, 0) // 16 % 4
    step = jnp.where(step == 2, 3, jnp.where(step == 3, 2, step))
    expert = (iota(rows, 0) // 64 * 4 + (y + step) % 4).astype(F32)
    hit0, hit1 = named[0:1] == expert, named[1:2] == expert
    hits = jnp.where(hit0 | hit1, 1.0, 0.0)
    chosen = (hits > 0.5) & (dot(hits.astype(BF), before) == slot) & same
    k["pw"][...] = jnp.where(chosen, jnp.where(hit0, weights[0:1], weights[1:2]), 0.0)

    for i in (2, 3, 4):
        loads[i].wait()
    with jax.named_scope("w_bar"):
        pl.semaphore_wait(barrier, 26)

    def along_b(d):
        return {"y": lax.rem(y + d * tp, NY), "x": lax.rem(x + d * other, NX)}

    def along_a(d):
        return {"y": lax.rem(y + d * other, NY), "x": lax.rem(x + d * tp, NX)}

    both = pl.ds(0, 2)

    def block(da, db):
        return k["wt"].at[both, lax.rem(a - da + 4, 4), lax.rem(b - db + 4, 4)]

    def push(ref, i, along):
        for d in ORDER[4]:
            start(ref, ref, sem("w", i, d), along(d))

    def pull(ref, i, d):
        await_recv(ref, sem("w", i, d), {"tp": other})

    push(block(0, 0), 4, along_b)
    push(block(0, 0), 0, along_a)
    near = (2, 6, 1, 7)
    lanes = (pl.ds(0, H // 2), pl.ds(H // 2, H // 2))

    def along_z(d):
        return {"z": lax.rem(z + d, NZ)}

    def slot(ref, d):
        return ref.at[lax.rem(z - d + NZ, NZ)]

    def column_send(ref, name):
        for d in near:
            start(ref.at[z], ref.at[z], sem(name, d), along_z(d))

    def column_relay(ref, name):
        for n, d in enumerate((2, 6)):
            got, piece = slot(ref, d), slot(ref, d).at[:, lanes[n]]
            await_recv(got, sem(name, d), {"tp": other})
            start(piece, piece, sem(name, (0, 4)[n]), along_z(d))
            start(got, got, sem(name, (3, 5)[n]), along_z((1, 7)[n]))

    def column_end(ref, name):
        for d in (3, 5):
            await_recv(slot(ref, d), sem(name, d), {"tp": other})
        for n in range(2):
            await_recv(slot(ref, 4).at[:, lanes[n]], sem(name, (0, 4)[n]), {"tp": other})

    rows_column = (k["xs"], "x")
    weight_column = (k["wo"].at[x], "oz")
    column_send(*rows_column)
    start(k["qs"], k["qr"], sem("t", 0), {"tp": other})
    start(k["sv"], k["svo"], sem("t", 3), {"tp": other})
    column_send(*weight_column)
    def spread_slots(ds, core):
        copies = []
        for d in ds:
            for n in range(2):
                ref, where = k["wo"].at[x, lax.rem(z - d + NZ, NZ)], {"x": lax.rem(x + (1, 3)[n], NX)}
                copies.append(remote(ref, ref, k["spread"].at[n, d], sem("ox", n, d), where))

        @pl.when(tp == core)
        def _():
            for c in copies:
                c.start()

        return copies

    def relay_slot(d):
        for n in range(2):
            ref = k["wo"].at[lax.rem(x + (3, 1)[n], NX), lax.rem(z - d + NZ, NZ)]
            await_recv(ref, sem("ox", n, d), {"tp": other})
            if n == (d in (3, 4, 5, 6)):
                start(ref, ref, sem("ol", d), {"x": lax.rem(x + (1, 3)[n], NX)})

    with jax.named_scope("w_b"):
        for i in (1, 3, 2):
            pull(block(0, i), 4, i)
            push(block(0, i), i, along_a)
    with jax.named_scope("w_xz"):
        column_relay(*rows_column)
    with jax.named_scope("w_oz"):
        column_relay(*weight_column)
        for d in (1, 7):
            await_recv(slot(weight_column[0], d), sem("oz", d), {"tp": other})
        spread_slots((0, 1, 7, 2, 6), 1)
    with jax.named_scope("w_xg"):
        for d in (1, 7):
            await_recv(slot(k["xs"], d), sem("x", d), {"tp": other})
        column_end(*rows_column)
    with jax.named_scope("w_oze"):
        column_end(*weight_column)
        spread_slots((3, 5, 4), 1)
        spread_slots((0, 1, 7, 2, 6, 3, 5, 4), 0)
    with jax.named_scope("w_aend"):
        for i in (0, 1, 3, 2):
            for d in (1, 3, 2):
                pull(block(d, i), i, d)

    def columns(kind):
        blocks = []
        for i in range(4):
            for j in range(4):
                blocks.append(k["wt"][kind, i + tp * (j - i), j + tp * (i - j)])
        return jnp.concatenate(blocks, axis=0)

    def project(rows_ref, kinds, width, ps, pr, ss, land, t, sends, lands, meanwhile):
        lhs = k[rows_ref][...].reshape(NZ * S, H)
        part = jnp.concatenate([dot(lhs, columns(kind), ((1,), (1,))) for kind in kinds], axis=1)

        @pl.when(tp != z // 4)
        def _():
            k[ps][...] = part.astype(BF)
            c = remote(k[ps], k[pr], k["p_s"].at[0], sem("t", t), {"tp": other})
            c.start()
            c.wait_send()

        @pl.when(tp == z // 4)
        def _():
            await_recv(k[pr], sem("t", t), {"tp": other})
            total = (part + k[pr][...].astype(F32)).astype(BF)
            k[ss][...] = total.reshape(NZ, S, width)
            mine = lax.rem(z, 4)
            for d in ORDER[8]:
                there = lax.rem(z + d, NZ)
                remote(k[ss].at[there], k[land].at[mine], k[sends].at[d], k[lands].at[mine], {"z": there}).start()
            k[land][mine] = k[ss][z]

        meanwhile()
        for i in range(4):
            @pl.when(4 * tp + i != z)
            def _():
                await_recv(k[land].at[i], k[lands].at[i], {"tp": other})

    def sends_done(ss, land, sends, lands):
        @pl.when(tp == z // 4)
        def _():
            for d in ORDER[8]:
                remote(k[ss].at[0], k[land].at[0], k[sends].at[d], k[lands].at[0], {"tp": other}).wait_send()

    def output_weight():
        with jax.named_scope("w_ox"):
            for d in (0, 1, 7, 2, 6):
                relay_slot(d)

    project("xs", (0, 1), 512, "ps", "pr", "ss", "ra", 1, "a_s", "a_r", output_weight)
    await_recv(k["qr"], sem("t", 0), {"tp": other})
    row_scale = lax.rsqrt((k["qs"][...] + k["qr"][...])[:, 0:1] / D + EPSILON)
    forward = (jnp.concatenate([k["ra"][i, :, 0:256] for i in range(4)], axis=1).astype(F32) * row_scale).astype(BF)
    branch = (jnp.concatenate([k["ra"][i, :, 256:512] for i in range(4)], axis=1).astype(F32) * row_scale).astype(BF)
    for i in range(9, 14):
        loads[i].wait()
    window = [k["cv"][0], k["cv"][1], k["cv"][2], forward]
    o_conv[0] = window[1]
    o_conv[1] = window[2]
    o_conv[2] = forward
    tap_rows = k["tv"][...].astype(F32)
    conv_out = sum(window[i].astype(F32) * tap_rows[i : i + 1] for i in range(4)).astype(BF)

    def gate_map(n):
        return jnp.concatenate([dot(conv_out[:, g * 256 : g * 256 + 256], k["bd"][n, g]) for g in range(4)], axis=1)

    recur_open = jax.nn.sigmoid(gate_map(0))
    inward = jax.nn.sigmoid(gate_map(1))
    logit = -k["dv"][...]
    softplus = jnp.maximum(logit, 0.0) + jnp.log1p(jnp.exp(-jnp.abs(logit)))
    log_decay = -DECAY_POWER * recur_open * softplus
    new_hidden = jnp.exp(log_decay) * k["hv"][...] + jnp.sqrt(-expm1(2.0 * log_decay)) * (
        inward * conv_out.astype(F32)
    )
    o_hidden[...] = new_hidden
    k["ms"][y] = (jax.nn.gelu(branch.astype(F32)) * new_hidden).astype(BF)
    for d in ORDER[4]:
        start(k["ms"].at[y], k["ms"].at[y], sem("m", d), {"y": lax.rem(y + d, NY)})
    with jax.named_scope("w_ox2"):
        for d in (3, 5, 4):
            relay_slot(d)
        for d in range(NZ):
            ref = k["wo"].at[lax.rem(x + 2, NX), lax.rem(z - d + NZ, NZ)]
            await_recv(ref, sem("ol", d), {"tp": other})
    with jax.named_scope("w_mg"):
        for d in ORDER[4]:
            await_recv(k["ms"].at[lax.rem(y - d + NY, NY)], sem("m", d), {"tp": other})
    lhs = k["ms"][...].reshape(NY * S, H)
    for h in range(2):
        out_columns = jnp.concatenate([k["wo"][j, 4 * h + i] for i in range(4) for j in range(NX)], axis=0)
        part = dot(lhs, out_columns, ((1,), (1,)))
        k["ps2"][:, h] = part.astype(BF).reshape(NY, S, 256)
    for d in ORDER[4] + (0,):
        there = lax.rem(y + d, NY)
        for n, core in enumerate((tp, other)):
            if d or n:
                where = {"y": there, "tp": core}
                start(k["ps2"].at[there], k["rb"].at[n, y], sem("b", n, d), where)
    k["rb"][0, y] = k["ps2"][y]
    with jax.named_scope("w_rb"):
        await_recv(k["svo"], sem("t", 3), {"tp": other})
        for d in ORDER[4] + (0,):
            for n in range(2):
                if d or n:
                    ref = k["rb"].at[n, lax.rem(y - d + NY, NY)]
                    await_recv(ref, sem("b", n, d), {"tp": other})

    def middle_of(ref, h):
        landed = k["rb"][0, :, h].astype(F32) + k["rb"][1, :, h].astype(F32)
        out_terms = jnp.concatenate(
            [landed[j, :, i * 64 : i * 64 + 64] for i in range(4) for j in range(NY)], axis=1
        )
        return (ref[...].astype(F32) + out_terms).astype(BF).astype(F32)

    mid_values = middle_of(k["sv"], tp)
    theirs_mid = middle_of(k["svo"], other)
    mid_power = sum(jnp.sum(m * m, axis=1, keepdims=True) for m in (mid_values, theirs_mid)) / D
    mid_scale = lax.rsqrt(mid_power + EPSILON)
    normed = (mid_values * mid_scale * k["g2v"][...]).astype(BF)

    stacked = jnp.concatenate([normed[:, q * LANES : (q + 1) * LANES] for q in range(Q)], axis=0)
    k["zsend"][...] = dot(k["pm"][...], stacked).astype(BF).reshape(NZ, NY, 16, LANES)
    for i in range(1, 8):
        there = lax.rem(z + ZORD[i], NZ)
        start(k["zsend"].at[there], k["zrecv"].at[i], sem("dz", i), {"z": there})
    k["zrecv"][0] = k["zsend"][z]

    def part_of(xi, yi, g, h=tp):
        return k["fb"].at[h, xi, yi, pl.ds(*GROUPS[g])]

    def wait_plane(xi, yi, g):
        if xi or yi:
            await_recv(part_of(xi, yi, g), sem("dp", g, xi, yi), {"tp": other})

    def send_core(xi, g):
        ref = k["fb"].at[tp, xi, :, pl.ds(*GROUPS[g])]
        start(ref, ref, sem("dt", xi, g), {"tp": other})

    for g, (low, count) in enumerate(GROUPS):
        with jax.named_scope(f"w_dz{g}"):
            for i in range(max(low, 1), low + count):
                await_recv(k["zrecv"].at[i], sem("dz", i), {"tp": other})
        for i, j in PLANE:
            there = lax.rem(y + XORD[j], NY)
            src = k["zrecv"].at[pl.ds(low, count), there]
            start(src, part_of(i, j, g), sem("dp", g, i, j), {"y": there, "x": lax.rem(x + XORD[i], NX)})
        k["fb"][tp, 0, 0, low : low + count] = k["zrecv"][low : low + count, y]
    for xi in range(3):
        for g in range(2):
            with jax.named_scope(f"w_dp{xi}{g}"):
                for yi in range(NY):
                    wait_plane(xi, yi, g)
            send_core(xi, g)
    with jax.named_scope("w_we"):
        for i in range(14, 19):
            loads[i].wait()

    turn = iota(square, 1) == iota(square, 0) % 16 * Q + iota(square, 0) // 16
    turn = jnp.where(turn, 1.0, 0.0).astype(BF)

    def to_rows(xi):
        with jax.named_scope(f"w_dt{xi}"):
            for g in range(2):
                ref = k["fb"].at[other, xi, :, pl.ds(*GROUPS[g])]
                await_recv(ref, sem("dt", xi, g), {"tp": other})
        for yi in range(NY):
            pair = jnp.concatenate([k["fb"][h, xi, yi].reshape(LANES, LANES) for h in range(2)], axis=1)
            turned = dot(turn, pair).astype(BF)
            at = (xi * NY + yi) * 16
            for q in range(Q):
                k["ab"][at : at + 16, q * 256 : q * 256 + 256] = turned[q * 16 : q * 16 + 16]

    def up(low, high):
        rows = k["ab"][low:high]
        gate_act = dot(rows, k["wg"][...].reshape(D, FD))
        upper = dot(rows, k["wu"][...].reshape(D, FD))
        k["ib"][low:high] = (jax.nn.silu(gate_act) * upper).astype(BF)

    theirs = pl.ds(pl.multiple_of(other * H, H), H)
    ours = pl.ds(pl.multiple_of(tp * H, H), H)

    def down(xi):
        inner = k["ib"][xi * 64 : xi * 64 + 64]
        k["hs"][xi] = dot(inner, k["wd"][:, theirs]).astype(BF)
        start(k["hs"].at[xi], k["hr"].at[xi], sem("ht", xi), {"tp": other})
        k["own"][xi] = dot(inner, k["wd"][:, ours])

    def whole(xi):
        with jax.named_scope(f"w_ht{xi}"):
            await_recv(k["hr"].at[xi], sem("ht", xi), {"tp": other})
        return k["own"][xi] + k["hr"][xi].astype(F32)

    def send_sum(xi):
        total = whole(xi)
        for yi in (3, 2, 1, 0):
            if xi or yi:
                k["xsend"][xi, yi] = total[yi * 16 : yi * 16 + 16].astype(BF)
                where = {"y": lax.rem(y - XORD[yi] + NY, NY), "x": lax.rem(x - XORD[xi] + NX, NX)}
                start(k["xsend"].at[xi, yi], k["xrecv"].at[xi, yi], sem("rx", xi, yi), where)
        return total[:16]

    for xi in range(3):
        to_rows(xi)
    up(0, 192)
    with jax.named_scope("w_dxl"):
        for g in range(2):
            for yi in range(NY):
                wait_plane(3, yi, g)
            send_core(3, g)
    down(1)
    down(2)
    to_rows(3)
    up(192, 256)
    send_sum(1)
    send_sum(2)
    down(3)
    send_sum(3)
    down(0)
    home = send_sum(0)
    back = iota(square, 0) == iota(square, 1) % 16 * Q + iota(square, 1) // 16
    back = jnp.where(back, 1.0, 0.0).astype(BF)
    for half in (1, 0):
        for yi in (2 * half + 1, 2 * half):
            with jax.named_scope(f"w_rx{yi}"):
                for xi in range(0 if yi else 1, NX):
                    await_recv(k["xrecv"].at[xi, yi], sem("rx", xi, yi), {"tp": other})
            rows = sum(k["xrecv"][xi, yi].astype(F32) for xi in range(1, NX))
            rows = (rows + (k["xrecv"][0, yi].astype(F32) if yi else home)).astype(BF)
            part = jnp.concatenate([rows[:, q * LANES : (q + 1) * LANES] for q in range(Q)], axis=0)
            k["ry"][yi] = dot(back, part).astype(BF).reshape(NZ, 16, LANES)
        pair = pl.ds(2 * half, 2)
        for i in range(7, 0, -1):
            there = lax.rem(z - ZORD[i] + NZ, NZ)
            start(
                k["ry"].at[pair, i], k["rz"].at[z, pair], sem("rz", half, i), {"z": there}
            )
        k["rz"][z, 2 * half : 2 * half + 2] = k["ry"][2 * half : 2 * half + 2, 0]
    with jax.named_scope("w_rz"):
        for half in (1, 0):
            pair = pl.ds(2 * half, 2)
            for i in range(1, 8):
                ref = k["rz"].at[lax.rem(z + ZORD[i], NZ), pair]
                await_recv(ref, sem("rz", half, i), {"tp": other})
    returned = k["rz"][...].reshape(EXPERTS * 16, LANES).astype(F32)
    mix = dot(k["pw"][...], returned, ((0,), (0,)), HIGHEST)
    expert_mix = jnp.concatenate([mix[q * S : (q + 1) * S] for q in range(Q)], axis=1)
    o_stream[...] = (mid_values + expert_mix).astype(BF)
    for n in range(2):
        for d in range(8):
            ref = k["wo"].at[x, 0]
            remote(ref, ref, k["spread"].at[n, d], sem("ox", n, d), {"tp": other}).wait_send()
    for c in sent[-SENDS:]:
        c.wait_send()
    sends_done("ss", "ra", "a_s", "a_r")


def handed_on(*refs):
    for src, dst in zip(refs[:3], refs[3:]):
        dst[...] = src[...]


def per_device(
    stream, hidden_state, conv_state, first_gain, input_weight, branch_weight, conv_taps, recur_gate, input_gate,
    decay_logit, output_weight, second_gain, routes, route_weight, expert_gate, expert_up, expert_down,
):
    shapes = scratch_shapes()
    vmem = pl.BlockSpec(memory_space=pltpu.VMEM)
    anywhere = pl.BlockSpec(memory_space=pl.ANY)
    outs = pl.pallas_call(
        kernel,
        name="layer",
        out_shape=(
            jax.ShapeDtypeStruct((S, H), BF),
            jax.ShapeDtypeStruct((S, H), F32),
            jax.ShapeDtypeStruct((3, S, H), BF),
        ),
        in_specs=[anywhere] * 17,
        out_specs=(vmem,) * 3,
        scratch_shapes=[shapes[n] for n in NAMES],
        compiler_params=pltpu.CompilerParams(
            collective_id=0, has_side_effects=True, vmem_limit_bytes=60 * 1024 * 1024
        ),
    )(
        stream,
        hidden_state,
        conv_state.transpose(1, 0, 2),
        first_gain.reshape(1, H),
        input_weight.T,
        branch_weight.T,
        conv_taps,
        recur_gate.reshape(H, 64),
        input_gate.reshape(H, 64),
        decay_logit.reshape(1, H),
        output_weight.T,
        second_gain.reshape(1, H),
        routes.T,
        route_weight.T,
        expert_gate.reshape(2, Q, LANES, FD),
        expert_up.reshape(2, Q, LANES, FD),
        expert_down,
    )
    new_stream, new_hidden, new_conv = pl.pallas_call(
        handed_on,
        name="handed_on",
        out_shape=tuple(jax.ShapeDtypeStruct(o.shape, o.dtype) for o in outs),
        in_specs=[vmem] * 3,
        out_specs=(vmem,) * 3,
    )(*outs)
    return new_stream, new_hidden, new_conv.transpose(1, 0, 2)


def solution(mesh):
    torus = Mesh(mesh.devices.reshape(NZ, NY, NX, mesh.shape["tp"]), EP_TP)
    in_specs = (
        P(EP, "tp"),
        P(EP, "tp"),
        P(EP, None, "tp"),
        P("tp"),
        P("tp", EP),
        P("tp", EP),
        P(None, "tp"),
        P("tp", None, None),
        P("tp", None, None),
        P("tp"),
        P("tp", EP),
        P("tp"),
        P(EP, None),
        P(EP, None),
        P(None, EP_TP),
        P(None, EP_TP),
        P(EP_TP, None),
    )
    out_specs = (P(EP, "tp"), P(EP, "tp"), P(EP, None, "tp"))
    return jax.shard_map(per_device, mesh=torus, in_specs=in_specs, out_specs=out_specs, check_vma=False)
```

```python
import jax
import jax.numpy as jnp
from jax import lax
from jax.experimental import pallas as pl
from jax.experimental.pallas import tpu as pltpu
from jax.sharding import Mesh
from jax.sharding import PartitionSpec as P

EP = ("z", "y", "x")
EP_TP = ("z", "y", "x", "tp")
MESH = pl.DeviceIdType.MESH
NZ, NY, NX = 8, 4, 4
ORDER = {8: (1, 7, 2, 6, 3, 5, 4), 4: (2, 1, 3)}
ZORD, XORD = (0, 1, 7, 2, 6, 3, 5, 4), (0, 1, 3, 2)
GROUPS = ((0, 5), (5, 3))
PLANE = tuple((i, j) for i in (3, 2, 1, 0) for j in (3, 2, 1, 0) if i or j)
BF, F32 = jnp.bfloat16, jnp.float32
EPSILON = 1e-6
DECAY_POWER = 8.0
S, H, D, FD = 16, 1024, 2048, 384
LANES, Q = 128, 8
EXPERTS, CAP = 32, 2
HIGHEST = lax.Precision.HIGHEST


SENDS = 32


def semaphores():
    first = {
        "load": [(i,) for i in range(19)],
        "t": [(i,) for i in range(4)],
        "w": [(i, d) for i in range(5) for d in (1, 2, 3)],
        "x": [(d,) for d in range(8)],
        "oz": [(d,) for d in range(8)],
        "ox": [(n, d) for n in range(2) for d in range(8)],
        "ol": [(d,) for d in range(8)],
        "m": [(d,) for d in (1, 2, 3)],
        "b": [(n, d) for n in range(2) for d in range(4) if n or d],
        "more": [(i,) for i in range(5)],
    }
    at = {}
    for name, indices in first.items():
        for index in indices:
            at[(name, *index)] = len(at)
    count = len(at)

    def share(keys, *names):
        free = [at[(name, *index)] for name in names for index in first[name]]
        for key, i in zip(keys, free, strict=False):
            at[key] = i
        return free[len(keys) :]

    groups, halves = (0, 1), (0, 1)
    left = share([("dz", i) for i in range(1, 8)], "w")
    for key, i in zip([("dt", xi, g) for xi in range(4) for g in groups], left, strict=True):
        at[key] = i
    plane = [(xi, yi) for xi in range(4) for yi in range(4) if xi or yi]
    share([("dp", g, *at_plane) for g in groups for at_plane in plane], "x", "oz", "more", "load")
    back = [("ht", xi) for xi in range(4)] + [("rx", *at_plane) for at_plane in plane]
    back += [("rz", half, i) for half in halves for i in range(1, 8)]
    share(back, "ox", "ol", "m", "b")
    return at, count


AT, COUNT = semaphores()


def scratch_shapes():
    vm, dma = pltpu.VMEM, pltpu.SemaphoreType.DMA
    return dict(
        sv=vm((S, H), BF),
        hv=vm((S, H), F32),
        cv=vm((3, S, H), BF),
        g1v=vm((1, H), F32),
        tv=vm((4, H), BF),
        rgv=vm((H, 64), BF),
        igv=vm((H, 64), BF),
        dv=vm((1, H), F32),
        g2v=vm((1, H), F32),
        rtv=vm((2, S), jnp.int32),
        rwv=vm((2, S), F32),
        wg=vm((Q, 2, LANES, FD), BF),
        wu=vm((Q, 2, LANES, FD), BF),
        wd=vm((FD, D), BF),
        xs=vm((NZ, S, H), BF),
        ms=vm((NY, S, H), BF),
        wt=vm((2, 4, 4, S, H), BF),
        wo=vm((NX, NZ, S, H), BF),
        ps=vm((NZ * S, 512), BF),
        pr=vm((NZ * S, 512), BF),
        ss=vm((NZ, S, 512), BF),
        ra=vm((4, S, 512), BF),
        ps2=vm((NY, 2, S, 256), BF),
        svo=vm((S, H), BF),
        rb=vm((2, NY, 2, S, 256), BF),
        qs=vm((S, LANES), F32),
        qr=vm((S, LANES), F32),
        bd=vm((2, 4, 256, 256), BF),
        pm=vm((EXPERTS * 16, LANES), BF),
        pw=vm((EXPERTS * 16, LANES), F32),
        zsend=vm((NZ, NY, 16, LANES), BF),
        zrecv=vm((NZ, NY, 16, LANES), BF),
        fb=vm((2, NX, NY, NZ, 16, LANES), BF),
        ab=vm((256, D), BF),
        ib=vm((256, FD), BF),
        hs=vm((NX, 64, H), BF),
        hr=vm((NX, 64, H), BF),
        own=vm((NX, 64, H), F32),
        xsend=vm((NX, NY, 16, H), BF),
        xrecv=vm((NX, NY, 16, H), BF),
        ry=vm((NY, NZ, 16, LANES), BF),
        rz=vm((NZ, NY, 16, LANES), BF),
        sends=dma((SENDS,)),
        spread=dma((2, 8)),
        a_s=dma((8,)),
        a_r=dma((4,)),
        p_s=dma((1,)),
        r=dma((COUNT,)),
    )


NAMES = tuple(scratch_shapes())


def dot(a, b, dims=((1,), (0,)), precision=None):
    return lax.dot_general(a, b, (dims, ((), ())), precision=precision, preferred_element_type=F32)


def iota(shape, dim):
    return lax.broadcasted_iota(jnp.int32, shape, dim)


def expm1(v):
    series = 1.0 + v * (1.0 / 9.0)
    for n in range(8, 1, -1):
        series = 1.0 + v * (1.0 / n) * series
    return jnp.where(v > -0.5, v * series, jnp.exp(v) - 1.0)


def remote(src, dst, ssem, rsem, where):
    return pltpu.make_async_remote_copy(
        src_ref=src, dst_ref=dst, send_sem=ssem, recv_sem=rsem, device_id=where, device_id_type=MESH
    )


def kernel(*refs):
    (stream, hidden, conv, gain1, w_in, w_br, taps, rg, ig, decay, w_out, gain2, routes, rw, eg, eu, ed) = refs[:17]
    o_stream, o_hidden, o_conv = refs[17:20]
    k = dict(zip(NAMES, refs[20:]))
    z, y, x, tp = (lax.axis_index(a) for a in EP_TP)
    other = 1 - tp
    sent = []

    barrier = pltpu.get_barrier_semaphore()
    for d in ORDER[8]:
        pl.semaphore_signal(barrier, inc=1, device_id={"z": lax.rem(z + d, NZ)}, device_id_type=MESH)
    for i, j in PLANE:
        there = {"y": lax.rem(y + XORD[j], NY), "x": lax.rem(x + XORD[i], NX)}
        pl.semaphore_signal(barrier, inc=1, device_id=there, device_id_type=MESH)
    for d in ORDER[4]:
        there = {"y": lax.rem(y + d, NY), "tp": other}
        pl.semaphore_signal(barrier, inc=1, device_id=there, device_id_type=MESH)
    pl.semaphore_signal(barrier, inc=1, device_id={"tp": other}, device_id_type=MESH)

    a = y + tp * (x - y)
    b = x + tp * (y - x)
    plan = [
        (stream, k["sv"]), (gain1, k["g1v"]),
        (w_in, k["wt"].at[0, a, b]), (w_br, k["wt"].at[1, a, b]), (w_out, k["wo"].at[x, z]),
        (rg, k["rgv"]), (ig, k["igv"]), (routes, k["rtv"]), (rw, k["rwv"]),
        (conv, k["cv"]), (taps, k["tv"]), (decay, k["dv"]), (hidden, k["hv"]), (gain2, k["g2v"]),
        (eg.at[0], k["wg"].at[:, 0]), (eg.at[1], k["wg"].at[:, 1]),
        (eu.at[0], k["wu"].at[:, 0]), (eu.at[1], k["wu"].at[:, 1]), (ed, k["wd"]),
    ]
    loads = [pltpu.make_async_copy(s, t, k["r"].at[AT[("load", i)]]) for i, (s, t) in enumerate(plan)]
    for c in loads:
        c.start()

    def sem(name, *index):
        return k["r"].at[AT[(name, *index)]]

    def start(src, dst, rsem, where):
        n = len(sent)
        if n >= SENDS:
            sent[n - SENDS].wait_send()
        c = remote(src, dst, k["sends"].at[n % SENDS], rsem, where)
        c.start()
        sent.append(c)

    def await_recv(ref, rsem, where):
        remote(ref, ref, k["sends"].at[0], rsem, where).wait_recv()

    loads[0].wait()
    loads[1].wait()
    values = k["sv"][...].astype(F32)
    k["xs"][z] = (values * k["g1v"][...]).astype(BF)
    k["qs"][...] = jnp.broadcast_to(jnp.sum(values * values, axis=1, keepdims=True), (S, LANES))
    loads[5].wait()
    loads[6].wait()
    eye = (iota((64, 256), 1) % 64 == iota((64, 256), 0)).astype(BF)
    on = iota((H, 256), 0) // 64 % 4 == iota((H, 256), 1) // 64
    for n, ref in enumerate((k["rgv"], k["igv"])):
        k["bd"][n] = jnp.where(on, dot(ref[...], eye), 0.0).astype(BF).reshape(4, 256, 256)

    loads[7].wait()
    loads[8].wait()
    spread = (iota((S, LANES), 1) % S == iota((S, LANES), 0)).astype(F32)
    named = dot(k["rtv"][...].astype(F32), spread, precision=HIGHEST)
    weights = dot(k["rwv"][...], spread, precision=HIGHEST)
    rows = (EXPERTS * 16, LANES)
    expert = (iota(rows, 0) // 16).astype(F32)
    hit0, hit1 = named[0:1] == expert, named[1:2] == expert
    hits = jnp.where(hit0 | hit1, 1.0, 0.0)
    square = (LANES, LANES)
    before = (iota(square, 0) < iota(square, 1) % S).astype(BF)
    rank = dot(hits.astype(BF), before)
    slot = (iota(rows, 0) // Q % CAP).astype(F32)
    same = iota(rows, 0) % Q == iota(rows, 1) // S
    chosen = (hits > 0.5) & (rank == slot) & same
    k["pm"][...] = jnp.where(chosen, 1.0, 0.0).astype(BF)
    step = iota(rows, 0) // 16 % 4
    step = jnp.where(step == 2, 3, jnp.where(step == 3, 2, step))
    expert = (iota(rows, 0) // 64 * 4 + (y + step) % 4).astype(F32)
    hit0, hit1 = named[0:1] == expert, named[1:2] == expert
    hits = jnp.where(hit0 | hit1, 1.0, 0.0)
    chosen = (hits > 0.5) & (dot(hits.astype(BF), before) == slot) & same
    k["pw"][...] = jnp.where(chosen, jnp.where(hit0, weights[0:1], weights[1:2]), 0.0)

    for i in (2, 3, 4):
        loads[i].wait()
    with jax.named_scope("w_bar"):
        pl.semaphore_wait(barrier, 26)

    def along_b(d):
        return {"y": lax.rem(y + d * tp, NY), "x": lax.rem(x + d * other, NX)}

    def along_a(d):
        return {"y": lax.rem(y + d * other, NY), "x": lax.rem(x + d * tp, NX)}

    both = pl.ds(0, 2)

    def block(da, db):
        return k["wt"].at[both, lax.rem(a - da + 4, 4), lax.rem(b - db + 4, 4)]

    def push(ref, i, along):
        for d in ORDER[4]:
            start(ref, ref, sem("w", i, d), along(d))

    def pull(ref, i, d):
        await_recv(ref, sem("w", i, d), {"tp": other})

    push(block(0, 0), 4, along_b)
    push(block(0, 0), 0, along_a)
    near = (2, 6, 1, 7)
    lanes = (pl.ds(0, H // 2), pl.ds(H // 2, H // 2))

    def along_z(d):
        return {"z": lax.rem(z + d, NZ)}

    def slot(ref, d):
        return ref.at[lax.rem(z - d + NZ, NZ)]

    def column_send(ref, name):
        for d in near:
            start(ref.at[z], ref.at[z], sem(name, d), along_z(d))

    def column_relay(ref, name):
        for n, d in enumerate((2, 6)):
            got, piece = slot(ref, d), slot(ref, d).at[:, lanes[n]]
            await_recv(got, sem(name, d), {"tp": other})
            start(piece, piece, sem(name, (0, 4)[n]), along_z(d))
            start(got, got, sem(name, (3, 5)[n]), along_z((1, 7)[n]))

    def column_end(ref, name):
        for d in (3, 5):
            await_recv(slot(ref, d), sem(name, d), {"tp": other})
        for n in range(2):
            await_recv(slot(ref, 4).at[:, lanes[n]], sem(name, (0, 4)[n]), {"tp": other})

    rows_column = (k["xs"], "x")
    weight_column = (k["wo"].at[x], "oz")
    column_send(*rows_column)
    start(k["qs"], k["qr"], sem("t", 0), {"tp": other})
    start(k["sv"], k["svo"], sem("t", 3), {"tp": other})
    column_send(*weight_column)
    def spread_slots(ds, core):
        copies = []
        for d in ds:
            for n in range(2):
                ref, where = k["wo"].at[x, lax.rem(z - d + NZ, NZ)], {"x": lax.rem(x + (1, 3)[n], NX)}
                copies.append(remote(ref, ref, k["spread"].at[n, d], sem("ox", n, d), where))

        @pl.when(tp == core)
        def _():
            for c in copies:
                c.start()

        return copies

    def relay_slot(d):
        for n in range(2):
            ref = k["wo"].at[lax.rem(x + (3, 1)[n], NX), lax.rem(z - d + NZ, NZ)]
            await_recv(ref, sem("ox", n, d), {"tp": other})
            if n == (d in (3, 4, 5, 6)):
                start(ref, ref, sem("ol", d), {"x": lax.rem(x + (1, 3)[n], NX)})

    with jax.named_scope("w_b"):
        for i in (1, 3, 2):
            pull(block(0, i), 4, i)
            push(block(0, i), i, along_a)
    with jax.named_scope("w_xz"):
        column_relay(*rows_column)
    with jax.named_scope("w_oz"):
        column_relay(*weight_column)
        for d in (1, 7):
            await_recv(slot(weight_column[0], d), sem("oz", d), {"tp": other})
        spread_slots((0, 1, 7, 2, 6), 1)
    with jax.named_scope("w_xg"):
        for d in (1, 7):
            await_recv(slot(k["xs"], d), sem("x", d), {"tp": other})
        column_end(*rows_column)
    with jax.named_scope("w_oze"):
        column_end(*weight_column)
        spread_slots((3, 5, 4), 1)
        spread_slots((0, 1, 7, 2, 6, 3, 5, 4), 0)
    with jax.named_scope("w_aend"):
        for i in (0, 1, 3, 2):
            for d in (1, 3, 2):
                pull(block(d, i), i, d)

    def columns(kind):
        blocks = []
        for i in range(4):
            for j in range(4):
                blocks.append(k["wt"][kind, i + tp * (j - i), j + tp * (i - j)])
        return jnp.concatenate(blocks, axis=0)

    def project(rows_ref, kinds, width, ps, pr, ss, land, t, sends, lands, meanwhile):
        lhs = k[rows_ref][...].reshape(NZ * S, H)
        part = jnp.concatenate([dot(lhs, columns(kind), ((1,), (1,))) for kind in kinds], axis=1)

        @pl.when(tp != z // 4)
        def _():
            k[ps][...] = part.astype(BF)
            c = remote(k[ps], k[pr], k["p_s"].at[0], sem("t", t), {"tp": other})
            c.start()
            c.wait_send()

        @pl.when(tp == z // 4)
        def _():
            await_recv(k[pr], sem("t", t), {"tp": other})
            total = (part + k[pr][...].astype(F32)).astype(BF)
            k[ss][...] = total.reshape(NZ, S, width)
            mine = lax.rem(z, 4)
            for d in ORDER[8]:
                there = lax.rem(z + d, NZ)
                remote(k[ss].at[there], k[land].at[mine], k[sends].at[d], k[lands].at[mine], {"z": there}).start()
            k[land][mine] = k[ss][z]

        meanwhile()
        for i in range(4):
            @pl.when(4 * tp + i != z)
            def _():
                await_recv(k[land].at[i], k[lands].at[i], {"tp": other})

    def sends_done(ss, land, sends, lands):
        @pl.when(tp == z // 4)
        def _():
            for d in ORDER[8]:
                remote(k[ss].at[0], k[land].at[0], k[sends].at[d], k[lands].at[0], {"tp": other}).wait_send()

    def output_weight():
        with jax.named_scope("w_ox"):
            for d in (0, 1, 7, 2, 6):
                relay_slot(d)

    project("xs", (0, 1), 512, "ps", "pr", "ss", "ra", 1, "a_s", "a_r", output_weight)
    await_recv(k["qr"], sem("t", 0), {"tp": other})
    row_scale = lax.rsqrt((k["qs"][...] + k["qr"][...])[:, 0:1] / D + EPSILON)
    forward = (jnp.concatenate([k["ra"][i, :, 0:256] for i in range(4)], axis=1).astype(F32) * row_scale).astype(BF)
    branch = (jnp.concatenate([k["ra"][i, :, 256:512] for i in range(4)], axis=1).astype(F32) * row_scale).astype(BF)
    for i in range(9, 14):
        loads[i].wait()
    window = [k["cv"][0], k["cv"][1], k["cv"][2], forward]
    o_conv[0] = window[1]
    o_conv[1] = window[2]
    o_conv[2] = forward
    tap_rows = k["tv"][...].astype(F32)
    conv_out = sum(window[i].astype(F32) * tap_rows[i : i + 1] for i in range(4)).astype(BF)

    def gate_map(n):
        return jnp.concatenate([dot(conv_out[:, g * 256 : g * 256 + 256], k["bd"][n, g]) for g in range(4)], axis=1)

    recur_open = jax.nn.sigmoid(gate_map(0))
    inward = jax.nn.sigmoid(gate_map(1))
    logit = -k["dv"][...]
    softplus = jnp.maximum(logit, 0.0) + jnp.log1p(jnp.exp(-jnp.abs(logit)))
    log_decay = -DECAY_POWER * recur_open * softplus
    new_hidden = jnp.exp(log_decay) * k["hv"][...] + jnp.sqrt(-expm1(2.0 * log_decay)) * (
        inward * conv_out.astype(F32)
    )
    o_hidden[...] = new_hidden
    k["ms"][y] = (jax.nn.gelu(branch.astype(F32)) * new_hidden).astype(BF)
    for d in ORDER[4]:
        start(k["ms"].at[y], k["ms"].at[y], sem("m", d), {"y": lax.rem(y + d, NY)})
    with jax.named_scope("w_ox2"):
        for d in (3, 5, 4):
            relay_slot(d)
        for d in range(NZ):
            ref = k["wo"].at[lax.rem(x + 2, NX), lax.rem(z - d + NZ, NZ)]
            await_recv(ref, sem("ol", d), {"tp": other})
    with jax.named_scope("w_mg"):
        for d in ORDER[4]:
            await_recv(k["ms"].at[lax.rem(y - d + NY, NY)], sem("m", d), {"tp": other})
    lhs = k["ms"][...].reshape(NY * S, H)
    for h in range(2):
        out_columns = jnp.concatenate([k["wo"][j, 4 * h + i] for i in range(4) for j in range(NX)], axis=0)
        part = dot(lhs, out_columns, ((1,), (1,)))
        k["ps2"][:, h] = part.astype(BF).reshape(NY, S, 256)
    for d in ORDER[4] + (0,):
        there = lax.rem(y + d, NY)
        for n, core in enumerate((tp, other)):
            if d or n:
                where = {"y": there, "tp": core}
                start(k["ps2"].at[there], k["rb"].at[n, y], sem("b", n, d), where)
    k["rb"][0, y] = k["ps2"][y]
    with jax.named_scope("w_rb"):
        await_recv(k["svo"], sem("t", 3), {"tp": other})
        for d in ORDER[4] + (0,):
            for n in range(2):
                if d or n:
                    ref = k["rb"].at[n, lax.rem(y - d + NY, NY)]
                    await_recv(ref, sem("b", n, d), {"tp": other})

    def middle_of(ref, h):
        landed = k["rb"][0, :, h].astype(F32) + k["rb"][1, :, h].astype(F32)
        out_terms = jnp.concatenate(
            [landed[j, :, i * 64 : i * 64 + 64] for i in range(4) for j in range(NY)], axis=1
        )
        return (ref[...].astype(F32) + out_terms).astype(BF).astype(F32)

    mid_values = middle_of(k["sv"], tp)
    theirs_mid = middle_of(k["svo"], other)
    mid_power = sum(jnp.sum(m * m, axis=1, keepdims=True) for m in (mid_values, theirs_mid)) / D
    mid_scale = lax.rsqrt(mid_power + EPSILON)
    normed = (mid_values * mid_scale * k["g2v"][...]).astype(BF)

    stacked = jnp.concatenate([normed[:, q * LANES : (q + 1) * LANES] for q in range(Q)], axis=0)
    k["zsend"][...] = dot(k["pm"][...], stacked).astype(BF).reshape(NZ, NY, 16, LANES)
    for i in range(1, 8):
        there = lax.rem(z + ZORD[i], NZ)
        start(k["zsend"].at[there], k["zrecv"].at[i], sem("dz", i), {"z": there})
    k["zrecv"][0] = k["zsend"][z]

    def part_of(xi, yi, g, h=tp):
        return k["fb"].at[h, xi, yi, pl.ds(*GROUPS[g])]

    def wait_plane(xi, yi, g):
        if xi or yi:
            await_recv(part_of(xi, yi, g), sem("dp", g, xi, yi), {"tp": other})

    def send_core(xi, g):
        ref = k["fb"].at[tp, xi, :, pl.ds(*GROUPS[g])]
        start(ref, ref, sem("dt", xi, g), {"tp": other})

    for g, (low, count) in enumerate(GROUPS):
        with jax.named_scope(f"w_dz{g}"):
            for i in range(max(low, 1), low + count):
                await_recv(k["zrecv"].at[i], sem("dz", i), {"tp": other})
        for i, j in PLANE:
            there = lax.rem(y + XORD[j], NY)
            src = k["zrecv"].at[pl.ds(low, count), there]
            start(src, part_of(i, j, g), sem("dp", g, i, j), {"y": there, "x": lax.rem(x + XORD[i], NX)})
        k["fb"][tp, 0, 0, low : low + count] = k["zrecv"][low : low + count, y]
    for xi in range(3):
        for g in range(2):
            with jax.named_scope(f"w_dp{xi}{g}"):
                for yi in range(NY):
                    wait_plane(xi, yi, g)
            send_core(xi, g)
    with jax.named_scope("w_we"):
        for i in range(14, 19):
            loads[i].wait()

    turn = iota(square, 1) == iota(square, 0) % 16 * Q + iota(square, 0) // 16
    turn = jnp.where(turn, 1.0, 0.0).astype(BF)

    def to_rows(xi):
        with jax.named_scope(f"w_dt{xi}"):
            for g in range(2):
                ref = k["fb"].at[other, xi, :, pl.ds(*GROUPS[g])]
                await_recv(ref, sem("dt", xi, g), {"tp": other})
        for yi in range(NY):
            pair = jnp.concatenate([k["fb"][h, xi, yi].reshape(LANES, LANES) for h in range(2)], axis=1)
            turned = dot(turn, pair).astype(BF)
            at = (xi * NY + yi) * 16
            for q in range(Q):
                k["ab"][at : at + 16, q * 256 : q * 256 + 256] = turned[q * 16 : q * 16 + 16]

    def up(low, high):
        rows = k["ab"][low:high]
        gate_act = dot(rows, k["wg"][...].reshape(D, FD))
        upper = dot(rows, k["wu"][...].reshape(D, FD))
        k["ib"][low:high] = (jax.nn.silu(gate_act) * upper).astype(BF)

    theirs = pl.ds(pl.multiple_of(other * H, H), H)
    ours = pl.ds(pl.multiple_of(tp * H, H), H)

    def down(xi):
        inner = k["ib"][xi * 64 : xi * 64 + 64]
        k["hs"][xi] = dot(inner, k["wd"][:, theirs]).astype(BF)
        start(k["hs"].at[xi], k["hr"].at[xi], sem("ht", xi), {"tp": other})
        k["own"][xi] = dot(inner, k["wd"][:, ours])

    def whole(xi):
        with jax.named_scope(f"w_ht{xi}"):
            await_recv(k["hr"].at[xi], sem("ht", xi), {"tp": other})
        return k["own"][xi] + k["hr"][xi].astype(F32)

    def send_sum(xi):
        total = whole(xi)
        for yi in (3, 2, 1, 0):
            if xi or yi:
                k["xsend"][xi, yi] = total[yi * 16 : yi * 16 + 16].astype(BF)
                where = {"y": lax.rem(y - XORD[yi] + NY, NY), "x": lax.rem(x - XORD[xi] + NX, NX)}
                start(k["xsend"].at[xi, yi], k["xrecv"].at[xi, yi], sem("rx", xi, yi), where)
        return total[:16]

    for xi in range(3):
        to_rows(xi)
    up(0, 192)
    with jax.named_scope("w_dxl"):
        for g in range(2):
            for yi in range(NY):
                wait_plane(3, yi, g)
            send_core(3, g)
    down(1)
    down(2)
    to_rows(3)
    up(192, 256)
    send_sum(1)
    send_sum(2)
    down(3)
    send_sum(3)
    down(0)
    home = send_sum(0)
    back = iota(square, 0) == iota(square, 1) % 16 * Q + iota(square, 1) // 16
    back = jnp.where(back, 1.0, 0.0).astype(BF)
    for half in (1, 0):
        for yi in (2 * half + 1, 2 * half):
            with jax.named_scope(f"w_rx{yi}"):
                for xi in range(0 if yi else 1, NX):
                    await_recv(k["xrecv"].at[xi, yi], sem("rx", xi, yi), {"tp": other})
            rows = sum(k["xrecv"][xi, yi].astype(F32) for xi in range(1, NX))
            rows = (rows + (k["xrecv"][0, yi].astype(F32) if yi else home)).astype(BF)
            part = jnp.concatenate([rows[:, q * LANES : (q + 1) * LANES] for q in range(Q)], axis=0)
            k["ry"][yi] = dot(back, part).astype(BF).reshape(NZ, 16, LANES)
        pair = pl.ds(2 * half, 2)
        for i in range(7, 0, -1):
            there = lax.rem(z - ZORD[i] + NZ, NZ)
            start(
                k["ry"].at[pair, i], k["rz"].at[z, pair], sem("rz", half, i), {"z": there}
            )
        k["rz"][z, 2 * half : 2 * half + 2] = k["ry"][2 * half : 2 * half + 2, 0]
    with jax.named_scope("w_rz"):
        for half in (1, 0):
            pair = pl.ds(2 * half, 2)
            for i in range(1, 8):
                ref = k["rz"].at[lax.rem(z + ZORD[i], NZ), pair]
                await_recv(ref, sem("rz", half, i), {"tp": other})
    returned = k["rz"][...].reshape(EXPERTS * 16, LANES).astype(F32)
    mix = dot(k["pw"][...], returned, ((0,), (0,)), HIGHEST)
    expert_mix = jnp.concatenate([mix[q * S : (q + 1) * S] for q in range(Q)], axis=1)
    o_stream[...] = (mid_values + expert_mix).astype(BF)
    for n in range(2):
        for d in range(8):
            ref = k["wo"].at[x, 0]
            remote(ref, ref, k["spread"].at[n, d], sem("ox", n, d), {"tp": other}).wait_send()
    for c in sent[-SENDS:]:
        c.wait_send()
    sends_done("ss", "ra", "a_s", "a_r")


def handed_on(*refs):
    for src, dst in zip(refs[:3], refs[3:]):
        dst[...] = src[...]


def per_device(
    stream, hidden_state, conv_state, first_gain, input_weight, branch_weight, conv_taps, recur_gate, input_gate,
    decay_logit, output_weight, second_gain, routes, route_weight, expert_gate, expert_up, expert_down,
):
    shapes = scratch_shapes()
    vmem = pl.BlockSpec(memory_space=pltpu.VMEM)
    anywhere = pl.BlockSpec(memory_space=pl.ANY)
    outs = pl.pallas_call(
        kernel,
        name="layer",
        out_shape=(
            jax.ShapeDtypeStruct((S, H), BF),
            jax.ShapeDtypeStruct((S, H), F32),
            jax.ShapeDtypeStruct((3, S, H), BF),
        ),
        in_specs=[anywhere] * 17,
        out_specs=(vmem,) * 3,
        scratch_shapes=[shapes[n] for n in NAMES],
        compiler_params=pltpu.CompilerParams(
            collective_id=0, has_side_effects=True, vmem_limit_bytes=60 * 1024 * 1024
        ),
    )(
        stream,
        hidden_state,
        conv_state.transpose(1, 0, 2),
        first_gain.reshape(1, H),
        input_weight.T,
        branch_weight.T,
        conv_taps,
        recur_gate.reshape(H, 64),
        input_gate.reshape(H, 64),
        decay_logit.reshape(1, H),
        output_weight.T,
        second_gain.reshape(1, H),
        routes.T,
        route_weight.T,
        expert_gate.reshape(2, Q, LANES, FD),
        expert_up.reshape(2, Q, LANES, FD),
        expert_down,
    )
    new_stream, new_hidden, new_conv = pl.pallas_call(
        handed_on,
        name="handed_on",
        out_shape=tuple(jax.ShapeDtypeStruct(o.shape, o.dtype) for o in outs),
        in_specs=[vmem] * 3,
        out_specs=(vmem,) * 3,
    )(*outs)
    return new_stream, new_hidden, new_conv.transpose(1, 0, 2)


def solution(mesh):
    torus = Mesh(mesh.devices.reshape(NZ, NY, NX, mesh.shape["tp"]), EP_TP)
    in_specs = (
        P(EP, "tp"),
        P(EP, "tp"),
        P(EP, None, "tp"),
        P("tp"),
        P("tp", EP),
        P("tp", EP),
        P(None, "tp"),
        P("tp", None, None),
        P("tp", None, None),
        P("tp"),
        P("tp", EP),
        P("tp"),
        P(EP, None),
        P(EP, None),
        P(None, EP_TP),
        P(None, EP_TP),
        P(EP_TP, None),
    )
    out_specs = (P(EP, "tp"), P(EP, "tp"), P(EP, None, "tp"))
    return jax.shard_map(per_device, mesh=torus, in_specs=in_specs, out_specs=out_specs, check_vma=False)
```
